32 devices in a mesh: grp: 2 (over y), sp: 8 (over z, core), tp: 2 (over x).
Axes of the slice: x: 2, y: 2, z: 4, core: 2. Of those that a mesh axis runs over, the one named last changes fastest.
Arguments:
- tokens: bfloat16 [12288, 2048], P(('grp', 'sp'), 'tp'), parts along dimension 0, may hold values from -4000 to 4000
- gain: float32 [2048], replicated, may hold values from 0.1 to 1.9
- w_query: bfloat16 [2048, 1024], P('sp', 'tp'), may hold values from -1 to 1
- w_key: bfloat16 [2048, 256], P('sp', 'tp'), may hold values from -1 to 1
- w_value: bfloat16 [2048, 256], P('sp', 'tp'), may hold values from -0.125 to 0.125
- w_input: bfloat16 [2048, 1024], P('sp', 'tp'), may hold values from -0.125 to 0.125
- w_bgate: bfloat16 [2048, 1024], P('sp', 'tp'), may hold values from -0.125 to 0.125
- w_cgate: bfloat16 [2048, 1024], P('sp', 'tp'), may hold values from -0.125 to 0.125
- w_attn_out: bfloat16 [1024, 2048], P('sp', 'tp'), may hold values from -2 to 2
- w_conv_out: bfloat16 [1024, 2048], P('sp', 'tp'), may hold values from -0.1875 to 0.1875
- sink_logit: float32 [16], P('tp'), may hold values from 0 to 5
- taps: float32 [3, 1024], P(None, 'tp'), may hold values from -3.5 to 3.5
- conv_bias: float32 [1024], P('tp'), may hold values from -4 to 4
- documents: int32 [12288], P(('grp', 'sp')), parts along dimension 0, may hold values from 0 to 3, never falling along the last dimension, each value on 1 to 3072 neighbouring positions
Outputs:
- mixed: bfloat16 [12288, 2048], P(('grp', 'sp'), 'tp'), parts along dimension 0
The draws below stay inside these ranges and needn't reach their ends.
There are 2 independent parts, one for each index of `grp`. The reference program is written for one: setup_inputs(seed, part) draws one part's arguments, and reference() takes and returns one part's arrays. A program takes and returns all parts, laid end to end along the dimension named above; an argument that names none is the same for every part. Nothing has to cross between parts.
All inputs are finite; a program needn't handle non-finite values.
Results may differ from the reference program's by a relative error of at most 0.013.
The reference program's roundings to bfloat16 on the way (of `scaled`, `weight`, `attended`, `carried` and `convolved`) count: a program that leaves them out, or rounds other values in their place, can miss the bound.
Values may be sent and summed in bfloat16 or wider, within the bound.
A program may use at most 64 MiB of HBM per device.

```python
import math
import jax
import jax.numpy as jnp
import numpy as np
from jax import lax

D = 2048
Q_HEADS = 16
KV_HEADS = 4
HEAD_DIM = 64
CW = 1024
WINDOW = 128
TOK_DEV = 768
QW = 1024
KVW = 256
TOKENS = 6144
DOCS = 4


def draw_tokens(key, part):
    f32 = jnp.float32
    base = jnp.clip(jax.random.normal(jax.random.fold_in(key, 11), (TOKENS, D), f32), -6.0, 6.0)
    columns = jnp.exp(jax.random.uniform(jax.random.fold_in(key, 12), (D,), f32, 0.0, jnp.log(10.0)))
    order = jax.random.permutation(jax.random.fold_in(key, 13), 4).astype(f32)
    blocks = jnp.power(3.0, order / 3.0)
    block_of = (jnp.arange(D) // (D // 4)).astype(jnp.int32)
    columns = columns * blocks[block_of]
    rows = jnp.exp(jax.random.uniform(jax.random.fold_in(key, 14), (TOKENS, 1), f32, 0.0, jnp.log(10.0)))
    values = base * columns[None, :] * rows
    return values.astype(jnp.bfloat16)


def query_parts(key):
    f32 = jnp.float32
    base = jnp.clip(jax.random.normal(jax.random.fold_in(key, 101), (D, Q_HEADS * HEAD_DIM), f32), -6.0, 6.0) * D ** (-0.5)
    return base


def draw_w_query(key, part):
    base = query_parts(key)
    values = base
    return jnp.clip(values, -1.0, 1.0).astype(jnp.bfloat16)


def draw_w_key(key, part):
    f32 = jnp.float32
    values = jnp.clip(jax.random.normal(jax.random.fold_in(key, 202), (D, KV_HEADS * HEAD_DIM), f32), -6.0, 6.0) * D ** (-0.5)
    return jnp.clip(values, -1.0, 1.0).astype(jnp.bfloat16)


def steps_of(stream_key, dims, cuts, least, top_value):
    def one(axis_at, blocks):
        steps = jax.random.uniform(jax.random.fold_in(jax.random.fold_in(stream_key, 6), axis_at), (blocks,), jnp.float32, least / len(cuts), top_value / len(cuts))
        return jnp.repeat(jnp.exp(steps), dims[axis_at] // blocks).reshape((-1,) + (1,) * (len(dims) - axis_at - 1))

    level = one(*cuts[0])
    for cut in cuts[1:]:
        level = level * one(*cut)
    return level


def split_up(number_of, total, reach, slope):
    weights = [(1 << 20) // math.isqrt(grade ** slope) + 1 for grade in range(2, number_of + 1)]
    rest, given = total - reach - (number_of - 1), [1] * (number_of - 1)
    while rest > 0:
        free = [i for i in range(number_of - 1) if given[i] < reach]
        whole, remaining = sum([weights[i] for i in free]), rest
        for i in free:
            addition = min(reach - given[i], max(1, remaining * weights[i] // whole), rest)
            given[i] = given[i] + addition
            rest = rest - addition
    return np.array([reach] + given)


def uneven(own_key, amount, total, limit, lean):
    if amount == 2:
        one = jax.random.randint(own_key, (), max(1, total - limit), min(limit, total - 1) + 1)
        return jnp.stack([one, total - one])
    sizes = jnp.asarray(split_up(amount, total, limit, lean), jnp.int32)
    twos = (amount - 1) // 2
    donor, receiver = sizes[1:1 + 2 * twos:2], sizes[2:2 + 2 * twos:2]
    slack = jnp.minimum(donor - 1, limit - receiver)
    shifted = jax.random.randint(jax.random.fold_in(own_key, 1), (twos,), 0, 1 << 20) % (slack + 1)
    sizes = sizes.at[1:1 + 2 * twos:2].set(donor - shifted).at[2:2 + 2 * twos:2].set(receiver + shifted)
    return sizes[jax.random.permutation(jax.random.fold_in(own_key, 2), amount)]


def centred(rng, dims, spread, most, cuts=(), kind=jnp.bfloat16):
    result = spread * jax.random.normal(rng, dims, jnp.float32)
    if cuts:
        result = result * steps_of(rng, dims, cuts, -0.22, 0.18)
    return jnp.clip(result, -most, most).astype(kind)


def setup_inputs(seed: int = 0, part: int = 0) -> dict:
    key_list = jax.random.split(jax.random.key(seed), 15)
    part_keys = jax.random.split(jax.random.fold_in(key_list[14], part), 15)
    tokens = draw_tokens(jax.random.fold_in(jax.random.fold_in(key_list[14], part), 71), part)
    gain = jnp.clip(1.0 + 0.18 * jax.random.normal(key_list[1], (D,), jnp.float32), 0.1, 1.9)
    w_query = draw_w_query(jax.random.fold_in(key_list[14], 71), part)
    w_key = draw_w_key(jax.random.fold_in(key_list[14], 71), part)
    w_value = centred(key_list[4], (D, KVW), D ** -0.5, 0.125, ((0, 8), (1, 2)))
    w_input = centred(key_list[5], (D, CW), D ** -0.5, 0.125, ((0, 8), (1, 2)))
    w_bgate = centred(key_list[6], (D, CW), D ** -0.5, 0.125, ((0, 8), (1, 2)))
    w_cgate = centred(key_list[7], (D, CW), D ** -0.5, 0.125, ((0, 8), (1, 2)))
    w_attn_out = centred(key_list[8], (QW, D), (max(1, QW // 128)) ** -0.5, 2.0, ((0, 8), (1, 2)))
    w_conv_out = centred(key_list[9], (CW, D), CW ** -0.5, 0.1875, ((0, 8), (1, 2)))
    sink_logit = jnp.clip(5.0 * jax.random.uniform(key_list[10], (Q_HEADS,), jnp.float32) ** steps_of(key_list[10], (Q_HEADS,), ((0, 2),), -0.2, 0.2), 0.0, 5.0)
    taps = centred(key_list[11], (3, CW), 3 ** -0.5, 3.5, ((1, 2),), jnp.float32)
    conv_bias = centred(key_list[12], (CW,), 1.0, 4.0, ((0, 2),), jnp.float32)
    documents = jnp.searchsorted(jnp.cumsum(uneven(part_keys[13], DOCS, TOKENS, 4 * TOK_DEV, 0)), jnp.arange(TOKENS), side="right").astype(jnp.int32)
    return {"tokens": tokens, "gain": gain, "w_query": w_query, "w_key": w_key, "w_value": w_value, "w_input": w_input, "w_bgate": w_bgate, "w_cgate": w_cgate, "w_attn_out": w_attn_out, "w_conv_out": w_conv_out, "sink_logit": sink_logit, "taps": taps, "conv_bias": conv_bias, "documents": documents}


EPS = 1e-06
THETA = 500000.0

def rotate(proj, positions, heads):
    rows = proj.shape[0]
    size = proj.shape[1] // heads
    half = size // 2
    freq = jnp.power(THETA, -(jnp.arange(half, dtype=jnp.float32) * (2.0 / size)))
    angle = positions.astype(jnp.float32)[:, None] * freq[None, :]
    cosine = jnp.cos(angle)[:, None, :]
    sine = jnp.sin(angle)[:, None, :]
    shaped = proj.reshape(rows, heads, size)
    first = shaped[..., :half]
    second = shaped[..., half:]
    turned = jnp.concatenate([first * cosine - second * sine, second * cosine + first * sine], axis=-1)
    return turned.reshape(rows, heads * size)

def sink_softmax(scores, allowed, sinks):
    masked = jnp.where(allowed, scores, -jnp.inf)
    top = jnp.maximum(lax.optimization_barrier(jnp.max(masked, axis=-1, keepdims=True)), sinks)
    expo = jnp.exp(masked - top)
    return expo / (lax.optimization_barrier(jnp.sum(expo, axis=-1, keepdims=True)) + jnp.exp(sinks - top))

def reference(tokens, gain, w_query, w_key, w_value, w_input, w_bgate, w_cgate, w_attn_out, w_conv_out, sink_logit, taps, conv_bias, documents):
    f32 = jnp.float32
    total = tokens.shape[0]
    xf = tokens.astype(f32)
    inv = lax.rsqrt(lax.optimization_barrier(jnp.sum(xf * xf, axis=1)) / D + EPS)[:, None]
    scaled = (xf * gain[None, :]).astype(jnp.bfloat16)
    qp = jnp.dot(scaled, w_query, preferred_element_type=f32) * inv
    kp = jnp.dot(scaled, w_key, preferred_element_type=f32) * inv
    vp = jnp.dot(scaled, w_value, preferred_element_type=f32) * inv
    upr = jnp.dot(scaled, w_input, preferred_element_type=f32) * inv
    bpr = jnp.dot(scaled, w_bgate, preferred_element_type=f32) * inv
    cpr = jnp.dot(scaled, w_cgate, preferred_element_type=f32) * inv
    positions = jnp.arange(total, dtype=jnp.int32)
    query = rotate(qp, positions, Q_HEADS).astype(jnp.bfloat16)
    keys = rotate(kp, positions, KV_HEADS).astype(jnp.bfloat16).reshape(total, KV_HEADS, HEAD_DIM)
    values = vp.astype(jnp.bfloat16).reshape(total, KV_HEADS, HEAD_DIM)
    groups = Q_HEADS // KV_HEADS
    sinks = sink_logit.astype(f32).reshape(KV_HEADS, groups, 1, 1)
    key_pad = jnp.pad(keys, ((WINDOW, WINDOW), (0, 0), (0, 0)))
    val_pad = jnp.pad(values, ((WINDOW, WINDOW), (0, 0), (0, 0)))
    doc_pad = jnp.pad(documents, (WINDOW, WINDOW), constant_values=-1)
    block = math.gcd(total, 512)
    span = block + 2 * WINDOW

    def one_block(index):
        begin = (index * block).astype(jnp.int32)
        qb = lax.dynamic_slice_in_dim(query, begin, block, 0).reshape(block, KV_HEADS, groups, HEAD_DIM)
        kb = lax.dynamic_slice_in_dim(key_pad, begin, span, 0)
        vb = lax.dynamic_slice_in_dim(val_pad, begin, span, 0)
        qdoc = lax.dynamic_slice_in_dim(documents, begin, block, 0)
        kdoc = lax.dynamic_slice_in_dim(doc_pad, begin, span, 0)
        qpos = begin + jnp.arange(block, dtype=jnp.int32)
        kpos = begin - WINDOW + jnp.arange(span, dtype=jnp.int32)
        scores = jnp.einsum('qhgd,khd->hgqk', qb.astype(f32), kb.astype(f32)) * HEAD_DIM ** (-0.5)
        allowed = (jnp.abs(qpos[:, None] - kpos[None, :]) <= WINDOW) & (qdoc[:, None] == kdoc[None, :])
        allowed = allowed & (kpos >= 0)[None, :] & (kpos < total)[None, :]
        weight = sink_softmax(scores, allowed, sinks).astype(jnp.bfloat16)
        out = jnp.einsum('hgqk,khd->qhgd', weight.astype(f32), vb.astype(f32))
        return out.astype(jnp.bfloat16).reshape(block, Q_HEADS * HEAD_DIM)
    attended = lax.map(one_block, jnp.arange(total // block, dtype=jnp.int32)).reshape(total, Q_HEADS * HEAD_DIM)
    carried = (cpr * upr).astype(jnp.bfloat16)
    car_pad = jnp.pad(carried, ((1, 1), (0, 0)))
    doc_near = jnp.pad(documents, (1, 1), constant_values=-1)
    conv = jnp.zeros((total, CW), f32)
    for tap in range(3):
        same = (doc_near[tap:tap + total] == documents)[:, None]
        conv = conv + jnp.where(same, car_pad[tap:tap + total].astype(f32) * taps[tap][None, :], 0.0)
    convolved = (bpr * (conv + conv_bias[None, :])).astype(jnp.bfloat16)
    mixed = jnp.dot(attended, w_attn_out, preferred_element_type=f32) + jnp.dot(convolved, w_conv_out, preferred_element_type=f32)
    return mixed.astype(jnp.bfloat16)
```

```python
import functools

import jax
import jax.numpy as jnp
import numpy as np
from jax import lax
from jax.experimental import pallas as pl
from jax.experimental.pallas import tpu as pltpu
from jax.sharding import PartitionSpec as P

HEAD_DIM = 64
WINDOW = 128


EPS = 1e-06
THETA = 500000.0
ATT_UNITS = 2
CONV_UNITS = 4
OUT_UNITS = 2
LATE = 3
CHUNK = 256
LANES = 128


def fused_plan(grp_count, sp_count, tp_count, rows, part, proj_rows, out_rows, q_width, k_width, c_width):
    lines = sp_count // 2
    return (
        grp_count == 2
        and tp_count == 2
        and sp_count % 2 == 0
        and lines == 4
        and proj_rows % (2 * CONV_UNITS * 16) == 0
        and proj_rows % (2 * ATT_UNITS * 16) == 0
        and out_rows % (2 * OUT_UNITS * 16) == 0
        and rows % CHUNK == 0
        and 3 * CHUNK <= rows <= 1024
        and CHUNK == 2 * WINDOW
        and WINDOW == LANES
        and part % 256 == 0
        and q_width % 256 == 0
        and k_width == LANES
        and c_width % 256 == 0
        and 2 * HEAD_DIM == LANES
    )


def layer_kernel(
    sizes,
    tok_hbm,
    gain_ref,
    wk_ref,
    wv_ref,
    wc_ref,
    wu_ref,
    wb_ref,
    wq_ref,
    wa_ref,
    wm_ref,
    sink_ref,
    taps_ref,
    bias_ref,
    doc_ref,
    freq_ref,
    out_ref,
    wp_full,
    wo_full,
    tok_own,
    tok_other,
    scaled,
    inv_ref,
    proj_ref,
    acc_ref,
    stage,
    pair_ext,
    query_s,
    carried,
    doc_row,
    doc_col,
    turn_ref,
    cos_ref,
    sin_ref,
    convolved,
    conv_other,
    attended,
    att_other,
    z_send,
    z_recv,
    y_send,
    y_recv,
    dz_send,
    dz_recv,
    dy_send,
    dy_recv,
    do_send,
    do_recv,
    x_send,
    x_recv,
    own_sem,
    tok_sem,
    out_sem,
    halo_send,
    halo_recv,
    conv_send,
    conv_recv,
    att_send,
    att_recv,
):
    lines, rp, ro = sizes
    f32 = jnp.float32
    bf16 = jnp.bfloat16
    rows, part = tok_own.shape
    k_width, c_width, q_width = wk_ref.shape[1], wc_ref.shape[1], wq_ref.shape[1]
    k_at = 3 * c_width
    q_at = k_at + 2 * k_width
    width = q_at + q_width
    chunks = rows // CHUNK
    blocks = rows // WINDOW
    order = (chunks - 1,) + tuple(range(chunks - 1))
    y = lax.axis_index("grp")
    sp = lax.axis_index("sp")
    x = lax.axis_index("tp")
    z, c = sp // 2, sp % 2
    counts = (ATT_UNITS, CONV_UNITS, OUT_UNITS)
    fulls = (wp_full, wp_full, wo_full)
    heights = (rp, rp, ro)
    spans = ((k_at, width), (0, k_at), (0, 2 * part))
    first_unit = (0, ATT_UNITS, ATT_UNITS + CONV_UNITS)
    marks = [0]
    for count in counts:
        marks.append(marks[-1] + (lines - 1) * count)
    to_y = {"grp": 1 - y}
    to_core = {"sp": z * 2 + 1 - c}
    to_x = {"tp": 1 - x}
    to_z = ({"sp": sp + 2}, {"sp": sp - 2})
    has_next = (z < lines - 1, z > 0)

    def origin(way, t):
        return z - t if way == 0 else z + t

    def arrives(way, t):
        return z >= t if way == 0 else z < lines - t

    def place(g, j, zo, cc, h):
        size = heights[g]
        tall = size // 2 // counts[g]
        row = (zo * 2 + cc) * size + h * (size // 2) + j * tall
        return fulls[g].at[pl.ds(pl.multiple_of(row, tall), tall), spans[g][0] : spans[g][1]]

    def remote(src, dst, send, recv, device):
        return pltpu.make_async_remote_copy(
            src_ref=src, dst_ref=dst, send_sem=send, recv_sem=recv,
            device_id=device, device_id_type=pl.DeviceIdType.MESH,
        )

    def z_copy(way, t, g, j):
        ref, u = place(g, j, origin(way, t), c, y), first_unit[g] + j
        return remote(ref, ref, z_send.at[way, t, u], z_recv.at[way, t, u], to_z[way])

    def z_arrival(way, t, g, j):
        ref, u = place(g, j, origin(way, t), c, y), first_unit[g] + j
        return remote(ref, ref, z_send.at[way, t - 1, u], z_recv.at[way, t - 1, u], to_z[way])

    def y_copy(way, t, g, j):
        ref, u = place(g, j, origin(way, t), c, y), first_unit[g] + j
        return remote(ref, ref, y_send.at[way, t - 1, u], y_recv.at[way, t - 1, u], to_y)

    def y_arrival(way, t, g, j):
        ref, u = place(g, j, origin(way, t), c, 1 - y), first_unit[g] + j
        return remote(ref, ref, y_send.at[way, t - 1, u], y_recv.at[way, t - 1, u], to_y)

    def d_copy(kind, way, t, g, j, cc):
        send, recv = (dz_send, dz_recv) if kind == 0 else (dy_send, dy_recv)
        ref, u = place(g, j, origin(way, t), cc, y if kind == 0 else 1 - y), first_unit[g] + j
        return remote(ref, ref, send.at[way, t - 1, u], recv.at[way, t - 1, u], to_core)

    def own_rows(g, cc):
        size = heights[g]
        return pl.ds(pl.multiple_of((z * 2 + cc) * size, size), size)

    def own_d(g, cc):
        dst = fulls[g].at[own_rows(g, cc), spans[g][0] : spans[g][1]]
        return remote(dst, dst, do_send.at[g], do_recv.at[g], to_core)

    own_refs = ((wk_ref, wv_ref, wq_ref), (wc_ref, wu_ref, wb_ref), (wa_ref, wm_ref))

    def own_local(g):
        at, copies, col = own_rows(g, c), [], spans[g][0]
        for j, ref in enumerate(own_refs[g]):
            size = ref.shape[1]
            copies.append(
                pltpu.make_async_copy(
                    ref, fulls[g].at[at, col : col + size], own_sem.at[3 * g + j]
                )
            )
            col += size
        return copies

    def tok_local(k):
        at = slice(k * CHUNK, (k + 1) * CHUNK)
        return pltpu.make_async_copy(tok_hbm.at[at, :], tok_own.at[at, :], tok_sem.at[k])

    def x_copy(k):
        at = slice(k * CHUNK, (k + 1) * CHUNK)
        return remote(tok_own.at[at, :], tok_other.at[at, :], x_send.at[k], x_recv.at[k], to_x)

    last = 2 * lines - 1
    steps_sp = (sp + 1, sp - 1)
    sends_to = (sp < last, sp > 0)
    gets_from = (sp > 0, sp < last)
    side = jnp.where(c == 0, sp - 1, sp + 1)
    has_side = (side >= 0) & (side <= last)
    edge = 16

    def halo(kind, way):
        if kind == 0:
            at = rows if way == 0 else WINDOW
            src = doc_row.at[:, at : at + WINDOW]
            at = 0 if way == 0 else WINDOW + rows
            dst = doc_row.at[:, at : at + WINDOW]
        elif kind == 1:
            at = rows if way == 0 else WINDOW
            src = pair_ext.at[at : at + WINDOW, :]
            at = 0 if way == 0 else WINDOW + rows
            dst = pair_ext.at[at : at + WINDOW, :]
        else:
            at = rows if way == 0 else edge
            src = carried.at[at : at + edge, :]
            at = 0 if way == 0 else edge + rows
            dst = carried.at[at : at + edge, :]
        return remote(
            src, dst, halo_send.at[kind, way], halo_recv.at[kind, way], {"sp": steps_sp[way]}
        )

    def start_halo(kind, way):
        @pl.when(sends_to[way])
        def _():
            halo(kind, way).start()

    def wait_halo(kind):
        for way in range(2):

            @pl.when(gets_from[way])
            def _():
                halo(kind, way).wait_recv()

    def conv_copy(k):
        at = slice(k * CHUNK, (k + 1) * CHUNK)
        return remote(
            convolved.at[at, :], conv_other.at[at, :], conv_send.at[k], conv_recv.at[k], to_x
        )

    def att_copy(i):
        at = pl.ds(pl.multiple_of(i * WINDOW, WINDOW), WINDOW)
        return remote(attended.at[at, :], att_other.at[at, :], att_send.at[i], att_recv.at[i], to_x)

    def start_own(g):
        for copy in own_local(g):
            copy.wait()
        for j in range(counts[g]):
            for way in range(2):

                @pl.when(has_next[way])
                def _():
                    z_copy(way, 0, g, j).start()

        own_d(g, c).start()

    def z_event(g, m):
        t, j = m // counts[g] + 1, m % counts[g]
        for way in range(2):

            @pl.when(arrives(way, t))
            def _():
                z_arrival(way, t, g, j).wait_recv()

                @pl.when(has_next[way] & (t < lines - 1))
                def _():
                    z_copy(way, t, g, j).start()

                y_copy(way, t, g, j).start()
                d_copy(0, way, t, g, j, c).start()

    def y_event(g, m):
        t, j = m // counts[g] + 1, m % counts[g]
        for way in range(2):

            @pl.when(arrives(way, t))
            def _():
                y_arrival(way, t, g, j).wait_recv()
                d_copy(1, way, t, g, j, c).start()

    def on(n, act):
        if isinstance(n, int):
            g = max(i for i in range(3) if marks[i] <= n)
            act(g, n - marks[g])
            return
        for g in range(3):

            @pl.when((n >= marks[g]) & (n < marks[g + 1]))
            def _():
                act(g, n - marks[g])

    state = [0, 0]

    def advance(goal):
        while state[0] < goal:
            on(state[0], z_event)
            state[0] += 1
            while state[1] < state[0] - LATE:
                on(state[1], y_event)
                state[1] += 1

    def settle(g):
        advance(marks[g + 1])
        while state[1] < marks[g + 1]:
            on(state[1], y_event)
            state[1] += 1
        own_d(g, 1 - c).wait_recv()

        def arrived(m, carry):
            t, j = m // counts[g] + 1, m % counts[g]
            for way in range(2):

                @pl.when(arrives(way, t))
                def _():
                    d_copy(0, way, t, g, j, 1 - c).wait_recv()
                    d_copy(1, way, t, g, j, 1 - c).wait_recv()

            return carry

        lax.fori_loop(0, marks[g + 1] - marks[g], arrived, 0)

    for k in order:
        tok_local(k).start()
    for g in range(3):
        for copy in own_local(g):
            copy.start()

    barrier = pltpu.get_barrier_semaphore()
    for device in (to_y, to_core, to_x):
        pl.semaphore_signal(barrier, inc=1, device_id=device, device_id_type=pl.DeviceIdType.MESH)
    for way in range(2):

        @pl.when(has_next[way])
        def _():
            pl.semaphore_signal(
                barrier, inc=1, device_id=to_z[way], device_id_type=pl.DeviceIdType.MESH
            )

    @pl.when(has_side)
    def _():
        pl.semaphore_signal(
            barrier, inc=1, device_id={"sp": side}, device_id_type=pl.DeviceIdType.MESH
        )

    docs = doc_ref[...].astype(f32)
    doc_row[:, WINDOW : WINDOW + rows] = jnp.broadcast_to(docs, (doc_row.shape[0], rows))

    @pl.when(sp == 0)
    def _():
        doc_row[:, :WINDOW] = jnp.full((doc_row.shape[0], WINDOW), -1.0, f32)
        pair_ext[:WINDOW, :] = jnp.zeros((WINDOW, pair_ext.shape[1]), bf16)

    @pl.when(sp == last)
    def _():
        doc_row[:, WINDOW + rows :] = jnp.full((doc_row.shape[0], WINDOW), -1.0, f32)
        pair_ext[WINDOW + rows :, :] = jnp.zeros((WINDOW, pair_ext.shape[1]), bf16)

    neighbours = jnp.where(has_side, 1, 0) + jnp.where(z > 0, 1, 0) + jnp.where(z < lines - 1, 1, 0) + 3
    with jax.named_scope("barrier"):
        pl.semaphore_wait(barrier, neighbours)

    for k in order:
        tok_local(k).wait()
        x_copy(k).start()
    start_own(0)
    for way in range(2):
        start_halo(0, way)

    for i in range(blocks):
        at = slice(i * WINDOW, (i + 1) * WINDOW)
        doc_col[at, :] = jnp.broadcast_to(docs[:, at], (WINDOW, LANES)).T

    tile = 32
    lane = lax.broadcasted_iota(jnp.int32, (tile, LANES), 1)
    step = lax.broadcasted_iota(jnp.int32, (tile, LANES), 0)
    freq = freq_ref[...]
    far = (sp * rows + step * tile).astype(f32) * freq
    near_angle = step.astype(f32) * freq
    turn_ref[0:tile, :] = jnp.cos(far)
    turn_ref[tile : 2 * tile, :] = jnp.sin(far)
    near_cos, near_sin = jnp.cos(near_angle), jnp.sin(near_angle)
    sign = jnp.where((lane % HEAD_DIM) < HEAD_DIM // 2, -1.0, 1.0)

    def table_body(i, carry):
        at = pl.ds(pl.multiple_of(i * tile, tile), tile)
        far_cos, far_sin = turn_ref[pl.ds(i, 1), :], turn_ref[pl.ds(tile + i, 1), :]
        cos_ref[at, :] = far_cos * near_cos - far_sin * near_sin
        sin_ref[at, :] = sign * (far_sin * near_cos + far_cos * near_sin)
        return carry

    lax.fori_loop(0, rows // tile, table_body, 0)

    mine_at = pl.multiple_of(x * part, part)
    yours_at = pl.multiple_of((1 - x) * part, part)

    def scale(k):
        x_copy(k).wait_recv()

        def body(i, carry):
            at = pl.ds(pl.multiple_of(k * CHUNK + i * tile, tile), tile)
            own = tok_own[at, :].astype(f32)
            other = tok_other[at, :].astype(f32)
            total = jnp.sum(own * own, axis=1, keepdims=True) + jnp.sum(
                other * other, axis=1, keepdims=True
            )
            inv_ref[at, :] = jnp.broadcast_to(
                lax.rsqrt(total / (2 * part) + EPS), (tile, inv_ref.shape[1])
            )
            scaled[at, pl.ds(mine_at, part)] = (own * gain_ref[:, pl.ds(mine_at, part)]).astype(bf16)
            scaled[at, pl.ds(yours_at, part)] = (
                other * gain_ref[:, pl.ds(yours_at, part)]
            ).astype(bf16)
            return carry

        lax.fori_loop(0, CHUNK // tile, body, 0)

    cut = 256

    def project(k, begin, end):
        mine = slice(k * CHUNK, (k + 1) * CHUNK)

        def body(j, carry):
            at = pl.ds(pl.multiple_of(j * cut, cut), cut)
            acc = jnp.dot(scaled[mine, :], wp_full[:, at], preferred_element_type=f32)
            proj_ref[mine, at] = acc * inv_ref[mine, :1]
            return carry

        lax.fori_loop(begin // cut, end // cut, body, 0)

    lane_c = lax.broadcasted_iota(jnp.int32, (CHUNK, LANES), 1)
    low = (lane_c % HEAD_DIM) < HEAD_DIM // 2

    def block(at, j):
        return pl.ds(pl.multiple_of(at + j * LANES, LANES), LANES)

    def project_att(k):
        mine = slice(k * CHUNK, (k + 1) * CHUNK)
        ext = slice(WINDOW + k * CHUNK, WINDOW + (k + 1) * CHUNK)
        project(k, k_at, width)

        def turned(cells):
            ahead = pltpu.roll(cells, LANES - HEAD_DIM // 2, 1)
            behind = pltpu.roll(cells, HEAD_DIM // 2, 1)
            return cells * cos_ref[mine, :] + jnp.where(low, ahead, behind) * sin_ref[mine, :]

        pair_ext[ext, :k_width] = turned(proj_ref[mine, k_at : k_at + k_width]).astype(bf16)
        pair_ext[ext, k_width:] = proj_ref[mine, k_at + k_width : q_at].astype(bf16)

        def query_body(j, carry):
            cells = turned(proj_ref[mine, block(q_at, j)])
            query_s[mine, block(0, j)] = (cells * HEAD_DIM ** (-0.5)).astype(bf16)
            return carry

        lax.fori_loop(0, q_width // LANES, query_body, 0)

    kv_heads = k_width // HEAD_DIM
    groups = q_width // HEAD_DIM // kv_heads
    span = 3 * WINDOW
    gap = lax.broadcasted_iota(jnp.int32, (WINDOW, span), 1) - lax.broadcasted_iota(
        jnp.int32, (WINDOW, span), 0
    )
    window = (gap >= 0) & (gap <= 2 * WINDOW)

    def attend(i):
        at = pl.ds(pl.multiple_of(i * WINDOW, WINDOW), WINDOW)
        near = pl.ds(pl.multiple_of(i * WINDOW, WINDOW), span)
        allowed = window & (doc_col[at, 0:1] == doc_row[0:1, near])
        bias = jnp.where(allowed, 0.0, -jnp.inf)
        bias = jnp.concatenate([bias] * groups, axis=0)
        queries = query_s[at, :]
        pairs = pair_ext[near, :]
        for head in range(kv_heads):
            keys = pairs[:, head * HEAD_DIM : (head + 1) * HEAD_DIM]
            values = pairs[:, k_width + head * HEAD_DIM : k_width + (head + 1) * HEAD_DIM]
            first = head * groups
            stack = jnp.concatenate(
                [
                    queries[:, (first + g) * HEAD_DIM : (first + g + 1) * HEAD_DIM]
                    for g in range(groups)
                ],
                axis=0,
            )
            sinks = jnp.concatenate(
                [jnp.full((WINDOW, 1), sink_ref[first + g], f32) for g in range(groups)], axis=0
            )
            scores = lax.dot_general(
                stack, keys, (((1,), (1,)), ((), ())), preferred_element_type=f32
            )
            scores = scores + bias
            top = jnp.maximum(jnp.max(scores, axis=1, keepdims=True), sinks)
            expo = jnp.exp(scores - top)
            total = jnp.sum(expo, axis=1, keepdims=True) + jnp.exp(sinks - top)
            weight = (expo * (1.0 / total)).astype(bf16)
            result = jnp.dot(weight, values, preferred_element_type=f32).astype(bf16)
            wide = jnp.concatenate(
                [result[g * WINDOW : (g + 1) * WINDOW] for g in range(groups)], axis=1
            )
            attended[at, first * HEAD_DIM : (first + groups) * HEAD_DIM] = wide

    def attend_all(count, pick):
        begin, lag = state[0], state[1]

        def body(j, carry):
            with jax.named_scope("attend"):
                attend(pick(j))
            with jax.named_scope("att_ev"):
                on(begin + j, z_event)
                on(lag + j, y_event)
                att_copy(pick(j)).start()
            return carry

        lax.fori_loop(0, count, body, 0)
        state[0] += count
        state[1] += count

    def carry_on(k):
        mine = slice(k * CHUNK, (k + 1) * CHUNK)
        ext = slice(edge + k * CHUNK, edge + (k + 1) * CHUNK)
        project(k, 0, 2 * c_width)

        def body(j, carry):
            carried[ext, block(0, j)] = (
                proj_ref[mine, block(0, j)] * proj_ref[mine, block(c_width, j)]
            ).astype(bf16)
            return carry

        lax.fori_loop(0, c_width // LANES, body, 0)

    row_c = lax.broadcasted_iota(jnp.int32, (CHUNK, LANES), 0)

    def convolve(k):
        begin, end = k * CHUNK, (k + 1) * CHUNK
        mine = slice(begin, end)
        project(k, 2 * c_width, k_at)

        def body(j, carry):
            at = block(0, j)
            docs_here = doc_col[mine, :]
            cells = carried[edge + begin : edge + end, at].astype(f32)
            head = carried[begin : begin + edge, at].astype(f32)
            foot = carried[edge + end : 2 * edge + end, at].astype(f32)
            before = jnp.where(row_c == 0, head[edge - 1 : edge, :], pltpu.roll(cells, 1, 0))
            after = jnp.where(row_c == CHUNK - 1, foot[0:1, :], pltpu.roll(cells, CHUNK - 1, 0))
            doc_before = jnp.where(
                row_c == 0,
                doc_row[0:1, WINDOW + begin - 1 : WINDOW + begin],
                pltpu.roll(docs_here, 1, 0),
            )
            doc_after = jnp.where(
                row_c == CHUNK - 1,
                doc_row[0:1, WINDOW + end : WINDOW + end + 1],
                pltpu.roll(docs_here, CHUNK - 1, 0),
            )
            conv = jnp.where(doc_before == docs_here, before * taps_ref[0:1, at], 0.0)
            conv = conv + cells * taps_ref[1:2, at]
            conv = conv + jnp.where(doc_after == docs_here, after * taps_ref[2:3, at], 0.0)
            convolved[mine, at] = (
                proj_ref[mine, block(2 * c_width, j)] * (conv + bias_ref[:, at])
            ).astype(bf16)
            return carry

        lax.fori_loop(0, c_width // LANES, body, 0)

    with jax.named_scope("adv_a"):
        advance(marks[1] - counts[0] + 1)
        start_own(1)
    with jax.named_scope("scale_0"):
        scale(order[0])
    with jax.named_scope("adv_b"):
        advance(marks[1] + 2)
    with jax.named_scope("settle_0"):
        settle(0)
    with jax.named_scope("att_proj_0"):
        project_att(order[0])
        start_halo(1, 0)
    with jax.named_scope("adv_c"):
        advance(marks[1] + 4)
    with jax.named_scope("scale_1"):
        scale(order[1])
    with jax.named_scope("att_proj_1"):
        project_att(order[1])
        start_halo(1, 1)
    with jax.named_scope("adv_d"):
        advance(marks[1] + 5)
        wait_halo(0)
        wait_halo(1)
    attend_all(2, lambda j: j * (blocks - 1))
    with jax.named_scope("adv_e"):
        advance(marks[2] - counts[1] + 1)
        start_own(2)
    for k in order[2:]:
        with jax.named_scope("scale_2"):
            scale(k)
        with jax.named_scope("att_proj_2"):
            project_att(k)
    with jax.named_scope("adv_f"):
        advance(marks[2] - 2)
    attend_all(blocks - 2, lambda j: j + 1)
    with jax.named_scope("settle_1"):
        settle(1)
    with jax.named_scope("carry_0"):
        carry_on(order[0])
    with jax.named_scope("carry_1"):
        carry_on(order[1])
        start_halo(2, 0)
        start_halo(2, 1)
    with jax.named_scope("adv_g"):
        advance(marks[2] + 3)
    for k in order[2:]:
        with jax.named_scope("carry_2"):
            carry_on(k)
    with jax.named_scope("adv_h"):
        advance(marks[2] + 4)
        wait_halo(2)
    for n, k in enumerate(order):
        with jax.named_scope("convolve"):
            convolve(k)
            conv_copy(k).start()
        with jax.named_scope("adv_i"):
            advance(min(marks[3], marks[2] + 5 + n))
    with jax.named_scope("settle_2"):
        settle(2)

    with jax.named_scope("att_wait"):
        for i in range(blocks):
            att_copy(i).wait_recv()
    q_mine = pl.ds(pl.multiple_of(x * q_width, q_width), q_width)
    q_yours = pl.ds(pl.multiple_of((1 - x) * q_width, q_width), q_width)
    c_mine = pl.ds(pl.multiple_of(x * c_width, c_width), c_width)
    c_yours = pl.ds(pl.multiple_of((1 - x) * c_width, c_width), c_width)

    def mix_body(j, carry):
        at = pl.ds(pl.multiple_of(j * cut, cut), cut)
        late = pl.ds(pl.multiple_of(part + j * cut, cut), cut)
        acc = jnp.dot(attended[...], wo_full[q_mine, at], preferred_element_type=f32)
        acc = acc + jnp.dot(att_other[...], wo_full[q_yours, at], preferred_element_type=f32)
        acc = acc + jnp.dot(convolved[...], wo_full[c_mine, late], preferred_element_type=f32)
        acc_ref[:, at] = acc
        return carry

    with jax.named_scope("mix"):
        lax.fori_loop(0, part // cut, mix_body, 0)

    with jax.named_scope("sends"):
        for kind in range(3):
            for way in range(2):

                @pl.when(sends_to[way])
                def _():
                    halo(kind, way).wait_send()

        for i in range(blocks):
            att_copy(i).wait_send()
        for k in range(chunks):
            x_copy(k).wait_send()
        for g in range(3):
            own_d(g, c).wait_send()

            def sent(m, carry):
                t, j = m // counts[g], m % counts[g]
                for way in range(2):

                    @pl.when(has_next[way] & (t < lines - 1) & arrives(way, t))
                    def _():
                        z_copy(way, t, g, j).wait_send()

                    @pl.when((t > 0) & arrives(way, t))
                    def _():
                        y_copy(way, t, g, j).wait_send()
                        d_copy(0, way, t, g, j, c).wait_send()
                        d_copy(1, way, t, g, j, c).wait_send()

                return carry

            lax.fori_loop(0, lines * counts[g], sent, 0)

    def out_copy(k):
        at = slice(k * CHUNK, (k + 1) * CHUNK)
        return pltpu.make_async_copy(stage.at[at, :], out_ref.at[at, :], out_sem.at[k])

    for k in order:
        mine = slice(k * CHUNK, (k + 1) * CHUNK)
        with jax.named_scope("conv_wait"):
            conv_copy(k).wait_recv()

        def last_body(j, carry):
            at = pl.ds(pl.multiple_of(j * cut, cut), cut)
            late = pl.ds(pl.multiple_of(part + j * cut, cut), cut)
            acc = acc_ref[mine, at] + jnp.dot(
                conv_other[mine, :], wo_full[c_yours, late], preferred_element_type=f32
            )
            stage[mine, at] = acc.astype(bf16)
            return carry

        with jax.named_scope("last"):
            lax.fori_loop(0, part // cut, last_body, 0)
            out_copy(k).start()

    with jax.named_scope("end"):
        for k in range(chunks):
            conv_copy(k).wait_send()
        for k in range(chunks):
            out_copy(k).wait()


def fused_layer(
    tokens, gain, projections, outputs, sink_logit, taps, conv_bias, documents, sp_count
):
    rows, part = tokens.shape
    f32 = jnp.float32
    bf16 = jnp.bfloat16
    lines = sp_count // 2
    wk, wv, wc, wu, wb, wq = projections
    width = sum(w.shape[1] for w in projections)
    rp, ro = wq.shape[0], outputs[0].shape[0]
    q_width, k_width, c_width = wq.shape[1], wk.shape[1], wc.shape[1]
    half = HEAD_DIM // 2
    freq = np.power(THETA, -(np.arange(half) / half))
    freq = jnp.asarray(np.tile(freq, LANES // half)[None, :], f32)
    chunks, blocks = rows // CHUNK, rows // WINDOW
    dma = pltpu.SemaphoreType.DMA
    hops = (2, lines - 1, CONV_UNITS + ATT_UNITS + OUT_UNITS)
    vmem = pl.BlockSpec(memory_space=pltpu.VMEM)
    hbm = pl.BlockSpec(memory_space=pl.ANY)
    smem = pl.BlockSpec(memory_space=pltpu.SMEM)
    flops = 2 * rows * 2 * part * width
    return pl.pallas_call(
        functools.partial(layer_kernel, (lines, rp, ro)),
        out_shape=jax.ShapeDtypeStruct((rows, part), bf16),
        in_specs=[hbm, vmem] + [hbm] * 8 + [smem] + [vmem] * 4,
        out_specs=hbm,
        scratch_shapes=[
            pltpu.VMEM((rp * sp_count, width), bf16),
            pltpu.VMEM((ro * sp_count, 2 * part), bf16),
            pltpu.VMEM((rows, part), bf16),
            pltpu.VMEM((rows, part), bf16),
            pltpu.VMEM((rows, 2 * part), bf16),
            pltpu.VMEM((rows, LANES), f32),
            pltpu.VMEM((rows, width), f32),
            pltpu.VMEM((rows, part), f32),
            pltpu.VMEM((rows, part), bf16),
            pltpu.VMEM((rows + 2 * WINDOW, 2 * k_width), bf16),
            pltpu.VMEM((rows, q_width), bf16),
            pltpu.VMEM((rows + 32, c_width), bf16),
            pltpu.VMEM((8, rows + 2 * WINDOW), f32),
            pltpu.VMEM((rows, LANES), f32),
            pltpu.VMEM((64, LANES), f32),
            pltpu.VMEM((rows, LANES), f32),
            pltpu.VMEM((rows, LANES), f32),
            pltpu.VMEM((rows, c_width), bf16),
            pltpu.VMEM((rows, c_width), bf16),
            pltpu.VMEM((rows, q_width), bf16),
            pltpu.VMEM((rows, q_width), bf16),
        ]
        + [dma(hops)] * 8
        + [dma((3,)), dma((3,)), dma((chunks,)), dma((chunks,)), dma((9,)), dma((chunks,))]
        + [dma((chunks,)), dma((3, 2)), dma((3, 2)), dma((chunks,)), dma((chunks,))]
        + [dma((blocks,)), dma((blocks,))],
        compiler_params=pltpu.CompilerParams(
            collective_id=0, has_side_effects=True, vmem_limit_bytes=62 * 1024 * 1024
        ),
        cost_estimate=pl.CostEstimate(flops=flops, bytes_accessed=0, transcendentals=0),
        name="layer",
    )(
        tokens,
        gain[None, :],
        *projections,
        *outputs,
        sink_logit,
        taps,
        conv_bias[None, :],
        documents[None, :],
        freq,
    )


def extended(cells, sides, width):
    for axis, dim in sides:
        count = lax.axis_size(axis)
        ends = count - 1
        head = lax.slice_in_dim(cells, 0, width, axis=dim)
        tail = lax.slice_in_dim(cells, cells.shape[dim] - width, cells.shape[dim], axis=dim)
        cells = jnp.concatenate(
            [
                lax.ppermute(tail, axis, [(i, (i + 1) % count) for i in range(ends)]),
                cells,
                lax.ppermute(head, axis, [((i + 1) % count, i) for i in range(ends)]),
            ],
            axis=dim,
        )
    return cells


def rotate(proj, positions, heads):
    rows = proj.shape[0]
    size = proj.shape[1] // heads
    half = size // 2
    freq = jnp.power(THETA, -(jnp.arange(half, dtype=jnp.float32) * (2.0 / size)))
    angle = positions.astype(jnp.float32)[:, None] * freq[None, :]
    cosine = jnp.cos(angle)[:, None, :]
    sine = jnp.sin(angle)[:, None, :]
    shaped = proj.reshape(rows, heads, size)
    first = shaped[..., :half]
    second = shaped[..., half:]
    turned = jnp.concatenate(
        [first * cosine - second * sine, second * cosine + first * sine], axis=-1
    )
    return turned.reshape(rows, heads * size)


def sink_softmax(scores, allowed, sinks):
    masked = jnp.where(allowed, scores, -jnp.inf)
    top = jnp.maximum(jnp.max(masked, axis=-1, keepdims=True), sinks)
    expo = jnp.exp(masked - top)
    return expo / (jnp.sum(expo, axis=-1, keepdims=True) + jnp.exp(sinks - top))


def local(
    tokens,
    gain,
    w_query,
    w_key,
    w_value,
    w_input,
    w_bgate,
    w_cgate,
    w_attn_out,
    w_conv_out,
    sink_logit,
    taps,
    conv_bias,
    documents,
):
    f32 = jnp.float32
    bf16 = jnp.bfloat16
    rows, part = tokens.shape
    tp_count = lax.axis_size("tp")
    sp_count = lax.axis_size("sp")
    width = part * tp_count
    head_dim = HEAD_DIM
    q_local = w_query.shape[1] // head_dim
    kv_local = w_key.shape[1] // head_dim
    groups = q_local // kv_local
    if fused_plan(
        lax.axis_size("grp"),
        sp_count,
        tp_count,
        rows,
        part,
        w_query.shape[0],
        w_attn_out.shape[0],
        w_query.shape[1],
        w_key.shape[1],
        w_input.shape[1],
    ):
        return fused_layer(
            tokens,
            gain,
            (w_key, w_value, w_cgate, w_input, w_bgate, w_query),
            (w_attn_out, w_conv_out),
            sink_logit,
            taps,
            conv_bias,
            documents,
            sp_count,
        )
    wq, wk, wv, wu, wb, wc, w_attn, w_conv = (
        lax.all_gather(w_query, "sp", axis=0, tiled=True),
        lax.all_gather(w_key, "sp", axis=0, tiled=True),
        lax.all_gather(w_value, "sp", axis=0, tiled=True),
        lax.all_gather(w_input, "sp", axis=0, tiled=True),
        lax.all_gather(w_bgate, "sp", axis=0, tiled=True),
        lax.all_gather(w_cgate, "sp", axis=0, tiled=True),
        lax.all_gather(w_attn_out, "sp", axis=0, tiled=True),
        lax.all_gather(w_conv_out, "sp", axis=0, tiled=True),
    )
    matrices = (wq, wk, wv, wu, wb, wc)
    piece_f = lax.all_gather(tokens, "tp", axis=1, tiled=True).astype(f32)
    scaled = (piece_f * gain[None, :]).astype(bf16)
    products = tuple((jnp.dot(scaled, mat, preferred_element_type=f32) for mat in matrices))
    folded = products + (jnp.sum(piece_f * piece_f, axis=1),)
    sums = folded[:6]
    squares = folded[6]
    inv = lax.rsqrt(squares / width + EPS)[:, None]
    q_acc, k_acc, v_acc, u_acc, b_acc, c_acc = sums
    positions = lax.axis_index("sp") * rows + jnp.arange(rows, dtype=jnp.int32)
    query = rotate(q_acc * inv, positions, q_local).astype(bf16)
    keys = rotate(k_acc * inv, positions, kv_local).astype(bf16)
    values = (v_acc * inv).astype(bf16)
    carried = (c_acc * inv * (u_acc * inv)).astype(bf16)
    bgate = b_acc * inv
    doc_col = documents.astype(f32).astype(bf16)[:, None]
    paired = jnp.concatenate([keys, values], axis=1)
    pair_ext, doc_ext = (
        extended(paired, (("sp", 0),), WINDOW),
        extended(doc_col, (("sp", 0),), WINDOW),
    )
    carry_ext, doc_near = (extended(carried, (("sp", 0),), 1), extended(doc_col, (("sp", 0),), 1))
    key_width = kv_local * head_dim
    key_ext = pair_ext[:, :key_width].reshape(-1, kv_local, head_dim)
    val_ext = pair_ext[:, key_width:].reshape(-1, kv_local, head_dim)
    key_doc = doc_ext[:, 0].astype(f32)
    own_doc = doc_col[:, 0].astype(f32)
    key_pos = positions[0] - WINDOW + jnp.arange(rows + 2 * WINDOW, dtype=jnp.int32)
    total = sp_count * rows
    sinks = sink_logit.reshape(kv_local, groups, 1, 1)
    block = rows // 2
    outputs = []
    for begin in range(0, rows, block):
        span = block + 2 * WINDOW
        q_block = query[begin : begin + block].reshape(block, kv_local, groups, head_dim)
        k_block = key_ext[begin : begin + span]
        v_block = val_ext[begin : begin + span]
        q_pos = positions[begin : begin + block]
        k_pos = key_pos[begin : begin + span]
        scores = jnp.einsum(
            "qhgd,khd->hgqk", q_block, k_block, preferred_element_type=f32
        ) * head_dim ** (-0.5)
        allowed = jnp.abs(q_pos[:, None] - k_pos[None, :]) <= WINDOW
        allowed = allowed & (
            own_doc[begin : begin + block, None] == key_doc[None, begin : begin + span]
        )
        allowed = allowed & (k_pos >= 0)[None, :] & (k_pos < total)[None, :]
        weight = sink_softmax(scores, allowed, sinks).astype(bf16)
        result = jnp.einsum("hgqk,khd->qhgd", weight, v_block, preferred_element_type=f32)
        outputs.append(result.astype(bf16).reshape(block, q_local * head_dim))
    attended = jnp.concatenate(outputs, axis=0)
    near_doc = doc_near[:, 0].astype(f32)
    conv = jnp.zeros((rows, carried.shape[1]), f32)
    for tap in range(3):
        same = (near_doc[tap : tap + rows] == near_doc[1 : rows + 1])[:, None]
        conv = conv + jnp.where(
            same, carry_ext[tap : tap + rows].astype(f32) * taps[tap][None, :], 0.0
        )
    convolved = (bgate * (conv + conv_bias[None, :])).astype(bf16)
    acc = jnp.dot(
        lax.all_gather(attended, "tp", axis=1, tiled=True), w_attn, preferred_element_type=f32
    )
    mixed = acc + jnp.dot(
        lax.all_gather(convolved, "tp", axis=1, tiled=True), w_conv, preferred_element_type=f32
    )
    return mixed.astype(bf16)


def solution(mesh):
    placed = (
        P(("grp", "sp"), "tp"),
        P(),
        P("sp", "tp"),
        P("sp", "tp"),
        P("sp", "tp"),
        P("sp", "tp"),
        P("sp", "tp"),
        P("sp", "tp"),
        P("sp", "tp"),
        P("sp", "tp"),
        P("tp"),
        P(None, "tp"),
        P("tp"),
        P(("grp", "sp")),
    )
    return jax.shard_map(
        local, mesh=mesh, in_specs=placed, out_specs=P(("grp", "sp"), "tp"), check_vma=False
    )
```

```python
import functools

import jax
import jax.numpy as jnp
import numpy as np
from jax import lax
from jax.experimental import pallas as pl
from jax.experimental.pallas import tpu as pltpu
from jax.sharding import PartitionSpec as P

HEAD_DIM = 64
WINDOW = 128


EPS = 1e-06
THETA = 500000.0
UNITS = (4, 4, 4)
LATES = (6, 3, 4)
CHUNK = 256
LANES = 128


def fused_plan(grp_count, sp_count, tp_count, rows, part, proj_rows, out_rows, q_width, k_width, c_width):
    lines = sp_count // 2
    return (
        grp_count == 2
        and tp_count == 2
        and sp_count % 2 == 0
        and lines == 4
        and all(proj_rows % (2 * units * 16) == 0 for units in UNITS[:2])
        and all(out_rows % (2 * units * 16) == 0 for units in UNITS[2:])
        and rows % CHUNK == 0
        and 3 * CHUNK <= rows <= 1024
        and CHUNK == 2 * WINDOW
        and WINDOW == LANES
        and part % 512 == 0
        and q_width == 4 * k_width
        and k_width == LANES
        and c_width % 256 == 0
        and 2 * HEAD_DIM == LANES
    )


def layer_kernel(
    sizes,
    tok_hbm,
    gain_ref,
    wk_ref,
    wv_ref,
    wc_ref,
    wu_ref,
    wb_ref,
    wq_ref,
    wa_ref,
    wm_ref,
    sink_ref,
    taps_ref,
    bias_ref,
    doc_ref,
    freq_ref,
    out_ref,
    wp_full,
    wo_full,
    tok_own,
    tok_other,
    scaled,
    inv_ref,
    acc_ref,
    stage,
    pair_ext,
    query_s,
    carried,
    doc_row,
    doc_col,
    turn_ref,
    cos_ref,
    sin_ref,
    convolved,
    conv_other,
    attended,
    att_other,
    z_send,
    z_recv,
    y_send,
    y_recv,
    d_send,
    d_recv,
    x_send,
    x_recv,
    own_sem,
    tok_sem,
    out_sem,
    halo_send,
    halo_recv,
    conv_send,
    conv_recv,
    att_send,
    att_recv,
):
    lines, rp, ro = sizes
    f32 = jnp.float32
    bf16 = jnp.bfloat16
    rows, part = tok_own.shape
    k_width, c_width, q_width = wk_ref.shape[1], wc_ref.shape[1], wq_ref.shape[1]
    k_at = 3 * c_width
    q_at = k_at + 2 * k_width
    width = q_at + q_width
    chunks = rows // CHUNK
    blocks = rows // WINDOW
    order = (chunks - 1,) + tuple(range(chunks - 1))
    y = lax.axis_index("grp")
    sp = lax.axis_index("sp")
    x = lax.axis_index("tp")
    z, c = sp // 2, sp % 2
    counts = UNITS
    kinds = range(len(counts))
    fulls = (wp_full, wp_full, wo_full)
    heights = (rp, rp, ro)
    spans = ((k_at, width), (0, k_at), (0, 2 * part))
    first_unit, marks = [0], [0]
    for count in counts:
        first_unit.append(first_unit[-1] + count)
        marks.append(marks[-1] + (lines - 1) * count)
    to_y = {"grp": 1 - y}
    to_core = {"sp": z * 2 + 1 - c}
    to_x = {"tp": 1 - x}
    to_z = ({"sp": sp + 2}, {"sp": sp - 2})
    has_next = (z < lines - 1, z > 0)

    def origin(way, t):
        return z - t if way == 0 else z + t

    def arrives(way, t):
        return z >= t if way == 0 else z < lines - t

    def place(g, j, zo, cc, h):
        size = heights[g]
        tall = size // 2 // counts[g]
        row = (zo * 2 + cc) * size + h * (size // 2) + j * tall
        return fulls[g].at[pl.ds(pl.multiple_of(row, tall), tall), spans[g][0] : spans[g][1]]

    def remote(src, dst, send, recv, device):
        return pltpu.make_async_remote_copy(
            src_ref=src, dst_ref=dst, send_sem=send, recv_sem=recv,
            device_id=device, device_id_type=pl.DeviceIdType.MESH,
        )

    def z_copy(way, t, g, j):
        zo = origin(way, t)
        ref, u = place(g, j, zo, c, y), first_unit[g] + j
        return remote(ref, ref, z_send.at[way, g], z_recv.at[zo - way, u], to_z[way])

    def y_copy(way, t, g, j, h):
        zo = origin(way, t)
        ref, u = place(g, j, zo, c, h), first_unit[g] + j
        return remote(ref, ref, y_send.at[g], y_recv.at[zo - way, u], to_y)

    def d_copy(way, t, g, j, h):
        ref = place(g, j, origin(way, t), c, h)
        return remote(ref, ref, d_send.at[g], d_recv.at[g], to_core)

    def some_rows(g, count):
        return fulls[g].at[0:count, spans[g][0] : spans[g][1]]

    def d_all(g, shards):
        ref = some_rows(g, shards * heights[g])
        return remote(ref, ref, d_send.at[g], d_recv.at[g], to_core)

    def own_ref(g):
        at = pl.ds(pl.multiple_of((z * 2 + c) * heights[g], heights[g]), heights[g])
        return fulls[g].at[at, spans[g][0] : spans[g][1]]

    def own_d(g):
        return remote(own_ref(g), own_ref(g), d_send.at[g], d_recv.at[g], to_core)

    own_refs = ((wk_ref, wv_ref, wq_ref), (wc_ref, wu_ref, wb_ref), (wa_ref, wm_ref))

    def own_local(g):
        at, copies, col = pl.ds(pl.multiple_of((z * 2 + c) * heights[g], heights[g]), heights[g]), [], spans[g][0]
        for ref in own_refs[g]:
            size = ref.shape[1]
            copies.append(
                pltpu.make_async_copy(ref, fulls[g].at[at, col : col + size], own_sem.at[g])
            )
            col += size
        return copies

    def tok_local(k):
        at = slice(k * CHUNK, (k + 1) * CHUNK)
        return pltpu.make_async_copy(tok_hbm.at[at, :], tok_own.at[at, :], tok_sem.at[k])

    def x_copy(k):
        at = slice(k * CHUNK, (k + 1) * CHUNK)
        return remote(tok_own.at[at, :], tok_other.at[at, :], x_send.at[0], x_recv.at[k], to_x)

    last = 2 * lines - 1
    steps_sp = (sp + 1, sp - 1)
    sends_to = (sp < last, sp > 0)
    gets_from = (sp > 0, sp < last)
    side = jnp.where(c == 0, sp - 1, sp + 1)
    has_side = (side >= 0) & (side <= last)
    edge = 16

    def halo(kind, way):
        if kind == 0:
            at = rows if way == 0 else WINDOW
            src = doc_row.at[:, at : at + WINDOW]
            at = 0 if way == 0 else WINDOW + rows
            dst = doc_row.at[:, at : at + WINDOW]
        elif kind == 1:
            at = rows if way == 0 else WINDOW
            src = pair_ext.at[at : at + WINDOW, :]
            at = 0 if way == 0 else WINDOW + rows
            dst = pair_ext.at[at : at + WINDOW, :]
        else:
            at = rows if way == 0 else edge
            src = carried.at[at : at + edge, :]
            at = 0 if way == 0 else edge + rows
            dst = carried.at[at : at + edge, :]
        return remote(
            src, dst, halo_send.at[kind, way], halo_recv.at[kind, way], {"sp": steps_sp[way]}
        )

    def start_halo(kind, way):
        @pl.when(sends_to[way])
        def _():
            halo(kind, way).start()

    def wait_halo(kind):
        for way in range(2):

            @pl.when(gets_from[way])
            def _():
                halo(kind, way).wait_recv()

    def conv_copy(k):
        at = slice(k * CHUNK, (k + 1) * CHUNK)
        return remote(
            convolved.at[at, :], conv_other.at[at, :], conv_send.at[0], conv_recv.at[k], to_x
        )

    def att_copy(i):
        at = pl.ds(pl.multiple_of(i * WINDOW, WINDOW), WINDOW)
        return remote(attended.at[at, :], att_other.at[at, :], att_send.at[0], att_recv.at[i], to_x)

    def start_own(g):
        pltpu.make_async_copy(own_ref(g), own_ref(g), own_sem.at[g]).wait()
        for j in range(counts[g]):
            for way in range(2):

                @pl.when(has_next[way])
                def _():
                    z_copy(way, 0, g, j).start()

        own_d(g).start()

    def z_event(g, m):
        t, j = m // counts[g] + 1, m % counts[g]
        for way in range(2):

            @pl.when(arrives(way, t))
            def _():
                z_copy(way, t, g, j).wait_recv()

                @pl.when(has_next[way] & (t < lines - 1))
                def _():
                    z_copy(way, t, g, j).start()

                y_copy(way, t, g, j, y).start()
                d_copy(way, t, g, j, y).start()

    def y_event(g, m):
        t, j = m // counts[g] + 1, m % counts[g]
        for way in range(2):

            @pl.when(arrives(way, t))
            def _():
                y_copy(way, t, g, j, 1 - y).wait_recv()
                d_copy(way, t, g, j, 1 - y).start()

    def on(n, act):
        if isinstance(n, int):
            g = max(i for i in kinds if marks[i] <= n)
            act(g, n - marks[g])
            return
        for g in kinds:

            @pl.when((n >= marks[g]) & (n < marks[g + 1]))
            def _():
                act(g, n - marks[g])

    state = [0, 0]

    def due(m):
        if m >= marks[-1]:
            return m
        return m + LATES[max(i for i in kinds if marks[i] <= m)]

    def advance(goal):
        while state[0] < goal:
            on(state[0], z_event)
            state[0] += 1
            while due(state[1]) < state[0]:
                on(state[1], y_event)
                state[1] += 1

    def settle(g):
        advance(marks[g + 1])
        while state[1] < marks[g + 1]:
            on(state[1], y_event)
            state[1] += 1
        d_all(g, lines).wait_recv()

    for k in order:
        tok_local(k).start()
    for g in kinds:
        for copy in own_local(g):
            copy.start()

    barrier = pltpu.get_barrier_semaphore()
    for device in (to_y, to_core, to_x):
        pl.semaphore_signal(barrier, inc=1, device_id=device, device_id_type=pl.DeviceIdType.MESH)
    for way in range(2):

        @pl.when(has_next[way])
        def _():
            pl.semaphore_signal(
                barrier, inc=1, device_id=to_z[way], device_id_type=pl.DeviceIdType.MESH
            )

    @pl.when(has_side)
    def _():
        pl.semaphore_signal(
            barrier, inc=1, device_id={"sp": side}, device_id_type=pl.DeviceIdType.MESH
        )

    docs = doc_ref[...].astype(f32)
    for i in range(blocks):
        doc_row[:, (i + 1) * WINDOW : (i + 2) * WINDOW] = jnp.broadcast_to(
            docs[i : i + 1, :], (doc_row.shape[0], LANES)
        )

    @pl.when(sp == 0)
    def _():
        doc_row[:, :WINDOW] = jnp.full((doc_row.shape[0], WINDOW), -1.0, f32)
        pair_ext[:WINDOW, :] = jnp.zeros((WINDOW, pair_ext.shape[1]), bf16)

    @pl.when(sp == last)
    def _():
        doc_row[:, WINDOW + rows :] = jnp.full((doc_row.shape[0], WINDOW), -1.0, f32)
        pair_ext[WINDOW + rows :, :] = jnp.zeros((WINDOW, pair_ext.shape[1]), bf16)

    neighbours = jnp.where(has_side, 1, 0) + jnp.where(z > 0, 1, 0) + jnp.where(z < lines - 1, 1, 0) + 3
    with jax.named_scope("barrier"):
        pl.semaphore_wait(barrier, neighbours)

    for k in order:
        tok_local(k).wait()
        x_copy(k).start()
    start_own(0)
    for way in range(2):
        start_halo(0, way)

    for i in range(blocks):
        at = slice(i * WINDOW, (i + 1) * WINDOW)
        doc_col[at, :] = jnp.broadcast_to(docs[i : i + 1, :], (WINDOW, LANES)).T

    tile = 32
    lane = lax.broadcasted_iota(jnp.int32, (tile, LANES), 1)
    step = lax.broadcasted_iota(jnp.int32, (tile, LANES), 0)
    freq = freq_ref[...]
    far = (sp * rows + step * tile).astype(f32) * freq
    near_angle = step.astype(f32) * freq
    turn_ref[0:tile, :] = jnp.cos(far)
    turn_ref[tile : 2 * tile, :] = jnp.sin(far)
    near_cos, near_sin = jnp.cos(near_angle), jnp.sin(near_angle)
    sign = jnp.where((lane % HEAD_DIM) < HEAD_DIM // 2, -1.0, 1.0)

    def table_body(i, carry):
        at = pl.ds(pl.multiple_of(i * tile, tile), tile)
        far_cos, far_sin = turn_ref[pl.ds(i, 1), :], turn_ref[pl.ds(tile + i, 1), :]
        cos_ref[at, :] = far_cos * near_cos - far_sin * near_sin
        sin_ref[at, :] = sign * (far_sin * near_cos + far_cos * near_sin)
        return carry

    lax.fori_loop(0, rows // tile, table_body, 0)

    mine_at = pl.multiple_of(x * part, part)
    yours_at = pl.multiple_of((1 - x) * part, part)

    def scale(k):
        x_copy(k).wait_recv()

        def body(i, carry):
            at = pl.ds(pl.multiple_of(k * CHUNK + i * tile, tile), tile)
            own = tok_own[at, :].astype(f32)
            other = tok_other[at, :].astype(f32)
            total = jnp.sum(own * own, axis=1, keepdims=True) + jnp.sum(
                other * other, axis=1, keepdims=True
            )
            inv_ref[at, :] = jnp.broadcast_to(
                lax.rsqrt(total / (2 * part) + EPS), (tile, inv_ref.shape[1])
            )
            scaled[at, pl.ds(mine_at, part)] = (own * gain_ref[:, pl.ds(mine_at, part)]).astype(bf16)
            scaled[at, pl.ds(yours_at, part)] = (
                other * gain_ref[:, pl.ds(yours_at, part)]
            ).astype(bf16)
            return carry

        lax.fori_loop(0, CHUNK // tile, body, 0)

    cut = 256

    def project(k, at):
        mine = slice(k * CHUNK, (k + 1) * CHUNK)
        acc = jnp.dot(scaled[mine, :], wp_full[:, at], preferred_element_type=f32)
        return acc * inv_ref[mine, :1]

    lane_c = lax.broadcasted_iota(jnp.int32, (CHUNK, LANES), 1)
    low = (lane_c % HEAD_DIM) < HEAD_DIM // 2
    left = lane_c < HEAD_DIM

    def project_att(k):
        mine = slice(k * CHUNK, (k + 1) * CHUNK)
        ext = slice(WINDOW + k * CHUNK, WINDOW + (k + 1) * CHUNK)

        def turned(cells):
            ahead = pltpu.roll(cells, LANES - HEAD_DIM // 2, 1)
            behind = pltpu.roll(cells, HEAD_DIM // 2, 1)
            return cells * cos_ref[mine, :] + jnp.where(low, ahead, behind) * sin_ref[mine, :]

        cells = project(k, slice(k_at, q_at))
        pair_ext[ext, :k_width] = turned(cells[:, :k_width]).astype(bf16)
        pair_ext[ext, k_width:] = cells[:, k_width:].astype(bf16)

        def query_body(j, carry):
            cells = project(k, pl.ds(pl.multiple_of(q_at + j * cut, cut), cut))
            for i in range(cut // LANES):
                pair = turned(cells[:, i * LANES : (i + 1) * LANES]) * HEAD_DIM ** (-0.5)
                swapped = pltpu.roll(pair, HEAD_DIM, 1)
                own_half = left == (j == 0)
                first = jnp.where(own_half, jnp.where(j == 0, pair, swapped), 0.0)
                second = jnp.where(own_half, jnp.where(j == 0, swapped, pair), 0.0)
                at = pl.multiple_of((j * (cut // LANES) + i) * 2 * LANES, LANES)
                query_s[mine, pl.ds(at, LANES)] = first.astype(bf16)
                query_s[mine, pl.ds(at + LANES, LANES)] = second.astype(bf16)
            return carry

        for j in range(q_width // cut):
            query_body(j, 0)

    kv_heads = k_width // HEAD_DIM
    groups = q_width // HEAD_DIM // kv_heads
    span = 3 * WINDOW
    gap = lax.broadcasted_iota(jnp.int32, (WINDOW, span), 1) - lax.broadcasted_iota(
        jnp.int32, (WINDOW, span), 0
    )
    window = (gap >= 0) & (gap <= 2 * WINDOW)
    left_w = left[:WINDOW, :]

    def attend(i):
        at = pl.ds(pl.multiple_of(i * WINDOW, WINDOW), WINDOW)
        near = pl.ds(pl.multiple_of(i * WINDOW, WINDOW), span)
        allowed = window & (doc_col[at, 0:1] == doc_row[0:1, near])
        bias = jnp.where(allowed, 0.0, -jnp.inf)
        bias = jnp.concatenate([bias] * groups, axis=0)
        keys = pair_ext[near, :k_width]
        values = jnp.concatenate(
            [pair_ext[near, k_width:], jnp.ones((span, LANES), bf16)], axis=1
        )
        for head in range(kv_heads):
            first = head * groups
            stack = jnp.concatenate(
                [
                    query_s[at, (first + g) * LANES : (first + g + 1) * LANES]
                    for g in range(groups)
                ],
                axis=0,
            )
            sinks = jnp.concatenate(
                [jnp.full((WINDOW, 1), sink_ref[first + g], f32) for g in range(groups)], axis=0
            )
            scores = lax.dot_general(
                stack, keys, (((1,), (1,)), ((), ())), preferred_element_type=f32
            )
            scores = scores + bias
            top = jnp.maximum(jnp.max(scores, axis=1, keepdims=True), sinks)
            expo = jnp.exp(scores - top).astype(bf16)
            result = jnp.dot(expo, values, preferred_element_type=f32)
            total = result[:, LANES:] + jnp.exp(sinks - top)
            result = result[:, :LANES] * (1.0 / total)
            for g in range(0, groups, 2):
                one = result[g * WINDOW : (g + 1) * WINDOW]
                two = result[(g + 1) * WINDOW : (g + 2) * WINDOW]
                if head == 0:
                    pair = jnp.where(left_w, one, pltpu.roll(two, HEAD_DIM, 1))
                else:
                    pair = jnp.where(left_w, pltpu.roll(one, HEAD_DIM, 1), two)
                to = (first + g) * HEAD_DIM
                attended[at, to : to + LANES] = pair.astype(bf16)

    def attend_all(count, pick):
        begin, lag = state[0], state[1]

        def body(j, carry):
            with jax.named_scope("attend"):
                attend(pick(j))
            with jax.named_scope("att_ev"):
                on(begin + j, z_event)
                on(lag + j, y_event)
                att_copy(pick(j)).start()
            return carry

        lax.fori_loop(0, count, body, 0)
        state[0] += count
        state[1] += count

    def carry_on(k):
        ext = slice(edge + k * CHUNK, edge + (k + 1) * CHUNK)
        for j in range(c_width // cut):
            at = slice(j * cut, (j + 1) * cut)
            gate = project(k, at)
            carried[ext, at] = (
                gate * project(k, slice(c_width + j * cut, c_width + (j + 1) * cut))
            ).astype(bf16)

    row_c = lax.broadcasted_iota(jnp.int32, (CHUNK, LANES), 0)

    def convolve(k):
        begin, end = k * CHUNK, (k + 1) * CHUNK
        mine = slice(begin, end)
        docs_here = doc_col[mine, :]
        doc_before = jnp.where(
            row_c == 0,
            doc_row[0:1, WINDOW + begin - 1 : WINDOW + begin],
            pltpu.roll(docs_here, 1, 0),
        )
        doc_after = jnp.where(
            row_c == CHUNK - 1,
            doc_row[0:1, WINDOW + end : WINDOW + end + 1],
            pltpu.roll(docs_here, CHUNK - 1, 0),
        )
        for j in range(c_width // cut):
            gates = project(k, slice(2 * c_width + j * cut, 2 * c_width + (j + 1) * cut))
            for i in range(cut // LANES):
                at = slice(j * cut + i * LANES, j * cut + (i + 1) * LANES)
                cells = carried[edge + begin : edge + end, at].astype(f32)
                head = carried[begin : begin + edge, at].astype(f32)
                foot = carried[edge + end : 2 * edge + end, at].astype(f32)
                before = jnp.where(row_c == 0, head[edge - 1 : edge, :], pltpu.roll(cells, 1, 0))
                after = jnp.where(row_c == CHUNK - 1, foot[0:1, :], pltpu.roll(cells, CHUNK - 1, 0))
                conv = jnp.where(doc_before == docs_here, before * taps_ref[0:1, at], 0.0)
                conv = conv + cells * taps_ref[1:2, at]
                conv = conv + jnp.where(doc_after == docs_here, after * taps_ref[2:3, at], 0.0)
                gate = gates[:, i * LANES : (i + 1) * LANES]
                convolved[mine, at] = (gate * (conv + bias_ref[:, at])).astype(bf16)

    def ahead_of(g):
        return marks[g + 1] - counts[g] + 1

    q_mine = pl.ds(pl.multiple_of(x * q_width, q_width), q_width)
    q_yours = pl.ds(pl.multiple_of((1 - x) * q_width, q_width), q_width)
    c_mine = pl.ds(pl.multiple_of(x * c_width, c_width), c_width)
    c_yours = pl.ds(pl.multiple_of((1 - x) * c_width, c_width), c_width)

    with jax.named_scope("adv_a"):
        advance(ahead_of(0))
        start_own(1)
        advance(marks[1] - 1)
    with jax.named_scope("scale_0"):
        scale(order[0])
    with jax.named_scope("adv_b"):
        advance(marks[1] + 2)
    with jax.named_scope("settle_0"):
        settle(0)
    with jax.named_scope("att_proj_0"):
        project_att(order[0])
        start_halo(1, 0)
    with jax.named_scope("adv_c"):
        advance(marks[1] + 4)
    with jax.named_scope("scale_1"):
        scale(order[1])
    with jax.named_scope("att_proj_1"):
        project_att(order[1])
        start_halo(1, 1)
    with jax.named_scope("adv_d"):
        advance(marks[1] + 6)
        wait_halo(0)
        wait_halo(1)
    attend_all(2, lambda j: j * (blocks - 1))
    with jax.named_scope("adv_e"):
        advance(ahead_of(1))
        start_own(2)
    for k in order[2:]:
        with jax.named_scope("scale_2"):
            scale(k)
        with jax.named_scope("att_proj_2"):
            project_att(k)
    with jax.named_scope("adv_f"):
        advance(marks[2] - 1)
    attend_all(blocks - 2, lambda j: j + 1)
    with jax.named_scope("settle_1"):
        settle(1)
    with jax.named_scope("carry_0"):
        carry_on(order[0])
    with jax.named_scope("adv_g"):
        advance(marks[2] + 4)
    with jax.named_scope("carry_1"):
        carry_on(order[1])
        start_halo(2, 0)
        start_halo(2, 1)
    with jax.named_scope("adv_g2"):
        advance(marks[2] + 5)
    for k in order[2:]:
        with jax.named_scope("carry_2"):
            carry_on(k)
    with jax.named_scope("adv_h"):
        advance(marks[2] + 6)
        wait_halo(2)
    for n, k in enumerate(order):
        with jax.named_scope("convolve"):
            convolve(k)
            conv_copy(k).start()
        with jax.named_scope("adv_i"):
            advance(min(marks[3], marks[2] + 7 + n))
    with jax.named_scope("settle_2"):
        settle(2)

    with jax.named_scope("att_wait"):
        for i in range(blocks):
            att_copy(i).wait_recv()

    def mix_body(j, carry):
        at = pl.ds(pl.multiple_of(j * cut, cut), cut)
        late = pl.ds(pl.multiple_of(part + j * cut, cut), cut)
        acc = jnp.dot(attended[...], wo_full[q_mine, at], preferred_element_type=f32)
        acc = acc + jnp.dot(att_other[...], wo_full[q_yours, at], preferred_element_type=f32)
        acc = acc + jnp.dot(convolved[...], wo_full[c_mine, late], preferred_element_type=f32)
        acc_ref[:, at] = acc
        return carry

    with jax.named_scope("mix"):
        lax.fori_loop(0, part // cut, mix_body, 0)

    with jax.named_scope("sends"):
        for kind in range(3):
            for way in range(2):

                @pl.when(sends_to[way])
                def _():
                    halo(kind, way).wait_send()

        for g in kinds:
            d_all(g, lines).wait_send()
            ref = some_rows(g, (lines - 1) * heights[g] // 2)
            remote(ref, ref, y_send.at[g], y_recv.at[0, 0], to_y).wait_send()
            for way in range(2):
                for shards in range(1, lines):

                    @pl.when((z + 1 if way == 0 else lines - z) == shards)
                    def _():
                        ref = some_rows(g, shards * heights[g] // 2)
                        remote(ref, ref, z_send.at[way, g], z_recv.at[0, 0], to_z[way]).wait_send()

        remote(tok_own, tok_other, x_send.at[0], x_recv.at[0], to_x).wait_send()
        remote(attended, att_other, att_send.at[0], att_recv.at[0], to_x).wait_send()

    def out_copy(k):
        at = slice(k * CHUNK, (k + 1) * CHUNK)
        return pltpu.make_async_copy(stage.at[at, :], out_ref.at[at, :], out_sem.at[0])

    wide = 512
    for k in order:
        mine = slice(k * CHUNK, (k + 1) * CHUNK)
        with jax.named_scope("conv_wait"):
            conv_copy(k).wait_recv()

        with jax.named_scope("last"):
            for j in range(part // wide):
                at = slice(j * wide, (j + 1) * wide)
                acc = acc_ref[mine, at] + jnp.dot(
                    conv_other[mine, :],
                    wo_full[c_yours, part + j * wide : part + (j + 1) * wide],
                    preferred_element_type=f32,
                )
                stage[mine, at] = acc.astype(bf16)
            out_copy(k).start()

    with jax.named_scope("end"):
        remote(convolved, conv_other, conv_send.at[0], conv_recv.at[0], to_x).wait_send()
        pltpu.make_async_copy(stage, out_ref, out_sem.at[0]).wait()


def fused_layer(
    tokens, gain, projections, outputs, sink_logit, taps, conv_bias, documents, sp_count
):
    rows, part = tokens.shape
    f32 = jnp.float32
    bf16 = jnp.bfloat16
    lines = sp_count // 2
    wk, wv, wc, wu, wb, wq = projections
    width = sum(w.shape[1] for w in projections)
    rp, ro = wq.shape[0], outputs[0].shape[0]
    q_width, k_width, c_width = wq.shape[1], wk.shape[1], wc.shape[1]
    half = HEAD_DIM // 2
    freq = np.power(THETA, -(np.arange(half) / half))
    freq = jnp.asarray(np.tile(freq, LANES // half)[None, :], f32)
    chunks, blocks = rows // CHUNK, rows // WINDOW
    dma = pltpu.SemaphoreType.DMA
    hops = (lines - 1, sum(UNITS))
    kinds = len(UNITS)
    vmem = pl.BlockSpec(memory_space=pltpu.VMEM)
    hbm = pl.BlockSpec(memory_space=pl.ANY)
    smem = pl.BlockSpec(memory_space=pltpu.SMEM)
    flops = 2 * rows * 2 * part * width
    return pl.pallas_call(
        functools.partial(layer_kernel, (lines, rp, ro)),
        out_shape=jax.ShapeDtypeStruct((rows, part), bf16),
        in_specs=[hbm, vmem] + [hbm] * 8 + [smem] + [vmem] * 4,
        out_specs=hbm,
        scratch_shapes=[
            pltpu.VMEM((rp * sp_count, width), bf16),
            pltpu.VMEM((ro * sp_count, 2 * part), bf16),
            pltpu.VMEM((rows, part), bf16),
            pltpu.VMEM((rows, part), bf16),
            pltpu.VMEM((rows, 2 * part), bf16),
            pltpu.VMEM((rows, LANES), f32),
            pltpu.VMEM((rows, part), f32),
            pltpu.VMEM((rows, part), bf16),
            pltpu.VMEM((rows + 2 * WINDOW, 2 * k_width), bf16),
            pltpu.VMEM((rows, 2 * q_width), bf16),
            pltpu.VMEM((rows + 32, c_width), bf16),
            pltpu.VMEM((8, rows + 2 * WINDOW), f32),
            pltpu.VMEM((rows, LANES), f32),
            pltpu.VMEM((64, LANES), f32),
            pltpu.VMEM((rows, LANES), f32),
            pltpu.VMEM((rows, LANES), f32),
            pltpu.VMEM((rows, c_width), bf16),
            pltpu.VMEM((rows, c_width), bf16),
            pltpu.VMEM((rows, q_width), bf16),
            pltpu.VMEM((rows, q_width), bf16),
        ]
        + [dma((2, kinds)), dma(hops), dma((kinds,)), dma(hops), dma((kinds,)), dma((kinds,))]
        + [dma((1,)), dma((chunks,)), dma((kinds,)), dma((chunks,)), dma((1,))]
        + [dma((3, 2)), dma((3, 2)), dma((1,)), dma((chunks,)), dma((1,)), dma((blocks,))],
        compiler_params=pltpu.CompilerParams(
            collective_id=0, has_side_effects=True, vmem_limit_bytes=62 * 1024 * 1024
        ),
        cost_estimate=pl.CostEstimate(flops=flops, bytes_accessed=0, transcendentals=0),
        name="layer",
    )(
        tokens,
        gain[None, :],
        *projections,
        *outputs,
        sink_logit,
        taps,
        conv_bias[None, :],
        documents.reshape(blocks, LANES),
        freq,
    )


def extended(cells, sides, width):
    for axis, dim in sides:
        count = lax.axis_size(axis)
        ends = count - 1
        head = lax.slice_in_dim(cells, 0, width, axis=dim)
        tail = lax.slice_in_dim(cells, cells.shape[dim] - width, cells.shape[dim], axis=dim)
        cells = jnp.concatenate(
            [
                lax.ppermute(tail, axis, [(i, (i + 1) % count) for i in range(ends)]),
                cells,
                lax.ppermute(head, axis, [((i + 1) % count, i) for i in range(ends)]),
            ],
            axis=dim,
        )
    return cells


def rotate(proj, positions, heads):
    rows = proj.shape[0]
    size = proj.shape[1] // heads
    half = size // 2
    freq = jnp.power(THETA, -(jnp.arange(half, dtype=jnp.float32) * (2.0 / size)))
    angle = positions.astype(jnp.float32)[:, None] * freq[None, :]
    cosine = jnp.cos(angle)[:, None, :]
    sine = jnp.sin(angle)[:, None, :]
    shaped = proj.reshape(rows, heads, size)
    first = shaped[..., :half]
    second = shaped[..., half:]
    turned = jnp.concatenate(
        [first * cosine - second * sine, second * cosine + first * sine], axis=-1
    )
    return turned.reshape(rows, heads * size)


def sink_softmax(scores, allowed, sinks):
    masked = jnp.where(allowed, scores, -jnp.inf)
    top = jnp.maximum(jnp.max(masked, axis=-1, keepdims=True), sinks)
    expo = jnp.exp(masked - top)
    return expo / (jnp.sum(expo, axis=-1, keepdims=True) + jnp.exp(sinks - top))


def local(
    tokens,
    gain,
    w_query,
    w_key,
    w_value,
    w_input,
    w_bgate,
    w_cgate,
    w_attn_out,
    w_conv_out,
    sink_logit,
    taps,
    conv_bias,
    documents,
):
    f32 = jnp.float32
    bf16 = jnp.bfloat16
    rows, part = tokens.shape
    tp_count = lax.axis_size("tp")
    sp_count = lax.axis_size("sp")
    width = part * tp_count
    head_dim = HEAD_DIM
    q_local = w_query.shape[1] // head_dim
    kv_local = w_key.shape[1] // head_dim
    groups = q_local // kv_local
    if fused_plan(
        lax.axis_size("grp"),
        sp_count,
        tp_count,
        rows,
        part,
        w_query.shape[0],
        w_attn_out.shape[0],
        w_query.shape[1],
        w_key.shape[1],
        w_input.shape[1],
    ):
        return fused_layer(
            tokens,
            gain,
            (w_key, w_value, w_cgate, w_input, w_bgate, w_query),
            (w_attn_out, w_conv_out),
            sink_logit,
            taps,
            conv_bias,
            documents,
            sp_count,
        )
    wq, wk, wv, wu, wb, wc, w_attn, w_conv = (
        lax.all_gather(w_query, "sp", axis=0, tiled=True),
        lax.all_gather(w_key, "sp", axis=0, tiled=True),
        lax.all_gather(w_value, "sp", axis=0, tiled=True),
        lax.all_gather(w_input, "sp", axis=0, tiled=True),
        lax.all_gather(w_bgate, "sp", axis=0, tiled=True),
        lax.all_gather(w_cgate, "sp", axis=0, tiled=True),
        lax.all_gather(w_attn_out, "sp", axis=0, tiled=True),
        lax.all_gather(w_conv_out, "sp", axis=0, tiled=True),
    )
    matrices = (wq, wk, wv, wu, wb, wc)
    piece_f = lax.all_gather(tokens, "tp", axis=1, tiled=True).astype(f32)
    scaled = (piece_f * gain[None, :]).astype(bf16)
    products = tuple((jnp.dot(scaled, mat, preferred_element_type=f32) for mat in matrices))
    folded = products + (jnp.sum(piece_f * piece_f, axis=1),)
    sums = folded[:6]
    squares = folded[6]
    inv = lax.rsqrt(squares / width + EPS)[:, None]
    q_acc, k_acc, v_acc, u_acc, b_acc, c_acc = sums
    positions = lax.axis_index("sp") * rows + jnp.arange(rows, dtype=jnp.int32)
    query = rotate(q_acc * inv, positions, q_local).astype(bf16)
    keys = rotate(k_acc * inv, positions, kv_local).astype(bf16)
    values = (v_acc * inv).astype(bf16)
    carried = (c_acc * inv * (u_acc * inv)).astype(bf16)
    bgate = b_acc * inv
    doc_col = documents.astype(f32).astype(bf16)[:, None]
    paired = jnp.concatenate([keys, values], axis=1)
    pair_ext, doc_ext = (
        extended(paired, (("sp", 0),), WINDOW),
        extended(doc_col, (("sp", 0),), WINDOW),
    )
    carry_ext, doc_near = (extended(carried, (("sp", 0),), 1), extended(doc_col, (("sp", 0),), 1))
    key_width = kv_local * head_dim
    key_ext = pair_ext[:, :key_width].reshape(-1, kv_local, head_dim)
    val_ext = pair_ext[:, key_width:].reshape(-1, kv_local, head_dim)
    key_doc = doc_ext[:, 0].astype(f32)
    own_doc = doc_col[:, 0].astype(f32)
    key_pos = positions[0] - WINDOW + jnp.arange(rows + 2 * WINDOW, dtype=jnp.int32)
    total = sp_count * rows
    sinks = sink_logit.reshape(kv_local, groups, 1, 1)
    block = rows // 2
    outputs = []
    for begin in range(0, rows, block):
        span = block + 2 * WINDOW
        q_block = query[begin : begin + block].reshape(block, kv_local, groups, head_dim)
        k_block = key_ext[begin : begin + span]
        v_block = val_ext[begin : begin + span]
        q_pos = positions[begin : begin + block]
        k_pos = key_pos[begin : begin + span]
        scores = jnp.einsum(
            "qhgd,khd->hgqk", q_block, k_block, preferred_element_type=f32
        ) * head_dim ** (-0.5)
        allowed = jnp.abs(q_pos[:, None] - k_pos[None, :]) <= WINDOW
        allowed = allowed & (
            own_doc[begin : begin + block, None] == key_doc[None, begin : begin + span]
        )
        allowed = allowed & (k_pos >= 0)[None, :] & (k_pos < total)[None, :]
        weight = sink_softmax(scores, allowed, sinks).astype(bf16)
        result = jnp.einsum("hgqk,khd->qhgd", weight, v_block, preferred_element_type=f32)
        outputs.append(result.astype(bf16).reshape(block, q_local * head_dim))
    attended = jnp.concatenate(outputs, axis=0)
    near_doc = doc_near[:, 0].astype(f32)
    conv = jnp.zeros((rows, carried.shape[1]), f32)
    for tap in range(3):
        same = (near_doc[tap : tap + rows] == near_doc[1 : rows + 1])[:, None]
        conv = conv + jnp.where(
            same, carry_ext[tap : tap + rows].astype(f32) * taps[tap][None, :], 0.0
        )
    convolved = (bgate * (conv + conv_bias[None, :])).astype(bf16)
    acc = jnp.dot(
        lax.all_gather(attended, "tp", axis=1, tiled=True), w_attn, preferred_element_type=f32
    )
    mixed = acc + jnp.dot(
        lax.all_gather(convolved, "tp", axis=1, tiled=True), w_conv, preferred_element_type=f32
    )
    return mixed.astype(bf16)


def solution(mesh):
    placed = (
        P(("grp", "sp"), "tp"),
        P(),
        P("sp", "tp"),
        P("sp", "tp"),
        P("sp", "tp"),
        P("sp", "tp"),
        P("sp", "tp"),
        P("sp", "tp"),
        P("sp", "tp"),
        P("sp", "tp"),
        P("tp"),
        P(None, "tp"),
        P("tp"),
        P(("grp", "sp")),
    )
    return jax.shard_map(
        local, mesh=mesh, in_specs=placed, out_specs=P(("grp", "sp"), "tp"), check_vma=False
    )
```

```python
import functools

import jax
import jax.numpy as jnp
import numpy as np
from jax import lax
from jax.experimental import pallas as pl
from jax.experimental.pallas import tpu as pltpu
from jax.sharding import PartitionSpec as P

HEAD_DIM = 64
WINDOW = 128


EPS = 1e-06
THETA = 500000.0
UNITS = (4, 4, 4, 4)
LAGS = (7, 6, 8, 6)
CHUNK = 256
LANES = 128


def fused_plan(grp_count, sp_count, tp_count, rows, part, proj_rows, out_rows, q_width, k_width, c_width):
    lines = sp_count // 2
    return (
        grp_count == 2
        and tp_count == 2
        and sp_count % 2 == 0
        and lines == 4
        and all(proj_rows % (2 * units * 16) == 0 for units in UNITS[:3])
        and all(out_rows % (2 * units * 16) == 0 for units in UNITS[3:])
        and rows % CHUNK == 0
        and 3 * CHUNK <= rows <= 1024
        and CHUNK == 2 * WINDOW
        and WINDOW == LANES
        and part % 512 == 0
        and q_width == 4 * k_width
        and k_width == LANES
        and c_width % 256 == 0
        and 2 * HEAD_DIM == LANES
    )


def layer_kernel(
    sizes,
    tok_hbm,
    gain_hbm,
    wk_ref,
    wv_ref,
    wc_ref,
    wu_ref,
    wb_ref,
    wq_ref,
    wa_ref,
    wm_ref,
    sink_hbm,
    taps_hbm,
    bias_hbm,
    doc_hbm,
    freq_hbm,
    out_ref,
    gain_ref,
    sink_ref,
    taps_ref,
    bias_ref,
    doc_ref,
    freq_ref,
    wp_full,
    wo_full,
    tok_own,
    tok_other,
    scaled,
    inv_ref,
    acc_ref,
    pair_ext,
    query_s,
    carried,
    doc_row,
    doc_col,
    turn_ref,
    cos_ref,
    sin_ref,
    convolved,
    conv_other,
    attended,
    att_other,
    z_send,
    z_recv,
    y_send,
    y_recv,
    d_send,
    d_recv,
    x_send,
    x_recv,
    own_sem,
    tok_sem,
    small_sem,
    halo_send,
    halo_recv,
    conv_send,
    conv_recv,
    att_send,
    att_recv,
):
    lines, rp, ro = sizes
    f32 = jnp.float32
    bf16 = jnp.bfloat16
    rows, part = tok_own.shape
    k_width, c_width, q_width = wk_ref.shape[1], wc_ref.shape[1], wq_ref.shape[1]
    k_at = 3 * c_width
    q_at = k_at + 2 * k_width
    width = q_at + q_width
    chunks = rows // CHUNK
    blocks = rows // WINDOW
    order = (chunks - 1,) + tuple(range(chunks - 1))
    pieces = [(k * CHUNK, CHUNK) for k in order[:-1]]
    pieces += [(order[-1] * CHUNK, WINDOW), (order[-1] * CHUNK + WINDOW, WINDOW)]
    y = lax.axis_index("grp")
    sp = lax.axis_index("sp")
    x = lax.axis_index("tp")
    z, c = sp // 2, sp % 2
    counts = UNITS
    kinds = range(len(counts))
    fulls = (wp_full, wp_full, wp_full, wo_full)
    heights = (rp, rp, rp, ro)
    spans = ((k_at, width), (0, 2 * c_width), (2 * c_width, k_at), (0, 2 * part))
    first_unit, marks = [0], [0]
    for count in counts:
        first_unit.append(first_unit[-1] + count)
        marks.append(marks[-1] + (lines - 1) * count)
    to_y = {"grp": 1 - y}
    to_core = {"sp": z * 2 + 1 - c}
    to_x = {"tp": 1 - x}
    to_z = ({"sp": sp + 2}, {"sp": sp - 2})
    has_next = (z < lines - 1, z > 0)

    def origin(way, t):
        return z - t if way == 0 else z + t

    def arrives(way, t):
        return z >= t if way == 0 else z < lines - t

    def place(g, j, zo, cc, h):
        size = heights[g]
        tall = size // 2 // counts[g]
        row = (zo * 2 + cc) * size + h * (size // 2) + j * tall
        return fulls[g].at[pl.ds(pl.multiple_of(row, tall), tall), spans[g][0] : spans[g][1]]

    def remote(src, dst, send, recv, device):
        return pltpu.make_async_remote_copy(
            src_ref=src, dst_ref=dst, send_sem=send, recv_sem=recv,
            device_id=device, device_id_type=pl.DeviceIdType.MESH,
        )

    def z_copy(way, t, g, j):
        zo = origin(way, t)
        ref, u = place(g, j, zo, c, y), first_unit[g] + j
        return remote(ref, ref, z_send.at[way, g], z_recv.at[zo - way, u], to_z[way])

    def y_copy(way, t, g, j, h):
        zo = origin(way, t)
        ref, u = place(g, j, zo, c, h), first_unit[g] + j
        return remote(ref, ref, y_send.at[g], y_recv.at[zo - way, u], to_y)

    def d_copy(way, t, g, j, h):
        ref = place(g, j, origin(way, t), c, h)
        return remote(ref, ref, d_send.at[g], d_recv.at[g], to_core)

    def some_rows(g, count):
        return fulls[g].at[0:count, spans[g][0] : spans[g][1]]

    def d_all(g, shards):
        ref = some_rows(g, shards * heights[g])
        return remote(ref, ref, d_send.at[g], d_recv.at[g], to_core)

    def own_ref(g):
        at = pl.ds(pl.multiple_of((z * 2 + c) * heights[g], heights[g]), heights[g])
        return fulls[g].at[at, spans[g][0] : spans[g][1]]

    def own_d(g):
        return remote(own_ref(g), own_ref(g), d_send.at[g], d_recv.at[g], to_core)

    own_refs = ((wk_ref, wv_ref, wq_ref), (wc_ref, wu_ref), (wb_ref,), (wa_ref, wm_ref))

    def own_local(g):
        at, copies, col = pl.ds(pl.multiple_of((z * 2 + c) * heights[g], heights[g]), heights[g]), [], spans[g][0]
        for ref in own_refs[g]:
            size = ref.shape[1]
            copies.append(
                pltpu.make_async_copy(ref, fulls[g].at[at, col : col + size], own_sem.at[g])
            )
            col += size
        return copies

    def tok_local(i):
        at = slice(pieces[i][0], sum(pieces[i]))
        return pltpu.make_async_copy(tok_hbm.at[at, :], tok_own.at[at, :], tok_sem.at[i])

    def x_copy(i):
        at = slice(pieces[i][0], sum(pieces[i]))
        return remote(tok_own.at[at, :], tok_other.at[at, :], x_send.at[0], x_recv.at[i], to_x)

    last = 2 * lines - 1
    steps_sp = (sp + 1, sp - 1)
    sends_to = (sp < last, sp > 0)
    gets_from = (sp > 0, sp < last)
    side = jnp.where(c == 0, sp - 1, sp + 1)
    has_side = (side >= 0) & (side <= last)
    edge = 16

    def halo(kind, way):
        if kind == 0:
            at = rows if way == 0 else WINDOW
            src = doc_row.at[:, at : at + WINDOW]
            at = 0 if way == 0 else WINDOW + rows
            dst = doc_row.at[:, at : at + WINDOW]
        elif kind == 1:
            at = rows if way == 0 else WINDOW
            src = pair_ext.at[at : at + WINDOW, :]
            at = 0 if way == 0 else WINDOW + rows
            dst = pair_ext.at[at : at + WINDOW, :]
        else:
            at = rows if way == 0 else edge
            src = carried.at[at : at + edge, :]
            at = 0 if way == 0 else edge + rows
            dst = carried.at[at : at + edge, :]
        return remote(
            src, dst, halo_send.at[kind, way], halo_recv.at[kind, way], {"sp": steps_sp[way]}
        )

    def start_halo(kind, way):
        @pl.when(sends_to[way])
        def _():
            halo(kind, way).start()

    def wait_halo(kind, way):
        @pl.when(gets_from[way])
        def _():
            halo(kind, way).wait_recv()

    def conv_copy(k):
        at = slice(k * CHUNK, (k + 1) * CHUNK)
        return remote(
            convolved.at[at, :], conv_other.at[at, :], conv_send.at[0], conv_recv.at[k], to_x
        )

    def att_copy(i):
        at = pl.ds(pl.multiple_of(i * WINDOW, WINDOW), WINDOW)
        return remote(attended.at[at, :], att_other.at[at, :], att_send.at[0], att_recv.at[i], to_x)

    def start_own(g):
        pltpu.make_async_copy(own_ref(g), own_ref(g), own_sem.at[g]).wait()
        for j in range(counts[g]):
            for way in range(2):

                @pl.when(has_next[way])
                def _():
                    z_copy(way, 0, g, j).start()

        own_d(g).start()

    def z_event(g, m):
        t, j = m // counts[g] + 1, m % counts[g]
        for way in range(2):

            @pl.when(arrives(way, t))
            def _():
                z_copy(way, t, g, j).wait_recv()

                @pl.when(has_next[way] & (t < lines - 1))
                def _():
                    z_copy(way, t, g, j).start()

                y_copy(way, t, g, j, y).start()
                d_copy(way, t, g, j, y).start()

    def y_event(g, m):
        t, j = m // counts[g] + 1, m % counts[g]
        for way in range(2):

            @pl.when(arrives(way, t))
            def _():
                y_copy(way, t, g, j, 1 - y).wait_recv()
                d_copy(way, t, g, j, 1 - y).start()

    def on(n, act):
        if isinstance(n, int):
            g = max(i for i in kinds if marks[i] <= n)
            act(g, n - marks[g])
            return
        for g in kinds:

            @pl.when((n >= marks[g]) & (n < marks[g + 1]))
            def _():
                act(g, n - marks[g])

    state = [0, 0]

    costs = [heights[g] // counts[g] * (spans[g][1] - spans[g][0]) for g in kinds]
    unit_of = [g for g in kinds for _ in range((lines - 1) * counts[g])]
    ends = [sum(costs[g] for g in unit_of[: n + 1]) for n in range(marks[-1])]

    def due(m):
        if m >= marks[-1]:
            return m
        limit = ends[m] + LAGS[unit_of[m]] * costs[unit_of[m]]
        return max(n for n in range(marks[-1]) if ends[n] <= limit)

    def advance(goal):
        while state[0] < goal:
            on(state[0], z_event)
            state[0] += 1
            while due(state[1]) < state[0]:
                on(state[1], y_event)
                state[1] += 1

    def flush(g):
        while state[1] < marks[g + 1]:
            on(state[1], y_event)
            state[1] += 1

    def settle(g):
        advance(marks[g + 1])
        flush(g)
        d_all(g, lines).wait_recv()

    small = [
        pltpu.make_async_copy(src, dst, small_sem.at[i])
        for i, (src, dst) in enumerate(
            (
                (doc_hbm, doc_ref),
                (freq_hbm, freq_ref),
                (gain_hbm, gain_ref),
                (taps_hbm, taps_ref),
                (bias_hbm, bias_ref),
                (sink_hbm, sink_ref),
            )
        )
    ]
    barrier = pltpu.get_barrier_semaphore()
    for device in (to_y, to_core, to_x):
        pl.semaphore_signal(barrier, inc=1, device_id=device, device_id_type=pl.DeviceIdType.MESH)
    for way in range(2):

        @pl.when(has_next[way])
        def _():
            pl.semaphore_signal(
                barrier, inc=1, device_id=to_z[way], device_id_type=pl.DeviceIdType.MESH
            )

    @pl.when(has_side)
    def _():
        pl.semaphore_signal(
            barrier, inc=1, device_id={"sp": side}, device_id_type=pl.DeviceIdType.MESH
        )

    for i in range(len(pieces)):
        tok_local(i).start()
    for g in kinds:
        for copy in own_local(g):
            copy.start()
    for copy in small:
        copy.start()
    small[0].wait()
    docs = doc_ref[...].astype(f32)
    for i in range(blocks):
        doc_row[:, (i + 1) * WINDOW : (i + 2) * WINDOW] = jnp.broadcast_to(
            docs[i : i + 1, :], (doc_row.shape[0], LANES)
        )

    @pl.when(sp == 0)
    def _():
        doc_row[:, :WINDOW] = jnp.full((doc_row.shape[0], WINDOW), -1.0, f32)
        pair_ext[:WINDOW, :] = jnp.zeros((WINDOW, pair_ext.shape[1]), bf16)

    @pl.when(sp == last)
    def _():
        doc_row[:, WINDOW + rows :] = jnp.full((doc_row.shape[0], WINDOW), -1.0, f32)
        pair_ext[WINDOW + rows :, :] = jnp.zeros((WINDOW, pair_ext.shape[1]), bf16)

    neighbours = jnp.where(has_side, 1, 0) + jnp.where(z > 0, 1, 0) + jnp.where(z < lines - 1, 1, 0) + 3
    with jax.named_scope("barrier"):
        pl.semaphore_wait(barrier, neighbours)

    for i in range(len(pieces)):
        tok_local(i).wait()
        x_copy(i).start()
    start_own(0)
    for way in range(2):
        start_halo(0, way)

    for i in range(blocks):
        at = slice(i * WINDOW, (i + 1) * WINDOW)
        doc_col[at, :] = jnp.broadcast_to(docs[i : i + 1, :], (WINDOW, LANES)).T

    tile = 32
    lane = lax.broadcasted_iota(jnp.int32, (tile, LANES), 1)
    step = lax.broadcasted_iota(jnp.int32, (tile, LANES), 0)
    for copy in small[1:]:
        copy.wait()
    freq = freq_ref[...]
    far = (sp * rows + step * tile).astype(f32) * freq
    near_angle = step.astype(f32) * freq
    turn_ref[0:tile, :] = jnp.cos(far)
    turn_ref[tile : 2 * tile, :] = jnp.sin(far)
    near_cos, near_sin = jnp.cos(near_angle), jnp.sin(near_angle)
    sign = jnp.where((lane % HEAD_DIM) < HEAD_DIM // 2, -1.0, 1.0)

    def table_body(i, carry):
        at = pl.ds(pl.multiple_of(i * tile, tile), tile)
        far_cos, far_sin = turn_ref[pl.ds(i, 1), :], turn_ref[pl.ds(tile + i, 1), :]
        cos_ref[at, :] = far_cos * near_cos - far_sin * near_sin
        sin_ref[at, :] = sign * (far_sin * near_cos + far_cos * near_sin)
        return carry

    lax.fori_loop(0, rows // tile, table_body, 0)

    mine_at = pl.multiple_of(x * part, part)
    yours_at = pl.multiple_of((1 - x) * part, part)

    def scale(piece):
        begin, size = pieces[piece]
        x_copy(piece).wait_recv()

        def body(i, carry):
            at = pl.ds(pl.multiple_of(begin + i * tile, tile), tile)
            own = tok_own[at, :].astype(f32)
            other = tok_other[at, :].astype(f32)
            total = jnp.sum(own * own, axis=1, keepdims=True) + jnp.sum(
                other * other, axis=1, keepdims=True
            )
            inv_ref[at, :] = jnp.broadcast_to(
                lax.rsqrt(total / (2 * part) + EPS), (tile, inv_ref.shape[1])
            )
            scaled[at, pl.ds(mine_at, part)] = (own * gain_ref[:, pl.ds(mine_at, part)]).astype(bf16)
            scaled[at, pl.ds(yours_at, part)] = (
                other * gain_ref[:, pl.ds(yours_at, part)]
            ).astype(bf16)
            return carry

        lax.fori_loop(0, size // tile, body, 0)

    cut = 256

    def project(mine, at):
        acc = jnp.dot(scaled[mine, :], wp_full[:, at], preferred_element_type=f32)
        return acc * inv_ref[mine, :1]

    lane_c = lax.broadcasted_iota(jnp.int32, (CHUNK, LANES), 1)
    low = (lane_c % HEAD_DIM) < HEAD_DIM // 2
    left = lane_c < HEAD_DIM

    def project_att(piece):
        begin, size = pieces[piece]
        mine = slice(begin, begin + size)
        ext = slice(WINDOW + begin, WINDOW + begin + size)

        def turned(cells):
            ahead = pltpu.roll(cells, LANES - HEAD_DIM // 2, 1)
            behind = pltpu.roll(cells, HEAD_DIM // 2, 1)
            return cells * cos_ref[mine, :] + jnp.where(low[:size], ahead, behind) * sin_ref[mine, :]

        cells = project(mine, slice(k_at, q_at))
        pair_ext[ext, :k_width] = turned(cells[:, :k_width]).astype(bf16)
        pair_ext[ext, k_width:] = cells[:, k_width:].astype(bf16)

        def query_body(j, carry):
            cells = project(mine, pl.ds(pl.multiple_of(q_at + j * cut, cut), cut))
            for i in range(cut // LANES):
                pair = turned(cells[:, i * LANES : (i + 1) * LANES]) * HEAD_DIM ** (-0.5)
                swapped = pltpu.roll(pair, HEAD_DIM, 1)
                own_half = left[:size] == (j == 0)
                first = jnp.where(own_half, jnp.where(j == 0, pair, swapped), 0.0)
                second = jnp.where(own_half, jnp.where(j == 0, swapped, pair), 0.0)
                at = pl.multiple_of((j * (cut // LANES) + i) * 2 * LANES, LANES)
                query_s[mine, pl.ds(at, LANES)] = first.astype(bf16)
                query_s[mine, pl.ds(at + LANES, LANES)] = second.astype(bf16)
            return carry

        for j in range(q_width // cut):
            query_body(j, 0)

    kv_heads = k_width // HEAD_DIM
    groups = q_width // HEAD_DIM // kv_heads
    span = 3 * WINDOW
    gap = lax.broadcasted_iota(jnp.int32, (WINDOW, span), 1) - lax.broadcasted_iota(
        jnp.int32, (WINDOW, span), 0
    )
    window = (gap >= 0) & (gap <= 2 * WINDOW)
    left_w = left[:WINDOW, :]

    def attend(i):
        at = pl.ds(pl.multiple_of(i * WINDOW, WINDOW), WINDOW)
        near = pl.ds(pl.multiple_of(i * WINDOW, WINDOW), span)
        allowed = window & (doc_col[at, 0:1] == doc_row[0:1, near])
        bias = jnp.where(allowed, 0.0, -jnp.inf)
        bias = jnp.concatenate([bias] * groups, axis=0)
        keys = pair_ext[near, :k_width]
        values = jnp.concatenate(
            [pair_ext[near, k_width:], jnp.ones((span, LANES), bf16)], axis=1
        )
        for head in range(kv_heads):
            first = head * groups
            stack = jnp.concatenate(
                [
                    query_s[at, (first + g) * LANES : (first + g + 1) * LANES]
                    for g in range(groups)
                ],
                axis=0,
            )
            sinks = jnp.concatenate(
                [jnp.full((WINDOW, 1), sink_ref[first + g], f32) for g in range(groups)], axis=0
            )
            scores = lax.dot_general(
                stack, keys, (((1,), (1,)), ((), ())), preferred_element_type=f32
            )
            scores = scores + bias
            top = jnp.maximum(jnp.max(scores, axis=1, keepdims=True), sinks)
            expo = jnp.exp(scores - top).astype(bf16)
            result = jnp.dot(expo, values, preferred_element_type=f32)
            total = result[:, LANES:] + jnp.exp(sinks - top)
            result = result[:, :LANES] * (1.0 / total)
            for g in range(0, groups, 2):
                one = result[g * WINDOW : (g + 1) * WINDOW]
                two = result[(g + 1) * WINDOW : (g + 2) * WINDOW]
                if head == 0:
                    pair = jnp.where(left_w, one, pltpu.roll(two, HEAD_DIM, 1))
                else:
                    pair = jnp.where(left_w, pltpu.roll(one, HEAD_DIM, 1), two)
                to = (first + g) * HEAD_DIM
                attended[at, to : to + LANES] = pair.astype(bf16)

    def attend_all(count, events, pick, guard=False):
        begin, lag = state

        def body(j, carry):
            if guard:
                with jax.named_scope("halo_wait"):
                    for way in range(2):

                        @pl.when(gets_from[way] & (j == way))
                        def _():
                            halo(1, way).wait_recv()

            with jax.named_scope("attend"):
                attend(pick(j))
                att_copy(pick(j)).start()
            with jax.named_scope("att_ev"):
                for e in range(events):
                    on(begin + j * events + e, z_event)
                    on(lag + j * events + e, y_event)
            return carry

        lax.fori_loop(0, count, body, 0)
        state[0] += count * events
        state[1] += count * events

    def carry_on(k):
        mine = slice(k * CHUNK, (k + 1) * CHUNK)
        ext = slice(edge + k * CHUNK, edge + (k + 1) * CHUNK)
        for j in range(c_width // cut):
            at = slice(j * cut, (j + 1) * cut)
            gate = project(mine, at)
            carried[ext, at] = (
                gate * project(mine, slice(c_width + j * cut, c_width + (j + 1) * cut))
            ).astype(bf16)

    row_c = lax.broadcasted_iota(jnp.int32, (CHUNK, LANES), 0)

    def convolve(k):
        begin, end = k * CHUNK, (k + 1) * CHUNK
        mine = slice(begin, end)
        docs_here = doc_col[mine, :]
        doc_before = jnp.where(
            row_c == 0,
            doc_row[0:1, WINDOW + begin - 1 : WINDOW + begin],
            pltpu.roll(docs_here, 1, 0),
        )
        doc_after = jnp.where(
            row_c == CHUNK - 1,
            doc_row[0:1, WINDOW + end : WINDOW + end + 1],
            pltpu.roll(docs_here, CHUNK - 1, 0),
        )
        for j in range(c_width // cut):
            gates = project(mine, slice(2 * c_width + j * cut, 2 * c_width + (j + 1) * cut))
            for i in range(cut // LANES):
                at = slice(j * cut + i * LANES, j * cut + (i + 1) * LANES)
                cells = carried[edge + begin : edge + end, at].astype(f32)
                head = carried[begin : begin + edge, at].astype(f32)
                foot = carried[edge + end : 2 * edge + end, at].astype(f32)
                before = jnp.where(row_c == 0, head[edge - 1 : edge, :], pltpu.roll(cells, 1, 0))
                after = jnp.where(row_c == CHUNK - 1, foot[0:1, :], pltpu.roll(cells, CHUNK - 1, 0))
                conv = jnp.where(doc_before == docs_here, before * taps_ref[0:1, at], 0.0)
                conv = conv + cells * taps_ref[1:2, at]
                conv = conv + jnp.where(doc_after == docs_here, after * taps_ref[2:3, at], 0.0)
                gate = gates[:, i * LANES : (i + 1) * LANES]
                convolved[mine, at] = (gate * (conv + bias_ref[:, at])).astype(bf16)

    def ahead_of(g):
        return marks[g + 1] - counts[g] + 1

    q_mine = pl.ds(pl.multiple_of(x * q_width, q_width), q_width)
    q_yours = pl.ds(pl.multiple_of((1 - x) * q_width, q_width), q_width)
    c_mine = pl.ds(pl.multiple_of(x * c_width, c_width), c_width)
    c_yours = pl.ds(pl.multiple_of((1 - x) * c_width, c_width), c_width)

    with jax.named_scope("adv_a"):
        advance(ahead_of(0))
        start_own(1)
        advance(marks[1] - 1)
    with jax.named_scope("scale_0"):
        scale(0)
    with jax.named_scope("adv_b"):
        advance(marks[1] + 3)
    with jax.named_scope("settle_0"):
        settle(0)
    with jax.named_scope("att_proj_0"):
        project_att(0)
        start_halo(1, 0)
    with jax.named_scope("adv_c"):
        advance(marks[1] + 7)
    with jax.named_scope("scale_1"):
        for i in range(1, len(pieces) - 2):
            scale(i)
    with jax.named_scope("att_proj_1"):
        project_att(1)
        start_halo(1, 1)
        for i in range(2, len(pieces) - 2):
            project_att(i)
    with jax.named_scope("adv_d"):
        advance(ahead_of(1))
        start_own(2)
        wait_halo(0, 0)
        wait_halo(0, 1)
    attend_all(2, 1, lambda j: j * (blocks - 1), True)
    with jax.named_scope("adv_e"):
        advance(marks[2] + 2)
    with jax.named_scope("scale_2"):
        scale(len(pieces) - 2)
    with jax.named_scope("att_proj_2"):
        project_att(len(pieces) - 2)
    with jax.named_scope("adv_e2"):
        advance(marks[2] + 5)
    attend_all(blocks - 5, 1, lambda j: j + 1)
    with jax.named_scope("scale_3"):
        scale(len(pieces) - 1)
    with jax.named_scope("adv_e3"):
        advance(marks[2] + 8)
        start_own(3)
    with jax.named_scope("att_proj_3"):
        project_att(len(pieces) - 1)
    attend_all(2, 2, lambda j: j + blocks - 4)
    attend_all(1, 0, lambda j: j + blocks - 2)
    with jax.named_scope("settle_1"):
        settle(1)
    with jax.named_scope("carry_0"):
        carry_on(order[0])
        start_halo(2, 0)
    with jax.named_scope("adv_f"):
        advance(marks[3] + 1)
    with jax.named_scope("carry_1"):
        carry_on(order[1])
        start_halo(2, 1)
    with jax.named_scope("adv_h"):
        advance(marks[3] + 2)
        flush(2)
    for k in order[2:]:
        with jax.named_scope("carry_2"):
            carry_on(k)
    with jax.named_scope("adv_i"):
        advance(marks[3] + 3)
    with jax.named_scope("settle_2"):
        settle(2)
    for k in range(chunks):
        with jax.named_scope("halo_2"):
            if k == 0:
                wait_halo(2, 0)
            if k == chunks - 1:
                wait_halo(2, 1)
        with jax.named_scope("convolve"):
            convolve(k)
            conv_copy(k).start()
        with jax.named_scope("adv_j"):
            advance(min(marks[4], marks[3] + 4 + k))
    with jax.named_scope("adv_k"):
        advance(marks[4])
    with jax.named_scope("settle_3"):
        settle(3)

    with jax.named_scope("att_wait"):
        for i in range(blocks):
            att_copy(i).wait_recv()

    def mix_body(j, carry):
        at = pl.ds(pl.multiple_of(j * cut, cut), cut)
        late = pl.ds(pl.multiple_of(part + j * cut, cut), cut)
        acc = jnp.dot(attended[...], wo_full[q_mine, at], preferred_element_type=f32)
        acc = acc + jnp.dot(att_other[...], wo_full[q_yours, at], preferred_element_type=f32)
        acc = acc + jnp.dot(convolved[...], wo_full[c_mine, late], preferred_element_type=f32)
        acc_ref[:, at] = acc
        return carry

    with jax.named_scope("mix"):
        lax.fori_loop(0, part // cut, mix_body, 0)

    with jax.named_scope("sends"):
        for kind in range(3):
            for way in range(2):

                @pl.when(sends_to[way])
                def _():
                    halo(kind, way).wait_send()

        for g in kinds:
            d_all(g, lines).wait_send()
            ref = some_rows(g, (lines - 1) * heights[g] // 2)
            remote(ref, ref, y_send.at[g], y_recv.at[0, 0], to_y).wait_send()
            for way in range(2):
                for shards in range(1, lines):

                    @pl.when((z + 1 if way == 0 else lines - z) == shards)
                    def _():
                        ref = some_rows(g, shards * heights[g] // 2)
                        remote(ref, ref, z_send.at[way, g], z_recv.at[0, 0], to_z[way]).wait_send()

        remote(tok_own, tok_other, x_send.at[0], x_recv.at[0], to_x).wait_send()
        remote(attended, att_other, att_send.at[0], att_recv.at[0], to_x).wait_send()

    wide = 512
    for k in range(chunks):
        mine = slice(k * CHUNK, (k + 1) * CHUNK)
        with jax.named_scope("conv_wait"):
            conv_copy(k).wait_recv()

        with jax.named_scope("last"):
            for j in range(part // wide):
                at = slice(j * wide, (j + 1) * wide)
                acc = acc_ref[mine, at] + jnp.dot(
                    conv_other[mine, :],
                    wo_full[c_yours, part + j * wide : part + (j + 1) * wide],
                    preferred_element_type=f32,
                )
                out_ref[mine, at] = acc.astype(bf16)

    with jax.named_scope("end"):
        remote(convolved, conv_other, conv_send.at[0], conv_recv.at[0], to_x).wait_send()


def fused_layer(
    tokens, gain, projections, outputs, sink_logit, taps, conv_bias, documents, sp_count
):
    rows, part = tokens.shape
    f32 = jnp.float32
    bf16 = jnp.bfloat16
    lines = sp_count // 2
    wk, wv, wc, wu, wb, wq = projections
    width = sum(w.shape[1] for w in projections)
    rp, ro = wq.shape[0], outputs[0].shape[0]
    q_width, k_width, c_width = wq.shape[1], wk.shape[1], wc.shape[1]
    half = HEAD_DIM // 2
    freq = np.power(THETA, -(np.arange(half) / half))
    freq = jnp.asarray(np.tile(freq, LANES // half)[None, :], f32)
    chunks, blocks = rows // CHUNK, rows // WINDOW
    dma = pltpu.SemaphoreType.DMA
    hops = (lines - 1, sum(UNITS))
    kinds = len(UNITS)
    vmem = pl.BlockSpec(memory_space=pltpu.VMEM)
    hbm = pl.BlockSpec(memory_space=pl.ANY)
    flops = 2 * rows * 2 * part * width
    return pl.pallas_call(
        functools.partial(layer_kernel, (lines, rp, ro)),
        out_shape=pltpu.VMEM((rows, part), bf16),
        in_specs=[hbm] * 15,
        out_specs=vmem,
        scratch_shapes=[
            pltpu.VMEM((1, 2 * part), f32),
            pltpu.SMEM(sink_logit.shape, f32),
            pltpu.VMEM(taps.shape, f32),
            pltpu.VMEM((1, c_width), f32),
            pltpu.VMEM((blocks, LANES), jnp.int32),
            pltpu.VMEM((1, LANES), f32),
            pltpu.VMEM((rp * sp_count, width), bf16),
            pltpu.VMEM((ro * sp_count, 2 * part), bf16),
            pltpu.VMEM((rows, part), bf16),
            pltpu.VMEM((rows, part), bf16),
            pltpu.VMEM((rows, 2 * part), bf16),
            pltpu.VMEM((rows, LANES), f32),
            pltpu.VMEM((rows, part), f32),
            pltpu.VMEM((rows + 2 * WINDOW, 2 * k_width), bf16),
            pltpu.VMEM((rows, 2 * q_width), bf16),
            pltpu.VMEM((rows + 32, c_width), bf16),
            pltpu.VMEM((8, rows + 2 * WINDOW), f32),
            pltpu.VMEM((rows, LANES), f32),
            pltpu.VMEM((64, LANES), f32),
            pltpu.VMEM((rows, LANES), f32),
            pltpu.VMEM((rows, LANES), f32),
            pltpu.VMEM((rows, c_width), bf16),
            pltpu.VMEM((rows, c_width), bf16),
            pltpu.VMEM((rows, q_width), bf16),
            pltpu.VMEM((rows, q_width), bf16),
        ]
        + [dma((2, kinds)), dma(hops), dma((kinds,)), dma(hops), dma((kinds,)), dma((kinds,))]
        + [dma((1,)), dma((chunks + 1,)), dma((kinds,)), dma((chunks + 1,)), dma((6,))]
        + [dma((3, 2)), dma((3, 2)), dma((1,)), dma((chunks,)), dma((1,)), dma((blocks,))],
        compiler_params=pltpu.CompilerParams(
            collective_id=0, has_side_effects=True, vmem_limit_bytes=62 * 1024 * 1024
        ),
        cost_estimate=pl.CostEstimate(flops=flops, bytes_accessed=0, transcendentals=0),
        name="layer",
    )(
        tokens,
        gain[None, :],
        *projections,
        *outputs,
        sink_logit,
        taps,
        conv_bias[None, :],
        documents.reshape(blocks, LANES),
        freq,
    )


def extended(cells, sides, width):
    for axis, dim in sides:
        count = lax.axis_size(axis)
        ends = count - 1
        head = lax.slice_in_dim(cells, 0, width, axis=dim)
        tail = lax.slice_in_dim(cells, cells.shape[dim] - width, cells.shape[dim], axis=dim)
        cells = jnp.concatenate(
            [
                lax.ppermute(tail, axis, [(i, (i + 1) % count) for i in range(ends)]),
                cells,
                lax.ppermute(head, axis, [((i + 1) % count, i) for i in range(ends)]),
            ],
            axis=dim,
        )
    return cells


def rotate(proj, positions, heads):
    rows = proj.shape[0]
    size = proj.shape[1] // heads
    half = size // 2
    freq = jnp.power(THETA, -(jnp.arange(half, dtype=jnp.float32) * (2.0 / size)))
    angle = positions.astype(jnp.float32)[:, None] * freq[None, :]
    cosine = jnp.cos(angle)[:, None, :]
    sine = jnp.sin(angle)[:, None, :]
    shaped = proj.reshape(rows, heads, size)
    first = shaped[..., :half]
    second = shaped[..., half:]
    turned = jnp.concatenate(
        [first * cosine - second * sine, second * cosine + first * sine], axis=-1
    )
    return turned.reshape(rows, heads * size)


def sink_softmax(scores, allowed, sinks):
    masked = jnp.where(allowed, scores, -jnp.inf)
    top = jnp.maximum(jnp.max(masked, axis=-1, keepdims=True), sinks)
    expo = jnp.exp(masked - top)
    return expo / (jnp.sum(expo, axis=-1, keepdims=True) + jnp.exp(sinks - top))


def local(
    tokens,
    gain,
    w_query,
    w_key,
    w_value,
    w_input,
    w_bgate,
    w_cgate,
    w_attn_out,
    w_conv_out,
    sink_logit,
    taps,
    conv_bias,
    documents,
):
    f32 = jnp.float32
    bf16 = jnp.bfloat16
    rows, part = tokens.shape
    tp_count = lax.axis_size("tp")
    sp_count = lax.axis_size("sp")
    width = part * tp_count
    head_dim = HEAD_DIM
    q_local = w_query.shape[1] // head_dim
    kv_local = w_key.shape[1] // head_dim
    groups = q_local // kv_local
    if fused_plan(
        lax.axis_size("grp"),
        sp_count,
        tp_count,
        rows,
        part,
        w_query.shape[0],
        w_attn_out.shape[0],
        w_query.shape[1],
        w_key.shape[1],
        w_input.shape[1],
    ):
        return fused_layer(
            tokens,
            gain,
            (w_key, w_value, w_cgate, w_input, w_bgate, w_query),
            (w_attn_out, w_conv_out),
            sink_logit,
            taps,
            conv_bias,
            documents,
            sp_count,
        )
    wq, wk, wv, wu, wb, wc, w_attn, w_conv = (
        lax.all_gather(w_query, "sp", axis=0, tiled=True),
        lax.all_gather(w_key, "sp", axis=0, tiled=True),
        lax.all_gather(w_value, "sp", axis=0, tiled=True),
        lax.all_gather(w_input, "sp", axis=0, tiled=True),
        lax.all_gather(w_bgate, "sp", axis=0, tiled=True),
        lax.all_gather(w_cgate, "sp", axis=0, tiled=True),
        lax.all_gather(w_attn_out, "sp", axis=0, tiled=True),
        lax.all_gather(w_conv_out, "sp", axis=0, tiled=True),
    )
    matrices = (wq, wk, wv, wu, wb, wc)
    piece_f = lax.all_gather(tokens, "tp", axis=1, tiled=True).astype(f32)
    scaled = (piece_f * gain[None, :]).astype(bf16)
    products = tuple((jnp.dot(scaled, mat, preferred_element_type=f32) for mat in matrices))
    folded = products + (jnp.sum(piece_f * piece_f, axis=1),)
    sums = folded[:6]
    squares = folded[6]
    inv = lax.rsqrt(squares / width + EPS)[:, None]
    q_acc, k_acc, v_acc, u_acc, b_acc, c_acc = sums
    positions = lax.axis_index("sp") * rows + jnp.arange(rows, dtype=jnp.int32)
    query = rotate(q_acc * inv, positions, q_local).astype(bf16)
    keys = rotate(k_acc * inv, positions, kv_local).astype(bf16)
    values = (v_acc * inv).astype(bf16)
    carried = (c_acc * inv * (u_acc * inv)).astype(bf16)
    bgate = b_acc * inv
    doc_col = documents.astype(f32).astype(bf16)[:, None]
    paired = jnp.concatenate([keys, values], axis=1)
    pair_ext, doc_ext = (
        extended(paired, (("sp", 0),), WINDOW),
        extended(doc_col, (("sp", 0),), WINDOW),
    )
    carry_ext, doc_near = (extended(carried, (("sp", 0),), 1), extended(doc_col, (("sp", 0),), 1))
    key_width = kv_local * head_dim
    key_ext = pair_ext[:, :key_width].reshape(-1, kv_local, head_dim)
    val_ext = pair_ext[:, key_width:].reshape(-1, kv_local, head_dim)
    key_doc = doc_ext[:, 0].astype(f32)
    own_doc = doc_col[:, 0].astype(f32)
    key_pos = positions[0] - WINDOW + jnp.arange(rows + 2 * WINDOW, dtype=jnp.int32)
    total = sp_count * rows
    sinks = sink_logit.reshape(kv_local, groups, 1, 1)
    block = rows // 2
    outputs = []
    for begin in range(0, rows, block):
        span = block + 2 * WINDOW
        q_block = query[begin : begin + block].reshape(block, kv_local, groups, head_dim)
        k_block = key_ext[begin : begin + span]
        v_block = val_ext[begin : begin + span]
        q_pos = positions[begin : begin + block]
        k_pos = key_pos[begin : begin + span]
        scores = jnp.einsum(
            "qhgd,khd->hgqk", q_block, k_block, preferred_element_type=f32
        ) * head_dim ** (-0.5)
        allowed = jnp.abs(q_pos[:, None] - k_pos[None, :]) <= WINDOW
        allowed = allowed & (
            own_doc[begin : begin + block, None] == key_doc[None, begin : begin + span]
        )
        allowed = allowed & (k_pos >= 0)[None, :] & (k_pos < total)[None, :]
        weight = sink_softmax(scores, allowed, sinks).astype(bf16)
        result = jnp.einsum("hgqk,khd->qhgd", weight, v_block, preferred_element_type=f32)
        outputs.append(result.astype(bf16).reshape(block, q_local * head_dim))
    attended = jnp.concatenate(outputs, axis=0)
    near_doc = doc_near[:, 0].astype(f32)
    conv = jnp.zeros((rows, carried.shape[1]), f32)
    for tap in range(3):
        same = (near_doc[tap : tap + rows] == near_doc[1 : rows + 1])[:, None]
        conv = conv + jnp.where(
            same, carry_ext[tap : tap + rows].astype(f32) * taps[tap][None, :], 0.0
        )
    convolved = (bgate * (conv + conv_bias[None, :])).astype(bf16)
    acc = jnp.dot(
        lax.all_gather(attended, "tp", axis=1, tiled=True), w_attn, preferred_element_type=f32
    )
    mixed = acc + jnp.dot(
        lax.all_gather(convolved, "tp", axis=1, tiled=True), w_conv, preferred_element_type=f32
    )
    return mixed.astype(bf16)


def solution(mesh):
    placed = (
        P(("grp", "sp"), "tp"),
        P(),
        P("sp", "tp"),
        P("sp", "tp"),
        P("sp", "tp"),
        P("sp", "tp"),
        P("sp", "tp"),
        P("sp", "tp"),
        P("sp", "tp"),
        P("sp", "tp"),
        P("tp"),
        P(None, "tp"),
        P("tp"),
        P(("grp", "sp")),
    )
    return jax.shard_map(
        local, mesh=mesh, in_specs=placed, out_specs=P(("grp", "sp"), "tp"), check_vma=False
    )
```

```python
import functools

import jax
import jax.numpy as jnp
import numpy as np
from jax import lax
from jax.experimental import pallas as pl
from jax.experimental.pallas import tpu as pltpu
from jax.sharding import PartitionSpec as P

HEAD_DIM = 64
WINDOW = 128


EPS = 1e-06
THETA = 500000.0
UNITS = (4, 4, 4, 4)
LAGS = (7, 6, 8, 6)
CHUNK = 256
LANES = 128


def fused_plan(grp_count, sp_count, tp_count, rows, part, proj_rows, out_rows, q_width, k_width, c_width):
    lines = sp_count // 2
    return (
        grp_count == 2
        and tp_count == 2
        and sp_count % 2 == 0
        and lines == 4
        and all(proj_rows % (2 * units * 16) == 0 for units in UNITS[:3])
        and UNITS[3] % 2 == 0
        and UNITS[3] <= UNITS[0]
        and out_rows % (UNITS[3] * 16) == 0
        and rows % CHUNK == 0
        and 3 * CHUNK <= rows <= 1024
        and CHUNK == 2 * WINDOW
        and WINDOW == LANES
        and part % 512 == 0
        and q_width == 4 * k_width
        and k_width == LANES
        and c_width % 256 == 0
        and 2 * HEAD_DIM == LANES
    )


def layer_kernel(
    sizes,
    tok_hbm,
    gain_hbm,
    wk_ref,
    wv_ref,
    wc_ref,
    wu_ref,
    wb_ref,
    wq_ref,
    wa_ref,
    wm_ref,
    sink_hbm,
    taps_hbm,
    bias_hbm,
    doc_hbm,
    freq_hbm,
    out_ref,
    gain_ref,
    sink_ref,
    taps_ref,
    bias_ref,
    doc_ref,
    freq_ref,
    wp_full,
    wo_full,
    tok_own,
    tok_other,
    scaled,
    inv_ref,
    acc_ref,
    pair_ext,
    query_s,
    carried,
    doc_row,
    doc_col,
    turn_ref,
    cos_ref,
    sin_ref,
    convolved,
    conv_other,
    attended,
    att_other,
    z_send,
    z_recv,
    y_send,
    y_recv,
    d_send,
    d_recv,
    x_send,
    x_recv,
    own_sem,
    tok_sem,
    small_sem,
    halo_send,
    halo_recv,
    conv_send,
    conv_recv,
    att_send,
    att_recv,
):
    lines, rp, ro = sizes
    f32 = jnp.float32
    bf16 = jnp.bfloat16
    rows, part = tok_own.shape
    k_width, c_width, q_width = wk_ref.shape[1], wc_ref.shape[1], wq_ref.shape[1]
    k_at = 3 * c_width
    q_at = k_at + 2 * k_width
    width = q_at + q_width
    chunks = rows // CHUNK
    blocks = rows // WINDOW
    order = (chunks - 1,) + tuple(range(chunks - 1))
    pieces = [(k * CHUNK, CHUNK) for k in order[:-1]]
    pieces += [(order[-1] * CHUNK, WINDOW), (order[-1] * CHUNK + WINDOW, WINDOW)]
    y = lax.axis_index("grp")
    sp = lax.axis_index("sp")
    x = lax.axis_index("tp")
    z, c = sp // 2, sp % 2
    counts = UNITS
    kinds = range(len(counts))
    fulls = (wp_full, wp_full, wp_full, wo_full)
    heights = (rp, rp, rp, ro)
    spans = ((k_at, width), (0, 2 * c_width), (2 * c_width, k_at), (0, 2 * part))
    first_unit, marks = (0, counts[0], counts[0] + counts[1], 0), [0]
    for count in counts:
        marks.append(marks[-1] + (lines - 1) * count)
    to_y = {"grp": 1 - y}
    to_core = {"sp": z * 2 + 1 - c}
    to_x = {"tp": 1 - x}
    to_z = ({"sp": sp + 2}, {"sp": sp - 2})
    has_next = (z < lines - 1, z > 0)

    def origin(way, t):
        return z - t if way == 0 else z + t

    def arrives(way, t):
        return z >= t if way == 0 else z < lines - t

    halves = counts[-1] // 2

    def place(g, j, zo, cc, h):
        size = heights[g]
        row = (zo * 2 + cc) * size + h * (size // 2)
        if g < 3:
            tall = size // 2 // counts[g]
            row = row + j * tall
            return fulls[g].at[pl.ds(pl.multiple_of(row, tall), tall), spans[g][0] : spans[g][1]]
        tall = size // 2 // halves
        row = row + j % halves * tall
        col = j // halves * part
        return fulls[g].at[
            pl.ds(pl.multiple_of(row, tall), tall), pl.ds(pl.multiple_of(col, part), part)
        ]

    def slot(g, j):
        return g if g < 3 else 3 + j // halves

    def remote(src, dst, send, recv, device):
        return pltpu.make_async_remote_copy(
            src_ref=src, dst_ref=dst, send_sem=send, recv_sem=recv,
            device_id=device, device_id_type=pl.DeviceIdType.MESH,
        )

    def z_copy(way, t, g, j):
        zo = origin(way, t)
        ref, u = place(g, j, zo, c, y), first_unit[g] + j
        return remote(ref, ref, z_send.at[way, g // 3], z_recv.at[zo - way, u], to_z[way])

    def y_copy(way, t, g, j, h):
        zo = origin(way, t)
        ref, u = place(g, j, zo, c, h), first_unit[g] + j
        return remote(ref, ref, y_send.at[g // 3], y_recv.at[zo - way, u], to_y)

    def d_copy(way, t, g, j, h):
        ref = place(g, j, origin(way, t), c, h)
        return remote(ref, ref, d_send.at[g // 3], d_recv.at[slot(g, j)], to_core)

    def d_all(n):
        at = slice(n % 3 * part, (n % 3 + 1) * part) if n >= 3 else slice(*spans[n])
        g = min(n, 3)
        ref = fulls[g].at[0 : lines * heights[g], at]
        return remote(ref, ref, d_send.at[g // 3], d_recv.at[n], to_core)

    def own_wait(full, size):
        ref = full.at[pl.ds(pl.multiple_of((z * 2 + c) * size, size), size), :]
        pltpu.make_async_copy(ref, ref, own_sem.at[0 if full is wp_full else 1]).wait()

    def own_d(n):
        g = min(n, 3)
        at = pl.ds(pl.multiple_of((z * 2 + c) * heights[g], heights[g]), heights[g])
        cols = slice(n % 3 * part, (n % 3 + 1) * part) if n >= 3 else slice(*spans[n])
        ref = fulls[g].at[at, cols]
        return remote(ref, ref, d_send.at[g // 3], d_recv.at[n], to_core)

    own_refs = ((wk_ref, wv_ref, wq_ref), (wc_ref, wu_ref), (wb_ref,), (wa_ref, wm_ref))

    def own_local(g):
        at, copies, col = pl.ds(pl.multiple_of((z * 2 + c) * heights[g], heights[g]), heights[g]), [], spans[g][0]
        for ref in own_refs[g]:
            size = ref.shape[1]
            copies.append(
                pltpu.make_async_copy(ref, fulls[g].at[at, col : col + size], own_sem.at[g // 3])
            )
            col += size
        return copies

    def tok_local(i):
        at = slice(pieces[i][0], sum(pieces[i]))
        return pltpu.make_async_copy(tok_hbm.at[at, :], tok_own.at[at, :], tok_sem.at[0])

    def x_copy(i):
        at = slice(pieces[i][0], sum(pieces[i]))
        return remote(tok_own.at[at, :], tok_other.at[at, :], x_send.at[0], x_recv.at[i], to_x)

    last = 2 * lines - 1
    steps_sp = (sp + 1, sp - 1)
    sends_to = (sp < last, sp > 0)
    gets_from = (sp > 0, sp < last)
    side = jnp.where(c == 0, sp - 1, sp + 1)
    has_side = (side >= 0) & (side <= last)
    edge = 16

    def halo(kind, way):
        if kind == 0:
            at = rows if way == 0 else WINDOW
            src = doc_row.at[:, at : at + WINDOW]
            at = 0 if way == 0 else WINDOW + rows
            dst = doc_row.at[:, at : at + WINDOW]
        elif kind == 1:
            at = rows if way == 0 else WINDOW
            src = pair_ext.at[at : at + WINDOW, :]
            at = 0 if way == 0 else WINDOW + rows
            dst = pair_ext.at[at : at + WINDOW, :]
        else:
            at = rows if way == 0 else edge
            src = carried.at[at : at + edge, :]
            at = 0 if way == 0 else edge + rows
            dst = carried.at[at : at + edge, :]
        return remote(
            src, dst, halo_send.at[kind, way], halo_recv.at[kind, way], {"sp": steps_sp[way]}
        )

    def start_halo(kind, way):
        @pl.when(sends_to[way])
        def _():
            halo(kind, way).start()

    def wait_halo(kind, way):
        @pl.when(gets_from[way])
        def _():
            halo(kind, way).wait_recv()

    tails = [(k * CHUNK, CHUNK) for k in range(chunks - 1)]
    tails += [(rows - CHUNK, WINDOW), (rows - WINDOW, WINDOW)]

    def conv_copy(i):
        at = slice(tails[i][0], sum(tails[i]))
        return remote(
            convolved.at[at, :], conv_other.at[at, :], conv_send.at[0], conv_recv.at[i], to_x
        )

    def att_copy(i):
        at = pl.ds(pl.multiple_of(i * WINDOW, WINDOW), WINDOW)
        return remote(attended.at[at, :], att_other.at[at, :], att_send.at[0], att_recv.at[0], to_x)

    def start_own(g):
        if g == 0 or g == 3:
            own_wait(fulls[g], heights[g])
        for j in range(counts[g]):
            for way in range(2):

                @pl.when(has_next[way])
                def _():
                    z_copy(way, 0, g, j).start()

        own_d(g).start()
        if g == 3:
            own_d(4).start()

    def z_event(g, m):
        t, j = m // counts[g] + 1, m % counts[g]
        for way in range(2):

            @pl.when(arrives(way, t))
            def _():
                z_copy(way, t, g, j).wait_recv()

                @pl.when(has_next[way] & (t < lines - 1))
                def _():
                    z_copy(way, t, g, j).start()

                y_copy(way, t, g, j, y).start()
                d_copy(way, t, g, j, y).start()

    def y_event(g, m):
        t, j = m // counts[g] + 1, m % counts[g]
        for way in range(2):

            @pl.when(arrives(way, t))
            def _():
                y_copy(way, t, g, j, 1 - y).wait_recv()
                d_copy(way, t, g, j, 1 - y).start()

    def on(n, act):
        if isinstance(n, int):
            g = max(i for i in kinds if marks[i] <= n)
            act(g, n - marks[g])
            return
        for g in kinds:

            @pl.when((n >= marks[g]) & (n < marks[g + 1]))
            def _():
                act(g, n - marks[g])

    state = [0, 0]

    costs = [heights[g] // counts[g] * (spans[g][1] - spans[g][0]) for g in kinds]
    unit_of = [g for g in kinds for _ in range((lines - 1) * counts[g])]
    ends = [sum(costs[g] for g in unit_of[: n + 1]) for n in range(marks[-1])]

    def due(m):
        if m >= marks[-1]:
            return m
        limit = ends[m] + LAGS[unit_of[m]] * costs[unit_of[m]]
        if limit > ends[-1]:
            return marks[-1]
        return max(n for n in range(marks[-1]) if ends[n] <= limit)

    def advance(goal):
        while state[0] < goal:
            on(state[0], z_event)
            state[0] += 1
            while due(state[1]) < state[0]:
                on(state[1], y_event)
                state[1] += 1

    def flush_to(goal):
        while state[1] < goal:
            on(state[1], y_event)
            state[1] += 1

    def flush(g):
        flush_to(marks[g + 1])

    def settle(g):
        advance(marks[g + 1])
        flush(g)
        d_all(g).wait_recv()

    def small(src, dst, i):
        return pltpu.make_async_copy(src, dst, small_sem.at[i])

    barrier = pltpu.get_barrier_semaphore()
    for device in (to_y, to_core, to_x):
        pl.semaphore_signal(barrier, inc=1, device_id=device, device_id_type=pl.DeviceIdType.MESH)
    for way in range(2):

        @pl.when(has_next[way])
        def _():
            pl.semaphore_signal(
                barrier, inc=1, device_id=to_z[way], device_id_type=pl.DeviceIdType.MESH
            )

    @pl.when(has_side)
    def _():
        pl.semaphore_signal(
            barrier, inc=1, device_id={"sp": side}, device_id_type=pl.DeviceIdType.MESH
        )

    for i in range(len(pieces)):
        tok_local(i).start()
    for g in kinds:
        for copy in own_local(g):
            copy.start()
    small(doc_hbm, doc_ref, 0).start()
    small(freq_hbm, freq_ref, 1).start()
    neighbours = jnp.where(has_side, 1, 0) + jnp.where(z > 0, 1, 0) + jnp.where(z < lines - 1, 1, 0) + 3
    with jax.named_scope("barrier"):
        pl.semaphore_wait(barrier, neighbours)

    pltpu.make_async_copy(tok_own, tok_own, tok_sem.at[0]).wait()
    for i in range(len(pieces)):
        x_copy(i).start()
    start_own(0)
    small(doc_hbm, doc_ref, 0).wait()
    small(gain_hbm, gain_ref, 0).start()
    small(freq_hbm, freq_ref, 1).wait()
    small(taps_hbm, taps_ref, 1).start()
    docs = doc_ref[...].astype(f32)
    for i in range(blocks):
        doc_row[:, (i + 1) * WINDOW : (i + 2) * WINDOW] = jnp.broadcast_to(
            docs[i : i + 1, :], (doc_row.shape[0], LANES)
        )

    @pl.when(sp == 0)
    def _():
        doc_row[:, :WINDOW] = jnp.full((doc_row.shape[0], WINDOW), -1.0, f32)
        pair_ext[:WINDOW, :] = jnp.zeros((WINDOW, pair_ext.shape[1]), bf16)

    @pl.when(sp == last)
    def _():
        doc_row[:, WINDOW + rows :] = jnp.full((doc_row.shape[0], WINDOW), -1.0, f32)
        pair_ext[WINDOW + rows :, :] = jnp.zeros((WINDOW, pair_ext.shape[1]), bf16)

    for i in range(blocks):
        at = slice(i * WINDOW, (i + 1) * WINDOW)
        doc_col[at, :] = jnp.broadcast_to(docs[i : i + 1, :], (WINDOW, LANES)).T

    tile = 32
    lane = lax.broadcasted_iota(jnp.int32, (tile, LANES), 1)
    step = lax.broadcasted_iota(jnp.int32, (tile, LANES), 0)
    freq = freq_ref[...]
    far = (sp * rows + step * tile).astype(f32) * freq
    near_angle = step.astype(f32) * freq
    turn_ref[0:tile, :] = jnp.cos(far)
    turn_ref[tile : 2 * tile, :] = jnp.sin(far)
    near_cos, near_sin = jnp.cos(near_angle), jnp.sin(near_angle)
    sign = jnp.where((lane % HEAD_DIM) < HEAD_DIM // 2, -1.0, 1.0)

    def table_body(i, carry):
        at = pl.ds(pl.multiple_of(i * tile, tile), tile)
        far_cos, far_sin = turn_ref[pl.ds(i, 1), :], turn_ref[pl.ds(tile + i, 1), :]
        cos_ref[at, :] = far_cos * near_cos - far_sin * near_sin
        sin_ref[at, :] = sign * (far_sin * near_cos + far_cos * near_sin)
        return carry

    lax.fori_loop(0, rows // tile, table_body, 0)
    for way in range(2):
        start_halo(0, way)
    small(gain_hbm, gain_ref, 0).wait()
    small(bias_hbm, bias_ref, 0).start()
    small(taps_hbm, taps_ref, 1).wait()
    small(sink_hbm, sink_ref, 1).start()
    small(bias_hbm, bias_ref, 0).wait()
    small(sink_hbm, sink_ref, 1).wait()

    mine_at = pl.multiple_of(x * part, part)
    yours_at = pl.multiple_of((1 - x) * part, part)

    def scale(piece):
        begin, size = pieces[piece]
        x_copy(piece).wait_recv()

        def body(i, carry):
            at = pl.ds(pl.multiple_of(begin + i * tile, tile), tile)
            own = tok_own[at, :].astype(f32)
            other = tok_other[at, :].astype(f32)
            total = jnp.sum(own * own, axis=1, keepdims=True) + jnp.sum(
                other * other, axis=1, keepdims=True
            )
            inv_ref[at, :] = jnp.broadcast_to(
                lax.rsqrt(total / (2 * part) + EPS), (tile, inv_ref.shape[1])
            )
            scaled[at, pl.ds(mine_at, part)] = (own * gain_ref[:, pl.ds(mine_at, part)]).astype(bf16)
            scaled[at, pl.ds(yours_at, part)] = (
                other * gain_ref[:, pl.ds(yours_at, part)]
            ).astype(bf16)
            return carry

        lax.fori_loop(0, size // tile, body, 0)

    cut = 256

    def project(mine, at):
        acc = jnp.dot(scaled[mine, :], wp_full[:, at], preferred_element_type=f32)
        return acc * inv_ref[mine, :1]

    lane_c = lax.broadcasted_iota(jnp.int32, (CHUNK, LANES), 1)
    low = (lane_c % HEAD_DIM) < HEAD_DIM // 2
    left = lane_c < HEAD_DIM

    def project_att(piece):
        begin, size = pieces[piece]
        mine = slice(begin, begin + size)
        ext = slice(WINDOW + begin, WINDOW + begin + size)

        def turned(cells):
            ahead = pltpu.roll(cells, LANES - HEAD_DIM // 2, 1)
            behind = pltpu.roll(cells, HEAD_DIM // 2, 1)
            return cells * cos_ref[mine, :] + jnp.where(low[:size], ahead, behind) * sin_ref[mine, :]

        cells = project(mine, slice(k_at, q_at))
        pair_ext[ext, :k_width] = turned(cells[:, :k_width]).astype(bf16)
        pair_ext[ext, k_width:] = cells[:, k_width:].astype(bf16)

        def query_body(j, carry):
            cells = project(mine, pl.ds(pl.multiple_of(q_at + j * cut, cut), cut))
            for i in range(cut // LANES):
                pair = turned(cells[:, i * LANES : (i + 1) * LANES]) * HEAD_DIM ** (-0.5)
                swapped = pltpu.roll(pair, HEAD_DIM, 1)
                own_half = left[:size] == (j == 0)
                first = jnp.where(own_half, jnp.where(j == 0, pair, swapped), 0.0)
                second = jnp.where(own_half, jnp.where(j == 0, swapped, pair), 0.0)
                at = pl.multiple_of((j * (cut // LANES) + i) * 2 * LANES, LANES)
                query_s[mine, pl.ds(at, LANES)] = first.astype(bf16)
                query_s[mine, pl.ds(at + LANES, LANES)] = second.astype(bf16)
            return carry

        for j in range(q_width // cut):
            query_body(j, 0)

    kv_heads = k_width // HEAD_DIM
    groups = q_width // HEAD_DIM // kv_heads
    span = 3 * WINDOW
    gap = lax.broadcasted_iota(jnp.int32, (WINDOW, span), 1) - lax.broadcasted_iota(
        jnp.int32, (WINDOW, span), 0
    )
    window = (gap >= 0) & (gap <= 2 * WINDOW)
    left_w = left[:WINDOW, :]

    def attend(i):
        at = pl.ds(pl.multiple_of(i * WINDOW, WINDOW), WINDOW)
        near = pl.ds(pl.multiple_of(i * WINDOW, WINDOW), span)
        allowed = window & (doc_col[at, 0:1] == doc_row[0:1, near])
        bias = jnp.where(allowed, 0.0, -jnp.inf)
        bias = jnp.concatenate([bias] * groups, axis=0)
        keys = pair_ext[near, :k_width]
        values = jnp.concatenate(
            [pair_ext[near, k_width:], jnp.ones((span, LANES), bf16)], axis=1
        )
        for head in range(kv_heads):
            first = head * groups
            stack = jnp.concatenate(
                [
                    query_s[at, (first + g) * LANES : (first + g + 1) * LANES]
                    for g in range(groups)
                ],
                axis=0,
            )
            sinks = jnp.concatenate(
                [jnp.full((WINDOW, 1), sink_ref[first + g], f32) for g in range(groups)], axis=0
            )
            scores = lax.dot_general(
                stack, keys, (((1,), (1,)), ((), ())), preferred_element_type=f32
            )
            scores = scores + bias
            top = jnp.maximum(jnp.max(scores, axis=1, keepdims=True), sinks)
            expo = jnp.exp(scores - top).astype(bf16)
            result = jnp.dot(expo, values, preferred_element_type=f32)
            total = result[:, LANES:] + jnp.exp(sinks - top)
            result = result[:, :LANES] * (1.0 / total)
            for g in range(0, groups, 2):
                one = result[g * WINDOW : (g + 1) * WINDOW]
                two = result[(g + 1) * WINDOW : (g + 2) * WINDOW]
                if head == 0:
                    pair = jnp.where(left_w, one, pltpu.roll(two, HEAD_DIM, 1))
                else:
                    pair = jnp.where(left_w, pltpu.roll(one, HEAD_DIM, 1), two)
                to = (first + g) * HEAD_DIM
                attended[at, to : to + LANES] = pair.astype(bf16)

    def attend_all(count, events, pick, guard=False):
        begin, lag = state

        def body(j, carry):
            if guard:
                with jax.named_scope("halo_wait"):
                    for way in range(2):

                        @pl.when(gets_from[way] & (j == way))
                        def _():
                            halo(1, way).wait_recv()

            with jax.named_scope("attend"):
                attend(pick(j))
                att_copy(pick(j)).start()
            with jax.named_scope("att_ev"):
                for e in range(events):
                    on(begin + j * events + e, z_event)
                    on(lag + j * events + e, y_event)
            return carry

        lax.fori_loop(0, count, body, 0)
        state[0] += count * events
        state[1] += count * events

    def carry_on(k):
        mine = slice(k * CHUNK, (k + 1) * CHUNK)
        ext = slice(edge + k * CHUNK, edge + (k + 1) * CHUNK)
        for j in range(c_width // cut):
            at = slice(j * cut, (j + 1) * cut)
            gate = project(mine, at)
            carried[ext, at] = (
                gate * project(mine, slice(c_width + j * cut, c_width + (j + 1) * cut))
            ).astype(bf16)

    row_c = lax.broadcasted_iota(jnp.int32, (CHUNK, LANES), 0)

    def convolve(k):
        begin, end = k * CHUNK, (k + 1) * CHUNK
        mine = slice(begin, end)
        docs_here = doc_col[mine, :]
        doc_before = jnp.where(
            row_c == 0,
            doc_row[0:1, WINDOW + begin - 1 : WINDOW + begin],
            pltpu.roll(docs_here, 1, 0),
        )
        doc_after = jnp.where(
            row_c == CHUNK - 1,
            doc_row[0:1, WINDOW + end : WINDOW + end + 1],
            pltpu.roll(docs_here, CHUNK - 1, 0),
        )
        for j in range(c_width // cut):
            gates = project(mine, slice(2 * c_width + j * cut, 2 * c_width + (j + 1) * cut))
            for i in range(cut // LANES):
                at = slice(j * cut + i * LANES, j * cut + (i + 1) * LANES)
                cells = carried[edge + begin : edge + end, at].astype(f32)
                head = carried[begin : begin + edge, at].astype(f32)
                foot = carried[edge + end : 2 * edge + end, at].astype(f32)
                before = jnp.where(row_c == 0, head[edge - 1 : edge, :], pltpu.roll(cells, 1, 0))
                after = jnp.where(row_c == CHUNK - 1, foot[0:1, :], pltpu.roll(cells, CHUNK - 1, 0))
                conv = jnp.where(doc_before == docs_here, before * taps_ref[0:1, at], 0.0)
                conv = conv + cells * taps_ref[1:2, at]
                conv = conv + jnp.where(doc_after == docs_here, after * taps_ref[2:3, at], 0.0)
                gate = gates[:, i * LANES : (i + 1) * LANES]
                convolved[mine, at] = (gate * (conv + bias_ref[:, at])).astype(bf16)

    def ahead_of(g):
        return marks[g + 1] - counts[g] + 1

    q_mine = pl.ds(pl.multiple_of(x * q_width, q_width), q_width)
    q_yours = pl.ds(pl.multiple_of((1 - x) * q_width, q_width), q_width)
    c_mine = pl.ds(pl.multiple_of(x * c_width, c_width), c_width)
    c_yours = pl.ds(pl.multiple_of((1 - x) * c_width, c_width), c_width)

    with jax.named_scope("adv_a"):
        advance(ahead_of(0))
        start_own(1)
        advance(marks[1] - 1)
    with jax.named_scope("scale_0"):
        scale(0)
    with jax.named_scope("adv_b"):
        advance(marks[1] + 3)
    with jax.named_scope("settle_0"):
        settle(0)
    with jax.named_scope("att_proj_0"):
        project_att(0)
        start_halo(1, 0)
    with jax.named_scope("adv_c"):
        advance(marks[1] + 7)
    with jax.named_scope("scale_1"):
        for i in range(1, len(pieces) - 2):
            scale(i)
    with jax.named_scope("att_proj_1"):
        project_att(1)
        start_halo(1, 1)
        for i in range(2, len(pieces) - 2):
            project_att(i)
    with jax.named_scope("adv_d"):
        advance(ahead_of(1))
        start_own(2)
        wait_halo(0, 0)
        wait_halo(0, 1)
    attend_all(2, 1, lambda j: j * (blocks - 1), True)
    with jax.named_scope("adv_e"):
        advance(marks[2] + 2)
    with jax.named_scope("scale_2"):
        scale(len(pieces) - 2)
    with jax.named_scope("att_proj_2"):
        project_att(len(pieces) - 2)
    with jax.named_scope("adv_e2"):
        advance(marks[2] + 5)
    attend_all(blocks - 5, 1, lambda j: j + 1)
    with jax.named_scope("scale_3"):
        scale(len(pieces) - 1)
    with jax.named_scope("adv_e3"):
        advance(marks[2] + 8)
        start_own(3)
    with jax.named_scope("att_proj_3"):
        project_att(len(pieces) - 1)
    attend_all(2, 2, lambda j: j + blocks - 4)
    attend_all(1, 0, lambda j: j + blocks - 2)
    with jax.named_scope("settle_1"):
        settle(1)
    with jax.named_scope("carry_0"):
        carry_on(order[0])
        start_halo(2, 0)
    with jax.named_scope("adv_f"):
        advance(marks[3] + 1)
    with jax.named_scope("carry_1"):
        carry_on(order[1])
        start_halo(2, 1)
    with jax.named_scope("adv_h"):
        advance(marks[3] + 2)
        flush(2)
    for k in order[2:]:
        with jax.named_scope("carry_2"):
            carry_on(k)
    with jax.named_scope("adv_i"):
        advance(marks[3] + 3)
    with jax.named_scope("settle_2"):
        settle(2)
    for k in range(chunks):
        with jax.named_scope("halo_2"):
            if k == 0:
                wait_halo(2, 0)
            if k == chunks - 1:
                wait_halo(2, 1)
        with jax.named_scope("convolve"):
            convolve(k)
            conv_copy(k).start()
            if k == chunks - 1:
                conv_copy(chunks).start()
        with jax.named_scope("adv_j"):
            advance(min(marks[4], marks[3] + 4 + k))
    with jax.named_scope("adv_k"):
        advance(marks[4])
        flush_to(marks[4] - counts[3] + halves)
    with jax.named_scope("settle_3"):
        d_all(3).wait_recv()
    with jax.named_scope("att_wait"):
        remote(attended, att_other, att_send.at[0], att_recv.at[0], to_x).wait_recv()

    def mix(begin, end):
        for j in range(begin, end):
            at = slice(j * cut, (j + 1) * cut)
            acc = jnp.dot(attended[...], wo_full[q_mine, at], preferred_element_type=f32)
            acc = acc + jnp.dot(att_other[...], wo_full[q_yours, at], preferred_element_type=f32)
            acc_ref[:, at] = acc

    cuts = part // cut
    for j in range(cuts):
        with jax.named_scope("mix"):
            mix(j, j + 1)
        with jax.named_scope("mix_ev"):
            flush_to(marks[4] - counts[3] + halves + (j + 1) * halves // cuts)
    with jax.named_scope("settle_4"):
        flush(3)
        d_all(4).wait_recv()

    def more_body(j, carry):
        at = pl.ds(pl.multiple_of(j * cut, cut), cut)
        late = pl.ds(pl.multiple_of(part + j * cut, cut), cut)
        acc_ref[:, at] = acc_ref[:, at] + jnp.dot(
            convolved[...], wo_full[c_mine, late], preferred_element_type=f32
        )
        return carry

    with jax.named_scope("more"):
        lax.fori_loop(0, cuts, more_body, 0)

    with jax.named_scope("sends"):
        for kind in range(3):
            for way in range(2):

                @pl.when(sends_to[way])
                def _():
                    halo(kind, way).wait_send()

        for n, (full, size) in enumerate(((wp_full, rp), (wo_full, ro))):
            ref = full.at[0 : lines * size, :]
            remote(ref, ref, d_send.at[n], d_recv.at[0], to_core).wait_send()
            ref = full.at[0 : (lines - 1) * size // 2, :]
            remote(ref, ref, y_send.at[n], y_recv.at[0, 0], to_y).wait_send()
            for way in range(2):
                for shards in range(1, lines):

                    @pl.when((z + 1 if way == 0 else lines - z) == shards)
                    def _():
                        ref = full.at[0 : shards * size // 2, :]
                        remote(ref, ref, z_send.at[way, n], z_recv.at[0, 0], to_z[way]).wait_send()

        remote(tok_own, tok_other, x_send.at[0], x_recv.at[0], to_x).wait_send()
        remote(attended, att_other, att_send.at[0], att_recv.at[0], to_x).wait_send()

    wide = 512
    for i, (begin, size) in enumerate(tails):
        mine = slice(begin, begin + size)
        with jax.named_scope("conv_wait"):
            conv_copy(i).wait_recv()

        with jax.named_scope("last"):
            for j in range(part // wide):
                at = slice(j * wide, (j + 1) * wide)
                acc = acc_ref[mine, at] + jnp.dot(
                    conv_other[mine, :],
                    wo_full[c_yours, part + j * wide : part + (j + 1) * wide],
                    preferred_element_type=f32,
                )
                out_ref[mine, at] = acc.astype(bf16)

    with jax.named_scope("end"):
        remote(convolved, conv_other, conv_send.at[0], conv_recv.at[0], to_x).wait_send()


def fused_layer(
    tokens, gain, projections, outputs, sink_logit, taps, conv_bias, documents, sp_count
):
    rows, part = tokens.shape
    f32 = jnp.float32
    bf16 = jnp.bfloat16
    lines = sp_count // 2
    wk, wv, wc, wu, wb, wq = projections
    width = sum(w.shape[1] for w in projections)
    rp, ro = wq.shape[0], outputs[0].shape[0]
    q_width, k_width, c_width = wq.shape[1], wk.shape[1], wc.shape[1]
    half = HEAD_DIM // 2
    freq = np.power(THETA, -(np.arange(half) / half))
    freq = jnp.asarray(np.tile(freq, LANES // half)[None, :], f32)
    chunks, blocks = rows // CHUNK, rows // WINDOW
    dma = pltpu.SemaphoreType.DMA
    hops = (lines - 1, sum(UNITS[:3]))
    kinds = len(UNITS)
    vmem = pl.BlockSpec(memory_space=pltpu.VMEM)
    hbm = pl.BlockSpec(memory_space=pl.ANY)
    flops = 2 * rows * 2 * part * width
    return pl.pallas_call(
        functools.partial(layer_kernel, (lines, rp, ro)),
        out_shape=pltpu.VMEM((rows, part), bf16),
        in_specs=[hbm] * 15,
        out_specs=vmem,
        scratch_shapes=[
            pltpu.VMEM((1, 2 * part), f32),
            pltpu.SMEM(sink_logit.shape, f32),
            pltpu.VMEM(taps.shape, f32),
            pltpu.VMEM((1, c_width), f32),
            pltpu.VMEM((blocks, LANES), jnp.int32),
            pltpu.VMEM((1, LANES), f32),
            pltpu.VMEM((rp * sp_count, width), bf16),
            pltpu.VMEM((ro * sp_count, 2 * part), bf16),
            pltpu.VMEM((rows, part), bf16),
            pltpu.VMEM((rows, part), bf16),
            pltpu.VMEM((rows, 2 * part), bf16),
            pltpu.VMEM((rows, LANES), f32),
            pltpu.VMEM((rows, part), f32),
            pltpu.VMEM((rows + 2 * WINDOW, 2 * k_width), bf16),
            pltpu.VMEM((rows, 2 * q_width), bf16),
            pltpu.VMEM((rows + 32, c_width), bf16),
            pltpu.VMEM((8, rows + 2 * WINDOW), f32),
            pltpu.VMEM((rows, LANES), f32),
            pltpu.VMEM((64, LANES), f32),
            pltpu.VMEM((rows, LANES), f32),
            pltpu.VMEM((rows, LANES), f32),
            pltpu.VMEM((rows, c_width), bf16),
            pltpu.VMEM((rows, c_width), bf16),
            pltpu.VMEM((rows, q_width), bf16),
            pltpu.VMEM((rows, q_width), bf16),
        ]
        + [dma((2, 2)), dma(hops), dma((2,)), dma(hops), dma((2,)), dma((kinds + 1,))]
        + [dma((1,)), dma((chunks + 1,)), dma((2,)), dma((1,)), dma((2,))]
        + [dma((3, 2)), dma((3, 2)), dma((1,)), dma((chunks + 1,)), dma((1,)), dma((1,))],
        compiler_params=pltpu.CompilerParams(
            collective_id=0, has_side_effects=True, vmem_limit_bytes=62 * 1024 * 1024
        ),
        cost_estimate=pl.CostEstimate(flops=flops, bytes_accessed=0, transcendentals=0),
        name="layer",
    )(
        tokens,
        gain[None, :],
        *projections,
        *outputs,
        sink_logit,
        taps,
        conv_bias[None, :],
        documents.reshape(blocks, LANES),
        freq,
    )


def extended(cells, sides, width):
    for axis, dim in sides:
        count = lax.axis_size(axis)
        ends = count - 1
        head = lax.slice_in_dim(cells, 0, width, axis=dim)
        tail = lax.slice_in_dim(cells, cells.shape[dim] - width, cells.shape[dim], axis=dim)
        cells = jnp.concatenate(
            [
                lax.ppermute(tail, axis, [(i, (i + 1) % count) for i in range(ends)]),
                cells,
                lax.ppermute(head, axis, [((i + 1) % count, i) for i in range(ends)]),
            ],
            axis=dim,
        )
    return cells


def rotate(proj, positions, heads):
    rows = proj.shape[0]
    size = proj.shape[1] // heads
    half = size // 2
    freq = jnp.power(THETA, -(jnp.arange(half, dtype=jnp.float32) * (2.0 / size)))
    angle = positions.astype(jnp.float32)[:, None] * freq[None, :]
    cosine = jnp.cos(angle)[:, None, :]
    sine = jnp.sin(angle)[:, None, :]
    shaped = proj.reshape(rows, heads, size)
    first = shaped[..., :half]
    second = shaped[..., half:]
    turned = jnp.concatenate(
        [first * cosine - second * sine, second * cosine + first * sine], axis=-1
    )
    return turned.reshape(rows, heads * size)


def sink_softmax(scores, allowed, sinks):
    masked = jnp.where(allowed, scores, -jnp.inf)
    top = jnp.maximum(jnp.max(masked, axis=-1, keepdims=True), sinks)
    expo = jnp.exp(masked - top)
    return expo / (jnp.sum(expo, axis=-1, keepdims=True) + jnp.exp(sinks - top))


def local(
    tokens,
    gain,
    w_query,
    w_key,
    w_value,
    w_input,
    w_bgate,
    w_cgate,
    w_attn_out,
    w_conv_out,
    sink_logit,
    taps,
    conv_bias,
    documents,
):
    f32 = jnp.float32
    bf16 = jnp.bfloat16
    rows, part = tokens.shape
    tp_count = lax.axis_size("tp")
    sp_count = lax.axis_size("sp")
    width = part * tp_count
    head_dim = HEAD_DIM
    q_local = w_query.shape[1] // head_dim
    kv_local = w_key.shape[1] // head_dim
    groups = q_local // kv_local
    if fused_plan(
        lax.axis_size("grp"),
        sp_count,
        tp_count,
        rows,
        part,
        w_query.shape[0],
        w_attn_out.shape[0],
        w_query.shape[1],
        w_key.shape[1],
        w_input.shape[1],
    ):
        return fused_layer(
            tokens,
            gain,
            (w_key, w_value, w_cgate, w_input, w_bgate, w_query),
            (w_attn_out, w_conv_out),
            sink_logit,
            taps,
            conv_bias,
            documents,
            sp_count,
        )
    wq, wk, wv, wu, wb, wc, w_attn, w_conv = (
        lax.all_gather(w_query, "sp", axis=0, tiled=True),
        lax.all_gather(w_key, "sp", axis=0, tiled=True),
        lax.all_gather(w_value, "sp", axis=0, tiled=True),
        lax.all_gather(w_input, "sp", axis=0, tiled=True),
        lax.all_gather(w_bgate, "sp", axis=0, tiled=True),
        lax.all_gather(w_cgate, "sp", axis=0, tiled=True),
        lax.all_gather(w_attn_out, "sp", axis=0, tiled=True),
        lax.all_gather(w_conv_out, "sp", axis=0, tiled=True),
    )
    matrices = (wq, wk, wv, wu, wb, wc)
    piece_f = lax.all_gather(tokens, "tp", axis=1, tiled=True).astype(f32)
    scaled = (piece_f * gain[None, :]).astype(bf16)
    products = tuple((jnp.dot(scaled, mat, preferred_element_type=f32) for mat in matrices))
    folded = products + (jnp.sum(piece_f * piece_f, axis=1),)
    sums = folded[:6]
    squares = folded[6]
    inv = lax.rsqrt(squares / width + EPS)[:, None]
    q_acc, k_acc, v_acc, u_acc, b_acc, c_acc = sums
    positions = lax.axis_index("sp") * rows + jnp.arange(rows, dtype=jnp.int32)
    query = rotate(q_acc * inv, positions, q_local).astype(bf16)
    keys = rotate(k_acc * inv, positions, kv_local).astype(bf16)
    values = (v_acc * inv).astype(bf16)
    carried = (c_acc * inv * (u_acc * inv)).astype(bf16)
    bgate = b_acc * inv
    doc_col = documents.astype(f32).astype(bf16)[:, None]
    paired = jnp.concatenate([keys, values], axis=1)
    pair_ext, doc_ext = (
        extended(paired, (("sp", 0),), WINDOW),
        extended(doc_col, (("sp", 0),), WINDOW),
    )
    carry_ext, doc_near = (extended(carried, (("sp", 0),), 1), extended(doc_col, (("sp", 0),), 1))
    key_width = kv_local * head_dim
    key_ext = pair_ext[:, :key_width].reshape(-1, kv_local, head_dim)
    val_ext = pair_ext[:, key_width:].reshape(-1, kv_local, head_dim)
    key_doc = doc_ext[:, 0].astype(f32)
    own_doc = doc_col[:, 0].astype(f32)
    key_pos = positions[0] - WINDOW + jnp.arange(rows + 2 * WINDOW, dtype=jnp.int32)
    total = sp_count * rows
    sinks = sink_logit.reshape(kv_local, groups, 1, 1)
    block = rows // 2
    outputs = []
    for begin in range(0, rows, block):
        span = block + 2 * WINDOW
        q_block = query[begin : begin + block].reshape(block, kv_local, groups, head_dim)
        k_block = key_ext[begin : begin + span]
        v_block = val_ext[begin : begin + span]
        q_pos = positions[begin : begin + block]
        k_pos = key_pos[begin : begin + span]
        scores = jnp.einsum(
            "qhgd,khd->hgqk", q_block, k_block, preferred_element_type=f32
        ) * head_dim ** (-0.5)
        allowed = jnp.abs(q_pos[:, None] - k_pos[None, :]) <= WINDOW
        allowed = allowed & (
            own_doc[begin : begin + block, None] == key_doc[None, begin : begin + span]
        )
        allowed = allowed & (k_pos >= 0)[None, :] & (k_pos < total)[None, :]
        weight = sink_softmax(scores, allowed, sinks).astype(bf16)
        result = jnp.einsum("hgqk,khd->qhgd", weight, v_block, preferred_element_type=f32)
        outputs.append(result.astype(bf16).reshape(block, q_local * head_dim))
    attended = jnp.concatenate(outputs, axis=0)
    near_doc = doc_near[:, 0].astype(f32)
    conv = jnp.zeros((rows, carried.shape[1]), f32)
    for tap in range(3):
        same = (near_doc[tap : tap + rows] == near_doc[1 : rows + 1])[:, None]
        conv = conv + jnp.where(
            same, carry_ext[tap : tap + rows].astype(f32) * taps[tap][None, :], 0.0
        )
    convolved = (bgate * (conv + conv_bias[None, :])).astype(bf16)
    acc = jnp.dot(
        lax.all_gather(attended, "tp", axis=1, tiled=True), w_attn, preferred_element_type=f32
    )
    mixed = acc + jnp.dot(
        lax.all_gather(convolved, "tp", axis=1, tiled=True), w_conv, preferred_element_type=f32
    )
    return mixed.astype(bf16)


def solution(mesh):
    placed = (
        P(("grp", "sp"), "tp"),
        P(),
        P("sp", "tp"),
        P("sp", "tp"),
        P("sp", "tp"),
        P("sp", "tp"),
        P("sp", "tp"),
        P("sp", "tp"),
        P("sp", "tp"),
        P("sp", "tp"),
        P("tp"),
        P(None, "tp"),
        P("tp"),
        P(("grp", "sp")),
    )
    return jax.shard_map(
        local, mesh=mesh, in_specs=placed, out_specs=P(("grp", "sp"), "tp"), check_vma=False
    )
```

```python
import functools

import jax
import jax.numpy as jnp
import numpy as np
from jax import lax
from jax.experimental import pallas as pl
from jax.experimental.pallas import tpu as pltpu
from jax.sharding import PartitionSpec as P

HEAD_DIM = 64
WINDOW = 128


EPS = 1e-06
THETA = 500000.0
UNITS = (4, 4, 4, 4)
LAGS = (7, 6, 8, 6)
CHUNK = 256
LANES = 128


def fused_plan(grp_count, sp_count, tp_count, rows, part, proj_rows, out_rows, q_width, k_width, c_width):
    lines = sp_count // 2
    return (
        grp_count == 2
        and tp_count == 2
        and sp_count % 2 == 0
        and lines == 4
        and all(proj_rows % (2 * units * 16) == 0 for units in UNITS[:3])
        and all(units % 2 == 0 for units in UNITS)
        and UNITS[3] <= UNITS[0]
        and out_rows % (UNITS[3] * 16) == 0
        and rows % CHUNK == 0
        and 3 * CHUNK <= rows <= 1024
        and CHUNK == 2 * WINDOW
        and WINDOW == LANES
        and part % 512 == 0
        and q_width == 4 * k_width
        and q_width + c_width == part
        and k_width == LANES
        and c_width % 256 == 0
        and 2 * HEAD_DIM == LANES
        and c_width % (16 * k_width // 8) == 0
    )


def layer_kernel(
    sizes,
    tok_hbm,
    gain_hbm,
    wk_ref,
    wv_ref,
    wc_ref,
    wu_ref,
    wb_ref,
    wq_ref,
    wa_ref,
    wm_ref,
    sink_hbm,
    taps_hbm,
    bias_hbm,
    doc_hbm,
    freq_hbm,
    out_ref,
    gain_ref,
    sink_ref,
    taps_ref,
    bias_ref,
    doc_ref,
    freq_ref,
    wp_full,
    wo_full,
    tok_own,
    tok_other,
    scaled,
    inv_ref,
    acc_ref,
    pair_ext,
    query_s,
    carried,
    doc_row,
    doc_col,
    turn_ref,
    cos_ref,
    sin_ref,
    convolved,
    conv_other,
    attended,
    att_other,
    z_send,
    z_recv,
    y_send,
    y_recv,
    d_send,
    d_recv,
    x_send,
    x_recv,
    own_sem,
    tok_sem,
    small_sem,
    halo_send,
    halo_recv,
    conv_recv,
    att_recv,
):
    lines, rp, ro = sizes
    f32 = jnp.float32
    bf16 = jnp.bfloat16
    rows, part = tok_own.shape
    k_width, c_width, q_width = wk_ref.shape[1], wc_ref.shape[1], wq_ref.shape[1]
    k_at = 3 * c_width
    q_at = k_at + 2 * k_width
    width = q_at + q_width
    chunks = rows // CHUNK
    blocks = rows // WINDOW
    order = (chunks - 1,) + tuple(range(chunks - 1))
    pieces = [(k * CHUNK, CHUNK) for k in order[:-1]]
    pieces += [(order[-1] * CHUNK, WINDOW), (order[-1] * CHUNK + WINDOW, WINDOW)]
    y = lax.axis_index("grp")
    sp = lax.axis_index("sp")
    x = lax.axis_index("tp")
    z, c = sp // 2, sp % 2
    counts = UNITS
    kinds = range(len(counts))
    fulls = (wp_full, wp_full, wp_full, wo_full)
    heights = (rp, rp, rp, ro)
    spans = ((k_at, width), (0, 2 * c_width), (2 * c_width, k_at), (0, 2 * part))
    first_unit, marks = (0, counts[0], counts[0] + counts[1], 0), [0]
    for count in counts:
        marks.append(marks[-1] + (lines - 1) * count)
    to_y = {"grp": 1 - y}
    to_core = {"sp": z * 2 + 1 - c}
    to_x = {"tp": 1 - x}
    to_z = ({"sp": sp + 2}, {"sp": sp - 2})
    has_next = (z < lines - 1, z > 0)

    def origin(way, t):
        return z - t if way == 0 else z + t

    def arrives(way, t):
        return z >= t if way == 0 else z < lines - t

    halves = counts[-1] // 2

    def place(g, j, zo, cc, h, n=1):
        size = heights[g]
        row = (zo * 2 + cc) * size + h * (size // 2)
        if g < 3:
            tall = size // 2 // counts[g]
            row = row + j * tall
            return fulls[g].at[pl.ds(pl.multiple_of(row, tall), n * tall), spans[g][0] : spans[g][1]]
        tall = size // 2 // halves
        row = row + j % halves * tall
        col = j // halves * part
        return fulls[g].at[
            pl.ds(pl.multiple_of(row, tall), n * tall), pl.ds(pl.multiple_of(col, part), part)
        ]

    def slot(g, j):
        return g if g < 3 else 3 + j // halves

    def remote(src, dst, send, recv, device):
        return pltpu.make_async_remote_copy(
            src_ref=src, dst_ref=dst, send_sem=send, recv_sem=recv,
            device_id=device, device_id_type=pl.DeviceIdType.MESH,
        )

    def z_copy(way, t, g, j):
        zo = origin(way, t)
        ref, u = place(g, j, zo, c, y), first_unit[g] + j
        return remote(ref, ref, z_send.at[way, g // 3], z_recv.at[zo - way, u], to_z[way])

    def y_copy(way, t, g, j, h, n=1):
        zo = origin(way, t)
        ref, u = place(g, j, zo, c, h, n), first_unit[g] + j
        return remote(ref, ref, y_send.at[g // 3], y_recv.at[zo - way, u // 2], to_y)

    def d_copy(way, t, g, j, h, n=1):
        ref = place(g, j, origin(way, t), c, h, n)
        return remote(ref, ref, d_send.at[g // 3], d_recv.at[slot(g, j)], to_core)

    def d_all(n):
        at = slice(n % 3 * part, (n % 3 + 1) * part) if n >= 3 else slice(*spans[n])
        g = min(n, 3)
        ref = fulls[g].at[0 : lines * heights[g], at]
        return remote(ref, ref, d_send.at[g // 3], d_recv.at[n], to_core)

    def own_wait(full, size):
        ref = full.at[pl.ds(pl.multiple_of((z * 2 + c) * size, size), size), :]
        pltpu.make_async_copy(ref, ref, own_sem.at[0 if full is wp_full else 1]).wait()

    def own_d(n):
        g = min(n, 3)
        at = pl.ds(pl.multiple_of((z * 2 + c) * heights[g], heights[g]), heights[g])
        cols = slice(n % 3 * part, (n % 3 + 1) * part) if n >= 3 else slice(*spans[n])
        ref = fulls[g].at[at, cols]
        return remote(ref, ref, d_send.at[g // 3], d_recv.at[n], to_core)

    own_refs = ((wk_ref, wv_ref, wq_ref), (wc_ref, wu_ref), (wb_ref,), (wa_ref, wm_ref))

    def own_local(g):
        at, copies, col = pl.ds(pl.multiple_of((z * 2 + c) * heights[g], heights[g]), heights[g]), [], spans[g][0]
        for ref in own_refs[g]:
            size = ref.shape[1]
            copies.append(
                pltpu.make_async_copy(ref, fulls[g].at[at, col : col + size], own_sem.at[g // 3])
            )
            col += size
        return copies

    def tok_local(i):
        at = slice(pieces[i][0], sum(pieces[i]))
        return pltpu.make_async_copy(tok_hbm.at[at, :], tok_own.at[at, :], tok_sem.at[0])

    def x_copy(i):
        at = slice(pieces[i][0], sum(pieces[i]))
        return remote(tok_own.at[at, :], tok_other.at[at, :], x_send.at[0], x_recv.at[i], to_x)

    last = 2 * lines - 1
    steps_sp = (sp + 1, sp - 1)
    sends_to = (sp < last, sp > 0)
    gets_from = (sp > 0, sp < last)
    side = jnp.where(c == 0, sp - 1, sp + 1)
    has_side = (side >= 0) & (side <= last)
    edge = 16

    def halo(kind, way):
        if kind == 0:
            at = rows if way == 0 else WINDOW
            src = doc_row.at[:, at : at + WINDOW]
            at = 0 if way == 0 else WINDOW + rows
            dst = doc_row.at[:, at : at + WINDOW]
        elif kind == 1:
            at = rows if way == 0 else WINDOW
            src = pair_ext.at[at : at + WINDOW, :]
            at = 0 if way == 0 else WINDOW + rows
            dst = pair_ext.at[at : at + WINDOW, :]
        else:
            at = rows if way == 0 else edge
            src = carried.at[at : at + edge, :]
            at = 0 if way == 0 else edge + rows
            dst = carried.at[at : at + edge, :]
        return remote(
            src, dst, halo_send.at[way], halo_recv.at[kind // 2, way], {"sp": steps_sp[way]}
        )

    def start_halo(kind, way):
        @pl.when(sends_to[way])
        def _():
            halo(kind, way).start()

    halo_bytes = [8 * WINDOW * 4, 2 * k_width * WINDOW * 2, edge * c_width * 2]
    halo_rows = [sum(halo_bytes[:2]) // (4 * k_width), sum(halo_bytes) // (4 * k_width)]

    def halo_all(kind, way, n):
        ref = pair_ext.at[0 : halo_rows[n], :]
        return remote(
            ref, ref, halo_send.at[way], halo_recv.at[kind // 2, way], {"sp": steps_sp[way]}
        )

    def wait_halo(kind, way):
        @pl.when(gets_from[way])
        def _():
            if kind == 2:
                halo(2, way).wait_recv()
            else:
                halo_all(0, way, 0).wait_recv()

    fold = c_width // 2

    def conv_copy(i):
        k = min(i, chunks - 1)
        at = slice(k * CHUNK, (k + 1) * CHUNK)
        cols = slice(0, c_width) if i < chunks - 1 else slice((i - k) * fold, (i - k + 1) * fold)
        return remote(
            convolved.at[at, cols], conv_other.at[at, cols], x_send.at[0], conv_recv.at[i], to_x
        )

    def att_copy(i):
        at = pl.ds(pl.multiple_of(i * WINDOW, WINDOW), WINDOW)
        return remote(attended.at[at, :], att_other.at[at, :], x_send.at[0], att_recv.at[0], to_x)

    def start_own(g):
        if g == 0 or g == 3:
            own_wait(fulls[g], heights[g])
        for j in range(counts[g]):
            for way in range(2):

                @pl.when(has_next[way])
                def _():
                    z_copy(way, 0, g, j).start()

        own_d(g).start()
        if g == 3:
            own_d(4).start()

    def z_event(g, m):
        t, j = m // counts[g] + 1, m % counts[g]
        for way in range(2):

            @pl.when(arrives(way, t))
            def _():
                z_copy(way, t, g, j).wait_recv()

                @pl.when(has_next[way] & (t < lines - 1))
                def _():
                    z_copy(way, t, g, j).start()

                y_copy(way, t, g, j, y).start()
                d_copy(way, t, g, j, y).start()

    def y_event(g, m):
        def pair():
            t, j = m // counts[g] + 1, m % counts[g] - 1
            for way in range(2):

                @pl.when(arrives(way, t))
                def _():
                    y_copy(way, t, g, j, 1 - y, 2).wait_recv()
                    d_copy(way, t, g, j, 1 - y, 2).start()

        if not isinstance(m, int):
            pl.when(m % 2 == 1)(pair)
        elif m % 2:
            pair()

    def on(n, act):
        if isinstance(n, int):
            g = max(i for i in kinds if marks[i] <= n)
            act(g, n - marks[g])
            return
        for g in kinds:

            @pl.when((n >= marks[g]) & (n < marks[g + 1]))
            def _():
                act(g, n - marks[g])

    state = [0, 0]

    costs = [heights[g] // counts[g] * (spans[g][1] - spans[g][0]) for g in kinds]
    unit_of = [g for g in kinds for _ in range((lines - 1) * counts[g])]
    ends = [sum(costs[g] for g in unit_of[: n + 1]) for n in range(marks[-1])]

    def due(m):
        if m >= marks[-1]:
            return m
        limit = ends[m] + LAGS[unit_of[m]] * costs[unit_of[m]]
        if limit > ends[-1]:
            return marks[-1]
        return max(n for n in range(marks[-1]) if ends[n] <= limit)

    def advance(goal):
        while state[0] < goal:
            on(state[0], z_event)
            state[0] += 1
            while due(state[1]) < state[0]:
                on(state[1], y_event)
                state[1] += 1

    def flush_to(goal):
        while state[1] < goal:
            on(state[1], y_event)
            state[1] += 1

    def flush(g):
        flush_to(marks[g + 1])

    def settle(g):
        advance(marks[g + 1])
        flush(g)
        d_all(g).wait_recv()

    def small(src, dst, i):
        return pltpu.make_async_copy(src, dst, small_sem.at[i])

    barrier = pltpu.get_barrier_semaphore()
    for device in (to_y, to_core, to_x):
        pl.semaphore_signal(barrier, inc=1, device_id=device, device_id_type=pl.DeviceIdType.MESH)
    for way in range(2):

        @pl.when(has_next[way])
        def _():
            pl.semaphore_signal(
                barrier, inc=1, device_id=to_z[way], device_id_type=pl.DeviceIdType.MESH
            )

    @pl.when(has_side)
    def _():
        pl.semaphore_signal(
            barrier, inc=1, device_id={"sp": side}, device_id_type=pl.DeviceIdType.MESH
        )

    for i in range(len(pieces)):
        tok_local(i).start()
    for g in kinds:
        for copy in own_local(g):
            copy.start()
    small(doc_hbm, doc_ref, 0).start()
    small(freq_hbm, freq_ref, 1).start()
    neighbours = jnp.where(has_side, 1, 0) + jnp.where(z > 0, 1, 0) + jnp.where(z < lines - 1, 1, 0) + 3
    with jax.named_scope("barrier"):
        pl.semaphore_wait(barrier, neighbours)

    pltpu.make_async_copy(tok_own, tok_own, tok_sem.at[0]).wait()
    for i in range(len(pieces)):
        x_copy(i).start()
    start_own(0)
    small(doc_hbm, doc_ref, 0).wait()
    small(gain_hbm, gain_ref, 0).start()
    small(freq_hbm, freq_ref, 1).wait()
    small(taps_hbm, taps_ref, 1).start()
    docs = doc_ref[...].astype(f32)
    for i in range(blocks):
        doc_row[:, (i + 1) * WINDOW : (i + 2) * WINDOW] = jnp.broadcast_to(
            docs[i : i + 1, :], (doc_row.shape[0], LANES)
        )

    @pl.when(sp == 0)
    def _():
        doc_row[:, :WINDOW] = jnp.full((doc_row.shape[0], WINDOW), -1.0, f32)
        pair_ext[:WINDOW, :] = jnp.zeros((WINDOW, pair_ext.shape[1]), bf16)

    @pl.when(sp == last)
    def _():
        doc_row[:, WINDOW + rows :] = jnp.full((doc_row.shape[0], WINDOW), -1.0, f32)
        pair_ext[WINDOW + rows :, :] = jnp.zeros((WINDOW, pair_ext.shape[1]), bf16)

    for i in range(blocks):
        at = slice(i * WINDOW, (i + 1) * WINDOW)
        doc_col[at, :] = jnp.broadcast_to(docs[i : i + 1, :], (WINDOW, LANES)).T

    tile = 32
    lane = lax.broadcasted_iota(jnp.int32, (tile, LANES), 1)
    step = lax.broadcasted_iota(jnp.int32, (tile, LANES), 0)
    freq = freq_ref[...]
    far = (sp * rows + step * tile).astype(f32) * freq
    near_angle = step.astype(f32) * freq
    turn_ref[0:tile, :] = jnp.cos(far)
    turn_ref[tile : 2 * tile, :] = jnp.sin(far)
    near_cos, near_sin = jnp.cos(near_angle), jnp.sin(near_angle)
    sign = jnp.where((lane % HEAD_DIM) < HEAD_DIM // 2, -1.0, 1.0)

    def table_body(i, carry):
        at = pl.ds(pl.multiple_of(i * tile, tile), tile)
        far_cos, far_sin = turn_ref[pl.ds(i, 1), :], turn_ref[pl.ds(tile + i, 1), :]
        cos_ref[at, :] = far_cos * near_cos - far_sin * near_sin
        sin_ref[at, :] = sign * (far_sin * near_cos + far_cos * near_sin)
        return carry

    lax.fori_loop(0, rows // tile, table_body, 0)
    for way in range(2):
        start_halo(0, way)
    small(gain_hbm, gain_ref, 0).wait()
    small(bias_hbm, bias_ref, 0).start()
    small(taps_hbm, taps_ref, 1).wait()
    small(sink_hbm, sink_ref, 1).start()
    small(bias_hbm, bias_ref, 0).wait()
    small(sink_hbm, sink_ref, 1).wait()

    mine_at = pl.multiple_of(x * part, part)
    yours_at = pl.multiple_of((1 - x) * part, part)

    def scale(piece):
        begin, size = pieces[piece]
        x_copy(piece).wait_recv()

        def body(i, carry):
            at = pl.ds(pl.multiple_of(begin + i * tile, tile), tile)
            own = tok_own[at, :].astype(f32)
            other = tok_other[at, :].astype(f32)
            total = jnp.sum(own * own, axis=1, keepdims=True) + jnp.sum(
                other * other, axis=1, keepdims=True
            )
            inv_ref[at, :] = jnp.broadcast_to(
                lax.rsqrt(total / (2 * part) + EPS), (tile, inv_ref.shape[1])
            )
            scaled[at, pl.ds(mine_at, part)] = (own * gain_ref[:, pl.ds(mine_at, part)]).astype(bf16)
            scaled[at, pl.ds(yours_at, part)] = (
                other * gain_ref[:, pl.ds(yours_at, part)]
            ).astype(bf16)
            return carry

        lax.fori_loop(0, size // tile, body, 0)

    cut = 256

    def project(mine, at):
        acc = jnp.dot(scaled[mine, :], wp_full[:, at], preferred_element_type=f32)
        return acc * inv_ref[mine, :1]

    lane_c = lax.broadcasted_iota(jnp.int32, (CHUNK, LANES), 1)
    low = (lane_c % HEAD_DIM) < HEAD_DIM // 2
    left = lane_c < HEAD_DIM

    def project_att(piece):
        begin, size = pieces[piece]
        mine = slice(begin, begin + size)
        ext = slice(WINDOW + begin, WINDOW + begin + size)

        def turned(cells):
            ahead = pltpu.roll(cells, LANES - HEAD_DIM // 2, 1)
            behind = pltpu.roll(cells, HEAD_DIM // 2, 1)
            return cells * cos_ref[mine, :] + jnp.where(low[:size], ahead, behind) * sin_ref[mine, :]

        cells = project(mine, slice(k_at, q_at))
        pair_ext[ext, :k_width] = turned(cells[:, :k_width]).astype(bf16)
        pair_ext[ext, k_width:] = cells[:, k_width:].astype(bf16)

        def query_body(j, carry):
            cells = project(mine, pl.ds(pl.multiple_of(q_at + j * cut, cut), cut))
            for i in range(cut // LANES):
                pair = turned(cells[:, i * LANES : (i + 1) * LANES]) * HEAD_DIM ** (-0.5)
                swapped = pltpu.roll(pair, HEAD_DIM, 1)
                own_half = left[:size] == (j == 0)
                first = jnp.where(own_half, jnp.where(j == 0, pair, swapped), 0.0)
                second = jnp.where(own_half, jnp.where(j == 0, swapped, pair), 0.0)
                at = pl.multiple_of((j * (cut // LANES) + i) * 2 * LANES, LANES)
                query_s[mine, pl.ds(at, LANES)] = first.astype(bf16)
                query_s[mine, pl.ds(at + LANES, LANES)] = second.astype(bf16)
            return carry

        for j in range(q_width // cut):
            query_body(j, 0)

    kv_heads = k_width // HEAD_DIM
    groups = q_width // HEAD_DIM // kv_heads
    span = 3 * WINDOW
    gap = lax.broadcasted_iota(jnp.int32, (WINDOW, span), 1) - lax.broadcasted_iota(
        jnp.int32, (WINDOW, span), 0
    )
    window = (gap >= 0) & (gap <= 2 * WINDOW)
    left_w = left[:WINDOW, :]

    def attend(i):
        at = pl.ds(pl.multiple_of(i * WINDOW, WINDOW), WINDOW)
        near = pl.ds(pl.multiple_of(i * WINDOW, WINDOW), span)
        allowed = window & (doc_col[at, 0:1] == doc_row[0:1, near])
        bias = jnp.where(allowed, 0.0, -jnp.inf)
        bias = jnp.concatenate([bias] * groups, axis=0)
        keys = pair_ext[near, :k_width]
        values = jnp.concatenate(
            [pair_ext[near, k_width:], jnp.ones((span, LANES), bf16)], axis=1
        )
        for head in range(kv_heads):
            first = head * groups
            stack = jnp.concatenate(
                [
                    query_s[at, (first + g) * LANES : (first + g + 1) * LANES]
                    for g in range(groups)
                ],
                axis=0,
            )
            sinks = jnp.concatenate(
                [jnp.full((WINDOW, 1), sink_ref[first + g], f32) for g in range(groups)], axis=0
            )
            scores = lax.dot_general(
                stack, keys, (((1,), (1,)), ((), ())), preferred_element_type=f32
            )
            scores = scores + bias
            top = jnp.maximum(jnp.max(scores, axis=1, keepdims=True), sinks)
            expo = jnp.exp(scores - top).astype(bf16)
            result = jnp.dot(expo, values, preferred_element_type=f32)
            total = result[:, LANES:] + jnp.exp(sinks - top)
            result = result[:, :LANES] * (1.0 / total)
            for g in range(0, groups, 2):
                one = result[g * WINDOW : (g + 1) * WINDOW]
                two = result[(g + 1) * WINDOW : (g + 2) * WINDOW]
                if head == 0:
                    pair = jnp.where(left_w, one, pltpu.roll(two, HEAD_DIM, 1))
                else:
                    pair = jnp.where(left_w, pltpu.roll(one, HEAD_DIM, 1), two)
                to = (first + g) * HEAD_DIM
                attended[at, to : to + LANES] = pair.astype(bf16)

    def attend_all(count, events, pick, guard=False):
        begin, lag = state

        def body(j, carry):
            if guard:
                with jax.named_scope("halo_wait"):
                    for way in range(2):

                        @pl.when(gets_from[way] & (j == way))
                        def _():
                            halo_all(0, way, 0).wait_recv()

            with jax.named_scope("attend"):
                attend(pick(j))
                att_copy(pick(j)).start()
            with jax.named_scope("att_ev"):
                for e in range(events):
                    on(begin + j * events + e, z_event)
                    on(lag + j * events + e, y_event)
            return carry

        lax.fori_loop(0, count, body, 0)
        state[0] += count * events
        state[1] += count * events

    def carry_on(k):
        mine = slice(k * CHUNK, (k + 1) * CHUNK)
        ext = slice(edge + k * CHUNK, edge + (k + 1) * CHUNK)
        for j in range(c_width // cut):
            at = slice(j * cut, (j + 1) * cut)
            gate = project(mine, at)
            carried[ext, at] = (
                gate * project(mine, slice(c_width + j * cut, c_width + (j + 1) * cut))
            ).astype(bf16)

    row_c = lax.broadcasted_iota(jnp.int32, (CHUNK, LANES), 0)

    def convolve(k):
        begin, end = k * CHUNK, (k + 1) * CHUNK
        mine = slice(begin, end)
        docs_here = doc_col[mine, :]
        doc_before = jnp.where(
            row_c == 0,
            doc_row[0:1, WINDOW + begin - 1 : WINDOW + begin],
            pltpu.roll(docs_here, 1, 0),
        )
        doc_after = jnp.where(
            row_c == CHUNK - 1,
            doc_row[0:1, WINDOW + end : WINDOW + end + 1],
            pltpu.roll(docs_here, CHUNK - 1, 0),
        )
        for j in range(c_width // cut):
            gates = project(mine, slice(2 * c_width + j * cut, 2 * c_width + (j + 1) * cut))
            for i in range(cut // LANES):
                at = slice(j * cut + i * LANES, j * cut + (i + 1) * LANES)
                cells = carried[edge + begin : edge + end, at].astype(f32)
                head = carried[begin : begin + edge, at].astype(f32)
                foot = carried[edge + end : 2 * edge + end, at].astype(f32)
                before = jnp.where(row_c == 0, head[edge - 1 : edge, :], pltpu.roll(cells, 1, 0))
                after = jnp.where(row_c == CHUNK - 1, foot[0:1, :], pltpu.roll(cells, CHUNK - 1, 0))
                conv = jnp.where(doc_before == docs_here, before * taps_ref[0:1, at], 0.0)
                conv = conv + cells * taps_ref[1:2, at]
                conv = conv + jnp.where(doc_after == docs_here, after * taps_ref[2:3, at], 0.0)
                gate = gates[:, i * LANES : (i + 1) * LANES]
                convolved[mine, at] = (gate * (conv + bias_ref[:, at])).astype(bf16)

    def ahead_of(g):
        return marks[g + 1] - counts[g] + 1

    q_mine = pl.ds(pl.multiple_of(x * q_width, q_width), q_width)
    q_yours = pl.ds(pl.multiple_of((1 - x) * q_width, q_width), q_width)
    c_mine = pl.ds(pl.multiple_of(x * c_width, c_width), c_width)
    c_yours = pl.ds(pl.multiple_of((1 - x) * c_width, c_width), c_width)

    with jax.named_scope("adv_a"):
        advance(ahead_of(0))
        start_own(1)
        advance(marks[1] - 1)
    with jax.named_scope("scale_0"):
        scale(0)
    with jax.named_scope("adv_b"):
        advance(marks[1] + 3)
    with jax.named_scope("settle_0"):
        settle(0)
    with jax.named_scope("att_proj_0"):
        project_att(0)
        start_halo(1, 0)
    with jax.named_scope("adv_c"):
        advance(marks[1] + 7)
    with jax.named_scope("scale_1"):
        for i in range(1, len(pieces) - 2):
            scale(i)
    with jax.named_scope("att_proj_1"):
        project_att(1)
        start_halo(1, 1)
        for i in range(2, len(pieces) - 2):
            project_att(i)
    with jax.named_scope("adv_d"):
        advance(ahead_of(1))
        start_own(2)
    attend_all(2, 1, lambda j: j * (blocks - 1), True)
    with jax.named_scope("adv_e"):
        advance(marks[2] + 2)
    with jax.named_scope("scale_2"):
        scale(len(pieces) - 2)
    with jax.named_scope("att_proj_2"):
        project_att(len(pieces) - 2)
    with jax.named_scope("adv_e2"):
        advance(marks[2] + 5)
    attend_all(blocks - 5, 1, lambda j: j + 1)
    with jax.named_scope("scale_3"):
        scale(len(pieces) - 1)
    with jax.named_scope("adv_e3"):
        advance(marks[2] + 8)
        start_own(3)
    with jax.named_scope("att_proj_3"):
        project_att(len(pieces) - 1)
    attend_all(2, 2, lambda j: j + blocks - 4)
    attend_all(1, 0, lambda j: j + blocks - 2)
    with jax.named_scope("settle_1"):
        settle(1)
    with jax.named_scope("carry_0"):
        carry_on(order[0])
        start_halo(2, 0)
    with jax.named_scope("adv_f"):
        advance(marks[3] + 1)
    with jax.named_scope("carry_1"):
        carry_on(order[1])
        start_halo(2, 1)
    with jax.named_scope("adv_h"):
        advance(marks[3] + 2)
        flush(2)
    for k in order[2:]:
        with jax.named_scope("carry_2"):
            carry_on(k)
    with jax.named_scope("adv_i"):
        advance(marks[3] + 3)
    with jax.named_scope("settle_2"):
        settle(2)
    for k in range(chunks):
        with jax.named_scope("halo_2"):
            if k == 0:
                wait_halo(2, 0)
            if k == chunks - 1:
                wait_halo(2, 1)
        with jax.named_scope("convolve"):
            convolve(k)
            if k < chunks - 1:

                @pl.when(c == 0)
                def _():
                    conv_copy(k).start()

            else:

                @pl.when(c == 1)
                def _():
                    for i in range(k):
                        conv_copy(i).start()

                conv_copy(k).start()
                conv_copy(chunks).start()
        with jax.named_scope("adv_j"):
            advance(min(marks[4], marks[3] + 4 + k))
    with jax.named_scope("adv_k"):
        advance(marks[4])
        flush_to(marks[4] - counts[3] + halves)
    with jax.named_scope("settle_3"):
        d_all(3).wait_recv()
    with jax.named_scope("att_wait"):
        remote(attended, att_other, x_send.at[0], att_recv.at[0], to_x).wait_recv()

    def mix(begin, end):
        for j in range(begin, end):
            at = slice(j * cut, (j + 1) * cut)
            acc = jnp.dot(attended[...], wo_full[q_mine, at], preferred_element_type=f32)
            acc = acc + jnp.dot(att_other[...], wo_full[q_yours, at], preferred_element_type=f32)
            acc_ref[:, at] = acc

    cuts = part // cut
    for j in range(cuts):
        with jax.named_scope("mix"):
            mix(j, j + 1)
        with jax.named_scope("mix_ev"):
            flush_to(marks[4] - counts[3] + halves + (j + 1) * halves // cuts)
    with jax.named_scope("settle_4"):
        flush(3)
        d_all(4).wait_recv()

    with jax.named_scope("sends"):
        for way in range(2):

            @pl.when(sends_to[way])
            def _():
                halo_all(0, way, 1).wait_send()

        for n, (full, size) in enumerate(((wp_full, rp), (wo_full, ro))):
            ref = full.at[0 : lines * size, :]
            remote(ref, ref, d_send.at[n], d_recv.at[0], to_core).wait_send()
            ref = full.at[0 : (lines - 1) * size // 2, :]
            remote(ref, ref, y_send.at[n], y_recv.at[0, 0], to_y).wait_send()
            for way in range(2):
                for shards in range(1, lines):

                    @pl.when((z + 1 if way == 0 else lines - z) == shards)
                    def _():
                        ref = full.at[0 : shards * size // 2, :]
                        remote(ref, ref, z_send.at[way, n], z_recv.at[0, 0], to_z[way]).wait_send()


    wide = 512

    def own_part(mine, at, late):
        acc = jnp.dot(convolved[mine, :], wo_full[c_mine, late], preferred_element_type=f32)
        return acc_ref[mine, at] + acc

    for i in range(chunks + 1):
        k = min(i, chunks - 1)
        mine = slice(k * CHUNK, (k + 1) * CHUNK)
        part_of = slice(0, c_width) if i < chunks - 1 else slice((i - k) * fold, (i - k + 1) * fold)
        size = part_of.stop - part_of.start
        rows_of = pl.ds(pl.multiple_of((1 - x) * c_width + part_of.start, size), size)
        if i == chunks - 1:
            with jax.named_scope("more"):
                for j in range(part // wide):
                    at, late = slice(j * wide, (j + 1) * wide), slice(part + j * wide, part + (j + 1) * wide)
                    acc_ref[mine, at] = own_part(mine, at, late)
        with jax.named_scope("conv_wait"):
            conv_copy(i).wait_recv()

        with jax.named_scope("last"):
            for j in range(part // wide):
                at, late = slice(j * wide, (j + 1) * wide), slice(part + j * wide, part + (j + 1) * wide)
                acc = own_part(mine, at, late) if i < chunks - 1 else acc_ref[mine, at]
                acc = acc + jnp.dot(
                    conv_other[mine, part_of], wo_full[rows_of, late], preferred_element_type=f32
                )
                if i == chunks - 1:
                    acc_ref[mine, at] = acc
                else:
                    out_ref[mine, at] = acc.astype(bf16)

    with jax.named_scope("end"):
        remote(scaled, scaled, x_send.at[0], x_recv.at[0], to_x).wait_send()


def fused_layer(
    tokens, gain, projections, outputs, sink_logit, taps, conv_bias, documents, sp_count
):
    rows, part = tokens.shape
    f32 = jnp.float32
    bf16 = jnp.bfloat16
    lines = sp_count // 2
    wk, wv, wc, wu, wb, wq = projections
    width = sum(w.shape[1] for w in projections)
    rp, ro = wq.shape[0], outputs[0].shape[0]
    q_width, k_width, c_width = wq.shape[1], wk.shape[1], wc.shape[1]
    half = HEAD_DIM // 2
    freq = np.power(THETA, -(np.arange(half) / half))
    freq = jnp.asarray(np.tile(freq, LANES // half)[None, :], f32)
    chunks, blocks = rows // CHUNK, rows // WINDOW
    dma = pltpu.SemaphoreType.DMA
    hops, joint = (lines - 1, sum(UNITS[:3])), (lines - 1, sum(UNITS[:3]) // 2)
    kinds = len(UNITS)
    vmem = pl.BlockSpec(memory_space=pltpu.VMEM)
    hbm = pl.BlockSpec(memory_space=pl.ANY)
    flops = 2 * rows * 2 * part * width
    return pl.pallas_call(
        functools.partial(layer_kernel, (lines, rp, ro)),
        out_shape=pltpu.VMEM((rows, part), bf16),
        in_specs=[hbm] * 15,
        out_specs=vmem,
        scratch_shapes=[
            pltpu.VMEM((1, 2 * part), f32),
            pltpu.SMEM(sink_logit.shape, f32),
            pltpu.VMEM(taps.shape, f32),
            pltpu.VMEM((1, c_width), f32),
            pltpu.VMEM((blocks, LANES), jnp.int32),
            pltpu.VMEM((1, LANES), f32),
            pltpu.VMEM((rp * sp_count, width), bf16),
            pltpu.VMEM((ro * sp_count, 2 * part), bf16),
            pltpu.VMEM((rows, part), bf16),
            pltpu.VMEM((rows, part), bf16),
            pltpu.VMEM((rows, 2 * part), bf16),
            pltpu.VMEM((rows, LANES), f32),
            pltpu.VMEM((rows, part), f32),
            pltpu.VMEM((rows + 2 * WINDOW, 2 * k_width), bf16),
            pltpu.VMEM((rows, 2 * q_width), bf16),
            pltpu.VMEM((rows + 32, c_width), bf16),
            pltpu.VMEM((8, rows + 2 * WINDOW), f32),
            pltpu.VMEM((rows, LANES), f32),
            pltpu.VMEM((64, LANES), f32),
            pltpu.VMEM((rows, LANES), f32),
            pltpu.VMEM((rows, LANES), f32),
            pltpu.VMEM((rows, c_width), bf16),
            pltpu.VMEM((rows, c_width), bf16),
            pltpu.VMEM((rows, q_width), bf16),
            pltpu.VMEM((rows, q_width), bf16),
        ]
        + [dma((2, 2)), dma(hops), dma((2,)), dma(joint), dma((2,)), dma((kinds + 1,))]
        + [dma((1,)), dma((chunks + 1,)), dma((2,)), dma((1,)), dma((2,))]
        + [dma((2,)), dma((2, 2)), dma((chunks + 1,)), dma((1,))],
        compiler_params=pltpu.CompilerParams(
            collective_id=0, has_side_effects=True, vmem_limit_bytes=62 * 1024 * 1024
        ),
        cost_estimate=pl.CostEstimate(flops=flops, bytes_accessed=0, transcendentals=0),
        name="layer",
    )(
        tokens,
        gain[None, :],
        *projections,
        *outputs,
        sink_logit,
        taps,
        conv_bias[None, :],
        documents.reshape(blocks, LANES),
        freq,
    )


def extended(cells, sides, width):
    for axis, dim in sides:
        count = lax.axis_size(axis)
        ends = count - 1
        head = lax.slice_in_dim(cells, 0, width, axis=dim)
        tail = lax.slice_in_dim(cells, cells.shape[dim] - width, cells.shape[dim], axis=dim)
        cells = jnp.concatenate(
            [
                lax.ppermute(tail, axis, [(i, (i + 1) % count) for i in range(ends)]),
                cells,
                lax.ppermute(head, axis, [((i + 1) % count, i) for i in range(ends)]),
            ],
            axis=dim,
        )
    return cells


def rotate(proj, positions, heads):
    rows = proj.shape[0]
    size = proj.shape[1] // heads
    half = size // 2
    freq = jnp.power(THETA, -(jnp.arange(half, dtype=jnp.float32) * (2.0 / size)))
    angle = positions.astype(jnp.float32)[:, None] * freq[None, :]
    cosine = jnp.cos(angle)[:, None, :]
    sine = jnp.sin(angle)[:, None, :]
    shaped = proj.reshape(rows, heads, size)
    first = shaped[..., :half]
    second = shaped[..., half:]
    turned = jnp.concatenate(
        [first * cosine - second * sine, second * cosine + first * sine], axis=-1
    )
    return turned.reshape(rows, heads * size)


def sink_softmax(scores, allowed, sinks):
    masked = jnp.where(allowed, scores, -jnp.inf)
    top = jnp.maximum(jnp.max(masked, axis=-1, keepdims=True), sinks)
    expo = jnp.exp(masked - top)
    return expo / (jnp.sum(expo, axis=-1, keepdims=True) + jnp.exp(sinks - top))


def local(
    tokens,
    gain,
    w_query,
    w_key,
    w_value,
    w_input,
    w_bgate,
    w_cgate,
    w_attn_out,
    w_conv_out,
    sink_logit,
    taps,
    conv_bias,
    documents,
):
    f32 = jnp.float32
    bf16 = jnp.bfloat16
    rows, part = tokens.shape
    tp_count = lax.axis_size("tp")
    sp_count = lax.axis_size("sp")
    width = part * tp_count
    head_dim = HEAD_DIM
    q_local = w_query.shape[1] // head_dim
    kv_local = w_key.shape[1] // head_dim
    groups = q_local // kv_local
    if fused_plan(
        lax.axis_size("grp"),
        sp_count,
        tp_count,
        rows,
        part,
        w_query.shape[0],
        w_attn_out.shape[0],
        w_query.shape[1],
        w_key.shape[1],
        w_input.shape[1],
    ):
        return fused_layer(
            tokens,
            gain,
            (w_key, w_value, w_cgate, w_input, w_bgate, w_query),
            (w_attn_out, w_conv_out),
            sink_logit,
            taps,
            conv_bias,
            documents,
            sp_count,
        )
    wq, wk, wv, wu, wb, wc, w_attn, w_conv = (
        lax.all_gather(w_query, "sp", axis=0, tiled=True),
        lax.all_gather(w_key, "sp", axis=0, tiled=True),
        lax.all_gather(w_value, "sp", axis=0, tiled=True),
        lax.all_gather(w_input, "sp", axis=0, tiled=True),
        lax.all_gather(w_bgate, "sp", axis=0, tiled=True),
        lax.all_gather(w_cgate, "sp", axis=0, tiled=True),
        lax.all_gather(w_attn_out, "sp", axis=0, tiled=True),
        lax.all_gather(w_conv_out, "sp", axis=0, tiled=True),
    )
    matrices = (wq, wk, wv, wu, wb, wc)
    piece_f = lax.all_gather(tokens, "tp", axis=1, tiled=True).astype(f32)
    scaled = (piece_f * gain[None, :]).astype(bf16)
    products = tuple((jnp.dot(scaled, mat, preferred_element_type=f32) for mat in matrices))
    folded = products + (jnp.sum(piece_f * piece_f, axis=1),)
    sums = folded[:6]
    squares = folded[6]
    inv = lax.rsqrt(squares / width + EPS)[:, None]
    q_acc, k_acc, v_acc, u_acc, b_acc, c_acc = sums
    positions = lax.axis_index("sp") * rows + jnp.arange(rows, dtype=jnp.int32)
    query = rotate(q_acc * inv, positions, q_local).astype(bf16)
    keys = rotate(k_acc * inv, positions, kv_local).astype(bf16)
    values = (v_acc * inv).astype(bf16)
    carried = (c_acc * inv * (u_acc * inv)).astype(bf16)
    bgate = b_acc * inv
    doc_col = documents.astype(f32).astype(bf16)[:, None]
    paired = jnp.concatenate([keys, values], axis=1)
    pair_ext, doc_ext = (
        extended(paired, (("sp", 0),), WINDOW),
        extended(doc_col, (("sp", 0),), WINDOW),
    )
    carry_ext, doc_near = (extended(carried, (("sp", 0),), 1), extended(doc_col, (("sp", 0),), 1))
    key_width = kv_local * head_dim
    key_ext = pair_ext[:, :key_width].reshape(-1, kv_local, head_dim)
    val_ext = pair_ext[:, key_width:].reshape(-1, kv_local, head_dim)
    key_doc = doc_ext[:, 0].astype(f32)
    own_doc = doc_col[:, 0].astype(f32)
    key_pos = positions[0] - WINDOW + jnp.arange(rows + 2 * WINDOW, dtype=jnp.int32)
    total = sp_count * rows
    sinks = sink_logit.reshape(kv_local, groups, 1, 1)
    block = rows // 2
    outputs = []
    for begin in range(0, rows, block):
        span = block + 2 * WINDOW
        q_block = query[begin : begin + block].reshape(block, kv_local, groups, head_dim)
        k_block = key_ext[begin : begin + span]
        v_block = val_ext[begin : begin + span]
        q_pos = positions[begin : begin + block]
        k_pos = key_pos[begin : begin + span]
        scores = jnp.einsum(
            "qhgd,khd->hgqk", q_block, k_block, preferred_element_type=f32
        ) * head_dim ** (-0.5)
        allowed = jnp.abs(q_pos[:, None] - k_pos[None, :]) <= WINDOW
        allowed = allowed & (
            own_doc[begin : begin + block, None] == key_doc[None, begin : begin + span]
        )
        allowed = allowed & (k_pos >= 0)[None, :] & (k_pos < total)[None, :]
        weight = sink_softmax(scores, allowed, sinks).astype(bf16)
        result = jnp.einsum("hgqk,khd->qhgd", weight, v_block, preferred_element_type=f32)
        outputs.append(result.astype(bf16).reshape(block, q_local * head_dim))
    attended = jnp.concatenate(outputs, axis=0)
    near_doc = doc_near[:, 0].astype(f32)
    conv = jnp.zeros((rows, carried.shape[1]), f32)
    for tap in range(3):
        same = (near_doc[tap : tap + rows] == near_doc[1 : rows + 1])[:, None]
        conv = conv + jnp.where(
            same, carry_ext[tap : tap + rows].astype(f32) * taps[tap][None, :], 0.0
        )
    convolved = (bgate * (conv + conv_bias[None, :])).astype(bf16)
    acc = jnp.dot(
        lax.all_gather(attended, "tp", axis=1, tiled=True), w_attn, preferred_element_type=f32
    )
    mixed = acc + jnp.dot(
        lax.all_gather(convolved, "tp", axis=1, tiled=True), w_conv, preferred_element_type=f32
    )
    return mixed.astype(bf16)


def solution(mesh):
    placed = (
        P(("grp", "sp"), "tp"),
        P(),
        P("sp", "tp"),
        P("sp", "tp"),
        P("sp", "tp"),
        P("sp", "tp"),
        P("sp", "tp"),
        P("sp", "tp"),
        P("sp", "tp"),
        P("sp", "tp"),
        P("tp"),
        P(None, "tp"),
        P("tp"),
        P(("grp", "sp")),
    )
    return jax.shard_map(
        local, mesh=mesh, in_specs=placed, out_specs=P(("grp", "sp"), "tp"), check_vma=False
    )
```
